512 devices in a mesh: sp: 32 (over z, x), tp: 16 (over y, core).
Axes of the slice: x: 4, y: 8, z: 8, core: 2. Of those that a mesh axis runs over, the one named last changes fastest.
Arguments:
- tokens: bfloat16 [4096, 2048], P('sp'), may hold values from -6 to 6
- query_narrow: bfloat16 [4096, 2048], P('sp', 'tp'), may hold values from -20 to 20
- key_narrow: bfloat16 [4096, 2048], P('sp', 'tp'), may hold values from -20 to 20
- value_narrow: bfloat16 [4096, 2048], P('sp', 'tp'), may hold values from -6 to 6
- query_broad: bfloat16 [4096, 4096], P('sp', 'tp'), may hold values from -20 to 20
- key_broad: bfloat16 [4096, 4096], P('sp', 'tp'), may hold values from -20 to 20
- value_broad: bfloat16 [4096, 2048], P('sp', 'tp'), may hold values from -6 to 6
- mix_lambda: float32 [2, 16], P(None, 'tp'), may hold values from 0.3 to 0.8
- head_gain: float32 [2, 128], replicated, may hold values from 0.1 to 1.9
- proj_narrow: bfloat16 [2048, 2048], P('tp'), may hold values from -0.09375 to 0.09375
- proj_broad: bfloat16 [2048, 2048], P('tp'), may hold values from -0.09375 to 0.09375
- gain_one: float32 [2048], replicated, may hold values from 0.1 to 1.9
- gain_two: float32 [2048], replicated, may hold values from 0.1 to 1.9
- expert_ids: int32 [4096, 2], P('sp'), may hold values from 0 to 31, all different within a row; in each aligned block of 128 rows (0 to 127, 128 to 255, ...) at most 16 rows name the same one
- expert_gates: float32 [4096, 2], P('sp'), may hold values from 0.1 to 0.9
- gate_weight: bfloat16 [32, 2048, 4096], P('sp', None, 'tp'), may hold values from -0.125 to 0.125
- up_weight: bfloat16 [32, 2048, 4096], P('sp', None, 'tp'), may hold values from -0.125 to 0.125
- down_weight: bfloat16 [32, 4096, 2048], P('sp', 'tp'), may hold values from -0.09375 to 0.09375
Outputs:
- result: bfloat16 [4096, 2048], P('sp')
The draws below stay inside these ranges and needn't reach their ends.
Inputs may be any that keep to these rules, and one draw needn't show every extreme that they name: `expert_ids`: the 2 experts of a token differ. Among the tokens of one index of sp (aligned blocks of 128 tokens) no expert is named by more than 16 tokens, and in some blocks one expert is named by exactly 16.
All inputs are finite; a program needn't handle non-finite values.
Results may differ from the reference program's by a relative error of at most 0.015.
Values may be sent and summed in bfloat16 or wider, within the bound.
A program may use at most 64 MiB of HBM per device.

```python
import math
import jax
import jax.numpy as jnp
import numpy as np
from jax import lax

D = 2048
HEADS = 16
QK_NARROW = 64
QK_BROAD = 128
V = 128
EXPERTS = 32
FF_EXP = 4096
TOP = 2
CAP = 16
TOK_DEV = 128
TOKENS = 4096
N_SP = 32
N_TP = 16


def draw_queries(key, key_width, salt):
    base = jax.random.normal(jax.random.fold_in(key, salt), (TOKENS, HEADS, 2, key_width), jnp.float32)
    base = jnp.clip(base * 1.35, -8.0, 8.0)
    return base.reshape(TOKENS, HEADS * 2 * key_width).astype(jnp.bfloat16)


def draw_keys(key, key_width, salt):
    base = jax.random.normal(jax.random.fold_in(key, salt), (TOKENS, HEADS, 2, key_width), jnp.float32)
    base = jnp.clip(base * 1.35, -8.0, 8.0)
    return base.reshape(TOKENS, HEADS * 2 * key_width).astype(jnp.bfloat16)


def draw_query_narrow(key, part):
    return draw_queries(key, QK_NARROW, 31)


def draw_key_narrow(key, part):
    return draw_keys(key, QK_NARROW, 32)


def draw_query_broad(key, part):
    return draw_queries(key, QK_BROAD, 33)


def draw_key_broad(key, part):
    return draw_keys(key, QK_BROAD, 34)


def block_scale(own_key, shape, cuts, least, top_value):
    factor_of, own = 1.0, jax.random.fold_in(own_key, 6)
    for axis_at, blocks in cuts:
        steps = jnp.exp(jax.random.uniform(jax.random.fold_in(own, axis_at), (blocks,), jnp.float32, least / len(cuts), top_value / len(cuts)))
        factor_of = factor_of * jnp.repeat(steps, shape[axis_at] // blocks).reshape([-1 if axis == axis_at else 1 for axis in range(len(shape))])
    return factor_of


def shared_out(own_key, own, number, rows, count, top, most, lean):
    sequence = jax.random.permutation(own_key, count)
    heavy_load, common = portions_of(count, rows * top, most, lean, True), portions_of(count, rows * top, most, lean, False)
    places = jnp.arange(count)

    def named(lengths, rotation):
        used = int((lengths > 0).sum())
        fixed = max(1, used // 4)
        moved = fixed + (places - fixed + rotation * (used - fixed)) % max(1, count - fixed)
        return jnp.zeros((count,), jnp.int32).at[sequence[jnp.where(places < fixed, places, moved)]].set(jnp.asarray(lengths, jnp.int32))

    lengths = jnp.where(number % 4 == 0, named(heavy_load, number // 4), named(common, number - number // 4 - 1))
    mixed = jax.random.permutation(jax.random.fold_in(own, 3), count)
    donor, taker = mixed[0:count // 2 * 2:2], mixed[1:count // 2 * 2:2]
    margin = jnp.minimum(lengths[donor] - 1, most - lengths[taker]) // 2
    margin = jnp.where((donor == sequence[0]) | (taker == sequence[0]) | (lengths[taker] == 0), 0, jnp.maximum(margin, 0))
    moved = jax.random.randint(jax.random.fold_in(own, 4), (count // 2,), 0, 1 << 20) % (margin + 1)
    lengths = lengths.at[donor].add(-moved).at[taker].add(moved)
    items = jnp.searchsorted(jnp.cumsum(lengths), jnp.arange(rows * top), side="right").astype(jnp.int32)
    listing = items.reshape(top, rows).T
    listing = listing[jax.random.permutation(jax.random.fold_in(own, 1), rows)]
    rotation = jax.random.randint(jax.random.fold_in(own, 2), (rows, 1), 0, top)
    return jnp.take_along_axis(listing, (jnp.arange(top)[None, :] + rotation) % top, axis=1)


def portions_of(amount, total, most, lean, full):
    weights = [(1 << 20) // math.isqrt(standing ** lean) + 1 for standing in range(1, amount + 1)]
    largest = most if full else min(most, max(-(-total // amount), total * weights[0] // sum(weights)))
    least = 1 if total - largest >= amount - 1 else 0
    given, spare = [largest] + [least] * (amount - 1), total - largest - least * (amount - 1)
    while spare > 0:
        movable = [i for i in range(1, amount) if given[i] < largest] or [i for i in range(1, amount) if given[i] < most]
        whole, budget = sum([weights[i] for i in movable]), spare
        for i in movable:
            extra = min(most - given[i], max(1, budget * weights[i] // whole), spare)
            given[i] = given[i] + extra
            spare = spare - extra
    return np.array(given)


def noise(own_key, dims, deviation, reach, split=(), kind=jnp.bfloat16):
    level = block_scale(own_key, dims, split, -0.22, 0.18) if split else 1.0
    values = jax.random.normal(own_key, dims, jnp.float32) * deviation * level
    return jnp.minimum(jnp.maximum(values, -reach), reach).astype(kind)


def setup_inputs(seed: int = 0) -> dict:
    arg_keys = jax.random.split(jax.random.key(seed), 19)
    tokens = noise(arg_keys[0], (TOKENS, D), 1.0, 6.0, ((0, 32),))
    query_narrow = draw_query_narrow(jax.random.fold_in(arg_keys[18], 71), 0)
    key_narrow = draw_key_narrow(jax.random.fold_in(arg_keys[18], 71), 0)
    value_narrow = noise(arg_keys[3], (TOKENS, HEADS * V), 1.0, 6.0, ((0, 32), (1, 16)))
    query_broad = draw_query_broad(jax.random.fold_in(arg_keys[18], 71), 0)
    key_broad = draw_key_broad(jax.random.fold_in(arg_keys[18], 71), 0)
    value_broad = noise(arg_keys[6], (TOKENS, HEADS * V), 1.0, 6.0, ((0, 32), (1, 16)))
    mix_lambda = jnp.clip(0.3 + 0.5 * jax.random.uniform(arg_keys[7], (2, HEADS), jnp.float32) ** block_scale(arg_keys[7], (2, HEADS), ((1, 16),), -0.2, 0.2), 0.3, 0.8)
    head_gain = jnp.clip(1.0 + 0.18 * jax.random.normal(arg_keys[8], (2, V), jnp.float32), 0.1, 1.9)
    proj_narrow = noise(arg_keys[9], (HEADS * V, D), (2 * HEADS * V) ** -0.5, 0.09375, ((0, 16),))
    proj_broad = noise(arg_keys[10], (HEADS * V, D), (2 * HEADS * V) ** -0.5, 0.09375, ((0, 16),))
    gain_one = jnp.clip(1.0 + 0.18 * jax.random.normal(arg_keys[11], (D,), jnp.float32), 0.1, 1.9)
    gain_two = jnp.clip(1.0 + 0.18 * jax.random.normal(arg_keys[12], (D,), jnp.float32), 0.1, 1.9)
    expert_ids_keys = jax.random.split(jax.random.fold_in(arg_keys[13], 1), TOKENS // TOK_DEV)
    expert_ids_turns = jax.random.permutation(jax.random.fold_in(arg_keys[13], 3), TOKENS // TOK_DEV)
    expert_ids = jax.vmap(lambda own, number: shared_out(jax.random.fold_in(arg_keys[13], 2), own, number, TOK_DEV, EXPERTS, TOP, CAP, 2))(expert_ids_keys, expert_ids_turns).reshape((TOKENS, TOP))
    expert_gates = jnp.clip(0.1 + 0.79999997 * jax.random.uniform(arg_keys[14], (TOKENS, TOP), jnp.float32) ** block_scale(arg_keys[14], (TOKENS, TOP), ((0, 32),), -0.2, 0.2), 0.1, 0.9)
    gate_weight = noise(arg_keys[15], (EXPERTS, D, FF_EXP), D ** -0.5, 0.125, ((0, 32), (2, 16)))
    up_weight = noise(arg_keys[16], (EXPERTS, D, FF_EXP), D ** -0.5, 0.125, ((0, 32), (2, 16)))
    down_weight = noise(arg_keys[17], (EXPERTS, FF_EXP, D), FF_EXP ** -0.5, 0.09375, ((0, 32), (1, 16)))
    return dict(tokens=tokens, query_narrow=query_narrow, key_narrow=key_narrow, value_narrow=value_narrow, query_broad=query_broad, key_broad=key_broad, value_broad=value_broad, mix_lambda=mix_lambda, head_gain=head_gain, proj_narrow=proj_narrow, proj_broad=proj_broad, gain_one=gain_one, gain_two=gain_two, expert_ids=expert_ids, expert_gates=expert_gates, gate_weight=gate_weight, up_weight=up_weight, down_weight=down_weight)


deep_alpha = 8.0 ** 0.25
norm_eps = 1e-05

def layer_scale(inputs, gains):
    center = lax.optimization_barrier(jnp.mean(inputs, -1, keepdims=True))
    spread = lax.optimization_barrier(jnp.mean(jnp.square(inputs - center), -1, keepdims=True))
    return (inputs - center) * lax.rsqrt(spread + norm_eps) * gains

def group_heads(queries, key_rows, values, mixing, gains, key_width):
    count = queries.shape[0]
    stacked_q = jnp.moveaxis(queries.reshape(count, HEADS, 2, key_width), 1, 0)
    stacked_k = jnp.moveaxis(key_rows.reshape(count, HEADS, 2, key_width), 1, 0)
    stacked_v = jnp.moveaxis(values.reshape(count, HEADS, V), 1, 0)
    factor = key_width ** (-0.5)

    def one_head(members):
        head_q, head_k, head_v, weight = members
        scores = jnp.einsum('qmd,kmd->mqk', head_q.astype(jnp.float32), head_k.astype(jnp.float32)) * factor
        highest = lax.optimization_barrier(jnp.max(scores, -1, keepdims=True))
        exponent = jnp.exp(scores - highest)
        totals = lax.optimization_barrier(jnp.sum(exponent, -1))
        probs = lax.optimization_barrier(exponent.astype(jnp.bfloat16))
        numer = jnp.einsum('mqk,kv->mqv', probs.astype(jnp.float32), head_v.astype(jnp.float32))
        diff = numer[0] / totals[0][:, None] - weight * numer[1] / totals[1][:, None]
        normed = diff * lax.rsqrt(lax.optimization_barrier(jnp.mean(diff * diff, -1, keepdims=True)) + norm_eps) * gains
        return normed.astype(jnp.bfloat16)
    output = lax.map(one_head, (stacked_q, stacked_k, stacked_v, mixing))
    return jnp.moveaxis(output, 0, 1).reshape(count, HEADS * V)

def attention_sum(heads_first, heads_second, proj_narrow, proj_broad):
    count = heads_first.shape[0]
    block_width = HEADS // N_TP * V
    first_blocks = jnp.moveaxis(heads_first.reshape(count, N_TP, block_width), 1, 0)
    second_blocks = jnp.moveaxis(heads_second.reshape(count, N_TP, block_width), 1, 0)
    first_weights = proj_narrow.reshape(N_TP, block_width, D)
    second_weights = proj_broad.reshape(N_TP, block_width, D)

    def add_block(running, members):
        part_one, part_two, weight_one, weight_two = members
        partial_value = jnp.dot(part_one, weight_one, preferred_element_type=jnp.float32)
        partial_value = partial_value + jnp.dot(part_two, weight_two, preferred_element_type=jnp.float32)
        rounded = lax.optimization_barrier(partial_value.astype(jnp.bfloat16))
        return (running + rounded.astype(jnp.float32), None)
    running, _ = lax.scan(add_block, jnp.zeros((count, D), jnp.float32), (first_blocks, second_blocks, first_weights, second_weights))
    return running

def one_expert(members):
    expert_rows, gate_part, up_part, down_part = members
    activated = (jax.nn.silu(jnp.dot(expert_rows, gate_part, preferred_element_type=jnp.float32)) * jnp.dot(expert_rows, up_part, preferred_element_type=jnp.float32)).astype(jnp.bfloat16)
    block_width = FF_EXP // N_TP
    act_blocks = jnp.moveaxis(activated.reshape(expert_rows.shape[0], N_TP, block_width), 1, 0)
    down_blocks = down_part.reshape(N_TP, block_width, D)

    def add_block(running, operands):
        product = jnp.dot(operands[0], operands[1], preferred_element_type=jnp.float32)
        rounded = lax.optimization_barrier(product.astype(jnp.bfloat16))
        return (running + rounded.astype(jnp.float32), None)
    running, _ = lax.scan(add_block, jnp.zeros((expert_rows.shape[0], D), jnp.float32), (act_blocks, down_blocks))
    return running.astype(jnp.bfloat16)

def reference(tokens, query_narrow, key_narrow, value_narrow, query_broad, key_broad, value_broad, mix_lambda, head_gain, proj_narrow, proj_broad, gain_one, gain_two, expert_ids, expert_gates, gate_weight, up_weight, down_weight):
    heads_first = group_heads(query_narrow, key_narrow, value_narrow, mix_lambda[0], head_gain[0], QK_NARROW)
    heads_second = group_heads(query_broad, key_broad, value_broad, mix_lambda[1], head_gain[1], QK_BROAD)
    attn = attention_sum(heads_first, heads_second, proj_narrow, proj_broad)
    mixed_rows = layer_scale(deep_alpha * tokens.astype(jnp.float32) + attn, gain_one).astype(jnp.bfloat16)
    chosen = expert_ids.reshape(N_SP, TOK_DEV * TOP).astype(jnp.int32)
    onehot = (chosen[:, :, None] == jnp.arange(EXPERTS, dtype=jnp.int32)[None, None, :]).astype(jnp.int32)
    before = jnp.cumsum(onehot, axis=1, dtype=jnp.int32) - onehot
    slot_index = lax.optimization_barrier(jnp.sum(before * onehot, axis=-1, dtype=jnp.int32))
    block_index = jnp.arange(N_SP, dtype=jnp.int32)[:, None]
    position = ((chosen * N_SP + block_index) * CAP + slot_index).reshape(-1).astype(jnp.int32)
    repeated = jnp.repeat(mixed_rows, TOP, axis=0)
    buffer = jnp.zeros((EXPERTS * N_SP * CAP, D), jnp.bfloat16).at[position].set(repeated)
    buffer = buffer.reshape(EXPERTS, N_SP * CAP, D)
    outputs = lax.map(one_expert, (buffer, gate_weight, up_weight, down_weight))
    picked = outputs.reshape(EXPERTS * N_SP * CAP, D)[position].reshape(N_SP * TOK_DEV, TOP, D)
    routed = lax.optimization_barrier(jnp.sum(expert_gates[:, :, None] * picked.astype(jnp.float32), axis=1))
    return layer_scale(deep_alpha * mixed_rows.astype(jnp.float32) + routed, gain_two).astype(jnp.bfloat16)
```

```python
import functools

import jax
import jax.numpy as jnp
from jax import lax
from jax.experimental import pallas as pl
from jax.experimental.pallas import tpu as pltpu
from jax.sharding import Mesh
from jax.sharding import PartitionSpec as P

MESH = pl.DeviceIdType.MESH
NZ, NX, NY = 8, 4, 8
NSP = NZ * NX
CAP = 16
F32, BF16 = jnp.float32, jnp.bfloat16
ALPHA = 8.0**0.25
EPS = 1e-05
LOG2E = 1.4426950408889634
SCALES = (64**-0.5 * LOG2E, 128**-0.5 * LOG2E)


def dot(a, b, ca, cb):
    return lax.dot_general(a, b, (((ca,), (cb,)), ((), ())), preferred_element_type=F32)


def wait(ref, sem):
    pltpu.make_async_copy(ref, ref, sem).wait()


def send(src, dst, send_sem, recv_sem, dev):
    pltpu.make_async_remote_copy(
        src_ref=src, dst_ref=dst, send_sem=send_sem, recv_sem=recv_sem, device_id=dev, device_id_type=MESH
    ).start()


def row_iota(shape):
    return lax.broadcasted_iota(jnp.int32, shape, 0)


def lane_iota(shape):
    return lax.broadcasted_iota(jnp.int32, shape, 1)


def kernel(
    lam, ids, gates, hgain, g1, g2, tok, qn, kn, vn, qb, kb, vb, pn, pb, gw, uw, dw,
    out,
    kv, qraw, qs, acc, ml, osend, orecv, ssend, srecv, wp, wpt, tokraw, tokt, rows, cols, dmat, pmat,
    heads, rsend, rrecv, stat1, mixed, disp, xg, wg, wu, wd, accg, accu, act, part, dsend, drecv,
    ret, eo, fin, stat2, outb,
    loc, kvs, kvr, qsd, qrv, wsd, wrv, osd, orv, ssd, srv, hsd, hrv, rsd, rrv, s1s, s1r, dps, dpr,
    xgs, xgr, dds, ddr, rts, rtr, fns, fnr, s2s, s2r, oud,
):
    z, x, y, c = (lax.axis_index(n) for n in ("z", "x", "y", "c"))
    me = z * NX + x
    own = 2 * y + c
    other = 1 - c
    half = me // 16
    zp, zm = lax.rem(z + 1, NZ), lax.rem(z + NZ - 1, NZ)
    yp, ym = lax.rem(y + 1, NY), lax.rem(y + NY - 1, NY)
    partner = (z, x, y, other)

    def col(j):
        return pl.ds(pl.multiple_of(j * 128, 128), 128)

    def local(i, src, dst):
        cp = pltpu.make_async_copy(src, dst, loc.at[i])
        cp.start()
        return cp

    first = [
        local(0, kn, kv.at[0, 0]), local(1, vn, kv.at[0, 1]),
        local(2, kb.at[:, pl.ds(0, 128)], kv.at[0, 2]), local(3, kb.at[:, pl.ds(128, 128)], kv.at[0, 3]),
        local(4, vb, kv.at[0, 4]),
        local(5, qn, qraw.at[0, 0]), local(6, qb.at[:, pl.ds(0, 128)], qraw.at[0, 1]),
        local(7, qb.at[:, pl.ds(128, 128)], qraw.at[0, 2]),
    ]
    tokcp = local(8, tok.at[:, col(own)], tokraw)

    barrier = pltpu.get_barrier_semaphore()

    def greet(j, carry):
        t = lax.rem(me + j, NSP)
        for cc in (c, other):
            pl.semaphore_signal(barrier, inc=1, device_id=(t // NX, lax.rem(t, NX), y, cc), device_id_type=MESH)
        return carry

    lax.fori_loop(1, NSP, greet, 0)
    for dy in range(NY):
        for dc in range(2):
            if dy or dc:
                pl.semaphore_signal(
                    barrier, inc=1, device_id=(z, x, lax.rem(y + dy, NY), c if dc == 0 else other), device_id_type=MESH
                )
    pl.semaphore_wait(barrier, 2 * (NSP - 1) + 2 * NY - 1)

    for cp in first:
        cp.wait()
    N, B = pl.ds(0, 2), pl.ds(2, 3)

    def kv_send(d, step, piece, src_slot, dst_slot):
        part_of = (N, B)[piece]
        send(
            kv.at[src_slot, part_of], kv.at[dst_slot, part_of], kvs.at[d, step, piece], kvr.at[dst_slot, piece],
            ((zp, zm)[d], x, y, c),
        )

    def kv_wait(slot, piece):
        wait(kv.at[slot, (N, B)[piece]], kvr.at[slot, piece])

    for piece in (0, 1):
        kv_send(0, 0, piece, 0, 1)
        kv_send(1, 0, piece, 0, 5)
    for r in (2, 1, 3):
        send(qraw.at[0], qraw.at[r], qsd.at[r - 1], qrv.at[r - 1], (z, lax.rem(x + NX - r, NX), y, c))

    def proj(j, carry):
        for k, w in enumerate((pn, pb)):
            dst = pl.ds(k * 128, 128)
            pltpu.make_async_copy(w.at[:, col(2 * j + c)], wp.at[0, j, dst], loc.at[9]).start()
            send(w.at[:, col(2 * j + other)], wp.at[1, j, dst], wsd.at[0], wrv.at[0], partner)
        return carry

    lax.fori_loop(0, NY, proj, 0)
    for k, (w, buf) in enumerate(((gw, wg), (uw, wu), (dw, wd))):
        local(10 + k, w.at[0], buf.at[0])
        send(w.at[0], buf.at[1], wsd.at[1 + k], wrv.at[1 + k], partner)

    lane = lane_iota((128, 128))
    sub = row_iota((128, 128))
    idf = ids[...].astype(F32)
    gat = gates[...]
    table = jnp.where(lane == 0, idf[:, 0:1], jnp.where(lane == 1, idf[:, 1:2], 0.0))
    idr = table.T
    rows_e = row_iota((NSP, 128)).astype(F32)
    hot = [(idr[k : k + 1, :] == rows_e).astype(F32) for k in range(2)]
    upper = (sub < lane).astype(F32).astype(BF16)
    before = dot((hot[0] + hot[1]).astype(BF16), upper, 1, 0)
    pos = [
        idr[k : k + 1, :] * float(CAP) + jnp.sum(before * hot[k], axis=0, keepdims=True) for k in range(2)
    ]
    rows_s = row_iota((CAP * NSP, 128)).astype(F32)
    dmat[...] = ((pos[0] == rows_s).astype(F32) + (pos[1] == rows_s).astype(F32)).astype(BF16)
    posc = jnp.where(sub == 0, pos[0], jnp.where(sub == 1, pos[1], 0.0)).T
    lanes_s = lane_iota((128, CAP * NSP)).astype(F32)
    for k in range(2):
        pmat[k] = (posc[:, k : k + 1] == lanes_s).astype(F32).astype(BF16)
    gain_rows = jnp.where(
        sub == 0, hgain[0:1, :], jnp.where(sub == 1, hgain[1:2, :], jnp.where(sub == 2, g1[pl.ds(own, 1), :], 0.0))
    )
    cols[...] = gain_rows.T
    tokcp.wait()
    tokt[...] = tokraw[...].astype(F32).T

    for r in (1, 3, 2):
        wait(qraw.at[r], qrv.at[r - 1])
    low = lane < 64
    for r in range(NX):
        at = pl.ds(r * 128, 128)
        narrow = qraw[r, 0]
        qs[0, at, :] = jnp.where(low, narrow, jnp.zeros_like(narrow))
        qs[1, at, :] = jnp.where(low, jnp.zeros_like(narrow), narrow)
        qs[2, at, :] = qraw[r, 1]
        qs[3, at, :] = qraw[r, 2]

    def attend(group, slots, start):
        def one_map(i, carry):
            m = group * 2 + i
            k_at = 0 if group == 0 else 2 + i
            v_at = 1 if group == 0 else 4
            query = qs[m]
            scores = [dot(kv[s, k_at], query, 1, 1) for s in slots]
            top = functools.reduce(jnp.maximum, [jnp.max(s, axis=0, keepdims=True) for s in scores])
            if not start:
                old = ml[pl.ds(m, 1), :]
                top = jnp.maximum(old, top)
            expo = [jnp.exp2((s - top) * SCALES[group]) for s in scores]
            total = functools.reduce(jnp.add, [jnp.sum(e, axis=0, keepdims=True) for e in expo])
            numer = functools.reduce(
                jnp.add, [dot(kv[s, v_at], e.astype(BF16), 0, 0) for s, e in zip(slots, expo)]
            )
            if start:
                acc[m] = numer
                ml[pl.ds(4 + m, 1), :] = total
            else:
                shrink = jnp.exp2((old - top) * SCALES[group])
                acc[m] = acc[m] * shrink + numer
                ml[pl.ds(4 + m, 1), :] = ml[pl.ds(4 + m, 1), :] * shrink + total
            ml[pl.ds(m, 1), :] = top
            return carry

        lax.fori_loop(0, 2, one_map, 0)

    def arrive(d, piece):
        kv_wait(d, piece)
        if d < 3 or piece == 0:
            kv_send(0, d, piece, d, d + 1)
        kv_wait(4 + d, piece)
        if d < 3:
            kv_send(1, d, piece, 4 + d, 5 + d)
        elif piece == 1:
            kv_send(1, d, piece, 7, 4)

    arrive(1, 0)
    attend(0, (0,), True)
    arrive(1, 1)
    attend(1, (0,), True)
    arrive(2, 0)
    attend(0, (1, 5), False)
    arrive(2, 1)
    attend(1, (1, 5), False)
    arrive(3, 0)
    attend(0, (2, 6), False)
    arrive(3, 1)
    attend(1, (2, 6), False)
    attend(0, (3, 7), False)
    kv_wait(4, 0)
    attend(1, (3, 7), False)
    attend(0, (4,), False)
    kv_wait(4, 1)
    attend(1, (4,), False)

    for r in (2, 1, 3):
        at = pl.ds(r * 128, 128)
        ssend[r - 1] = ml[:, at]
        for m in range(4):
            osend[r - 1, m] = acc[m, :, at].astype(BF16)
        dev = (z, lax.rem(x + r, NX), y, c)
        send(osend.at[r - 1], orecv.at[r - 1], osd.at[r - 1], orv.at[r - 1], dev)
        send(ssend.at[r - 1], srecv.at[r - 1], ssd.at[r - 1], srv.at[r - 1], dev)

    wait(wp.at[0], loc.at[9])
    wait(wp.at[1], wrv.at[0])

    def turn(j, carry):
        for s in range(2):
            wpt[j, :, pl.ds(s * 256, 256)] = wp[s, j].T
        return carry

    lax.fori_loop(0, NY, turn, 0)

    for r in (1, 3, 2):
        wait(orecv.at[r - 1], orv.at[r - 1])
        wait(srecv.at[r - 1], srv.at[r - 1])
    for g in range(2):
        means = []
        for i in range(2):
            m = 2 * g + i
            tops = [ml[m : m + 1, 0:128]] + [srecv[r, m : m + 1, :] for r in range(3)]
            sums = [ml[4 + m : 5 + m, 0:128]] + [srecv[r, 4 + m : 5 + m, :] for r in range(3)]
            nums = [acc[m, :, 0:128]] + [orecv[r, m].astype(F32) for r in range(3)]
            top = functools.reduce(jnp.maximum, tops)
            w = [jnp.exp2((t - top) * SCALES[g]) for t in tops]
            total = functools.reduce(jnp.add, [a * b for a, b in zip(w, sums)])
            numer = functools.reduce(jnp.add, [a * b for a, b in zip(w, nums)])
            means.append(numer * ((1.0 if i == 0 else lam[g, 0]) / total))
        diff = means[0] - means[1]
        scale = lax.rsqrt(jnp.mean(diff * diff, axis=0, keepdims=True) + EPS)
        heads[0, pl.ds(g * 128, 128), :] = (diff * scale * cols[:, g : g + 1]).astype(BF16)
    send(heads.at[0], heads.at[1], hsd.at[0], hrv.at[0], partner)
    wait(heads.at[1], hrv.at[0])

    both = jnp.concatenate([heads[0], heads[1]], axis=0)
    for r in (4, 3, 5, 2, 6, 1, 7):
        t = lax.rem(y + r, NY)
        rsend[r - 1] = dot(wpt[t], both, 1, 0).astype(BF16)
        send(rsend.at[r - 1], rrecv.at[r - 1], rsd.at[r - 1], rrv.at[r - 1], (z, x, t, c))
    zt = ALPHA * tokt[...] + dot(wpt[y], both, 1, 0)
    for r in (1, 7, 2, 6, 3, 5, 4):
        wait(rrecv.at[r - 1], rrv.at[r - 1])
        zt = zt + rrecv[r - 1].astype(F32)

    sub8 = row_iota((8, 128))

    def local_stats(mean, dev2):
        return jnp.where(sub8 == 0, mean, jnp.where(sub8 == 1, dev2, 0.0))

    mean = jnp.mean(zt, axis=0, keepdims=True)
    dev2 = jnp.sum(jnp.square(zt - mean), axis=0, keepdims=True)
    stat1[0] = local_stats(mean, dev2)
    order = [(dy, dc) for dy in (4, 3, 5, 2, 6, 1, 7, 0) for dc in (1, 0) if dy or dc]
    for dy, dc in order:
        s = 2 * dy + dc
        send(
            stat1.at[0], stat1.at[s], s1s.at[s - 1], s1r.at[s - 1],
            (z, x, lax.rem(y + dy, NY), c if dc == 0 else other),
        )
    for s in range(1, 16):
        wait(stat1.at[s], s1r.at[s - 1])
    total = functools.reduce(jnp.add, [stat1[s] for s in range(16)])
    mean = total[0:1, :] * (1.0 / 16)
    spread = total[1:2, :] + 128.0 * functools.reduce(
        jnp.add, [jnp.square(stat1[s, 0:1, :] - mean) for s in range(16)]
    )
    scale = lax.rsqrt(spread * (1.0 / 2048) + EPS)
    normed = ((zt - mean) * scale * cols[:, 2:3]).astype(BF16)

    disp[...] = dot(dmat[...], normed, 1, 1).astype(BF16)

    def unit(j):
        return pl.ds(pl.multiple_of(j * CAP, CAP), CAP)

    arrive_at = unit(c * 16 + lax.rem(me, 16))

    def dispatch(j, carry):
        t = lax.rem(me + j, NSP)
        send(disp.at[unit(t)], xg.at[0, arrive_at], dps.at[0], dpr.at[0], (t // NX, lax.rem(t, NX), y, half))
        return carry

    lax.fori_loop(1, NSP, dispatch, 0)

    @pl.when(half == c)
    def _():
        xg[0, arrive_at, :] = disp[unit(me), :]

    @pl.when(half != c)
    def _():
        send(disp.at[unit(me)], xg.at[0, arrive_at], dps.at[0], dpr.at[0], partner)

    mixed[...] = normed.astype(F32).T * ALPHA
    for k, buf in enumerate((wg, wu, wd)):
        wait(buf.at[0], loc.at[10 + k])
        wait(buf.at[1], wrv.at[1 + k])

    def wait_units(ref, sem):
        @pl.when(half == c)
        def _():
            wait(ref.at[pl.ds(0, 496)], sem)

        @pl.when(half != c)
        def _():
            wait(ref, sem)

    wait_units(xg.at[0], dpr.at[0])

    pieces = (pl.ds(0, 256), pl.ds(256, 256))

    def xg_send(d, step, piece, src_slot, dst_slot):
        send(
            xg.at[src_slot, pieces[piece]], xg.at[dst_slot, pieces[piece]], xgs.at[d, step, piece],
            xgr.at[dst_slot, piece], (z, x, (yp, ym)[d], c),
        )

    def xg_wait(slot, piece):
        wait(xg.at[slot, pieces[piece]], xgr.at[slot, piece])

    def xg_arrive(d, piece):
        xg_wait(d, piece)
        if d < 3 or piece == 0:
            xg_send(0, d, piece, d, d + 1)
        xg_wait(4 + d, piece)
        if d < 3:
            xg_send(1, d, piece, 4 + d, 5 + d)
        elif piece == 1:
            xg_send(1, d, piece, 7, 4)

    def slot_y(slot):
        away = NY - slot if slot <= 4 else slot - 4
        return lax.rem(y + away, NY)

    def absorb(slot, piece, start=False):
        chunk = 2 * slot_y(slot) + piece
        at = pl.ds(pl.multiple_of(chunk * 128, 128), 128)
        rows_in = xg[slot, pieces[piece], :]
        for s in range(2):
            for w, a in ((wg, accg), (wu, accu)):
                value = dot(rows_in, w[s, at, :], 1, 0)
                a[s] = value if start else a[s] + value

    for piece in (0, 1):
        xg_send(0, 0, piece, 0, 1)
        xg_send(1, 0, piece, 0, 5)
    absorb(0, 0, True)
    absorb(0, 1)
    for d in (1, 2, 3):
        for piece in (0, 1):
            xg_arrive(d, piece)
            absorb(d, piece)
            absorb(4 + d, piece)
    for piece in (0, 1):
        xg_wait(4, piece)
        absorb(4, piece)
    for s in range(2):
        g = accg[s]
        act[s] = (g / (1.0 + jnp.exp(-g)) * accu[s]).astype(BF16)

    def produce(r):
        at = pl.ds(pl.multiple_of(lax.rem(y + r, NY) * 256, 256), 256)
        part[r] = dot(act[0], wd[0, :, at], 1, 0) + dot(act[1], wd[1, :, at], 1, 0)

    def away(d, h, step):
        return (4 - h - step) if d == 0 else (NY - 3 - h + step) % NY

    def length(d, h):
        return 4 - h if d == 0 else 3 + h

    def pass_on(d, h, step):
        value = part[away(d, h, step), :, h * 128 : h * 128 + 128]
        if step:
            wait(drecv.at[d, h, step - 1], ddr.at[d, h, step - 1])
            value = value + drecv[d, h, step - 1].astype(F32)
        dsend[d, h, step] = value.astype(BF16)
        send(
            dsend.at[d, h, step], drecv.at[d, h, step], dds.at[d, h, step], ddr.at[d, h, step],
            (z, x, (yp, ym)[d], c),
        )

    produce(4)
    pass_on(0, 0, 0)
    pass_on(1, 1, 0)
    produce(3)
    pass_on(0, 1, 0)
    produce(5)
    pass_on(1, 0, 0)
    for r in (2, 6, 1, 7, 0):
        produce(r)
    for step in (1, 2, 3):
        for h in (0, 1):
            for d in ((0, 1) if h == 0 else (1, 0)):
                if step < length(d, h):
                    pass_on(d, h, step)
    for h in (0, 1):
        value = part[0, :, h * 128 : h * 128 + 128]
        for d in range(2):
            last = length(d, h) - 1
            wait(drecv.at[d, h, last], ddr.at[d, h, last])
            value = value + drecv[d, h, last].astype(F32)
        eo[h] = value.astype(BF16)

    ret_at = unit(me)

    def give_back(i, carry):
        t = c * 16 + i
        for h in range(2):
            @pl.when(jnp.logical_or(t != me, c != h))
            def _():
                send(eo.at[h, unit(i)], ret.at[ret_at], rts.at[0], rtr.at[0], (t // NX, lax.rem(t, NX), y, h))
        return carry

    lax.fori_loop(0, 16, give_back, 0)

    @pl.when(half == c)
    def _():
        ret[ret_at, :] = eo[c, unit(lax.rem(me, 16)), :]

    wait_units(ret, rtr.at[0])

    zz = mixed[...]
    for k in range(2):
        zz = zz + gat[:, k : k + 1] * dot(pmat[k], ret[...], 1, 0)

    mean = jnp.mean(zz, axis=1, keepdims=True)
    dev = zz - mean
    dev2 = jnp.sum(dev * dev, axis=1, keepdims=True)
    fin[0] = dev.astype(BF16)
    packed = jnp.where(lane == 0, mean, jnp.where(lane == 1, dev2, 0.0)).T
    stat2[0] = packed[0:8, :]
    send(fin.at[0], fin.at[1], fns.at[0], fnr.at[0], partner)
    for dy, dc in order:
        s = 2 * dy + dc
        dev_id = (z, x, lax.rem(y + dy, NY), c if dc == 0 else other)
        send(stat2.at[0], stat2.at[s], s2s.at[s - 1], s2r.at[s - 1], dev_id)
    for dy in (4, 3, 5, 2, 6, 1, 7):
        send(fin.at[0], fin.at[2 * dy], fns.at[2 * dy - 1], fnr.at[2 * dy - 1], (z, x, lax.rem(y + dy, NY), c))
    for s in range(1, 16):
        wait(stat2.at[s], s2r.at[s - 1])
    total = functools.reduce(jnp.add, [stat2[s] for s in range(16)])
    mean = total[0:1, :] * (1.0 / 16)
    spread = total[1:2, :] + 128.0 * functools.reduce(
        jnp.add, [jnp.square(stat2[s, 0:1, :] - mean) for s in range(16)]
    )
    scale = lax.rsqrt(spread * (1.0 / 2048) + EPS)
    table = jnp.where(sub == 16, scale, 0.0)
    for s in range(16):
        table = jnp.where(sub == s, stat2[s, 0:1, :] - mean, table)
    table = table.T

    def finish(dy, dc):
        s = 2 * dy + dc
        j = 2 * lax.rem(y + NY - dy, NY) + (c if dc == 0 else other)
        value = (fin[s].astype(F32) + table[:, s : s + 1]) * table[:, 16:17] * g2[pl.ds(j, 1), :]
        outb[s] = value.astype(BF16)
        pltpu.make_async_copy(outb.at[s], out.at[:, col(j)], oud.at[s]).start()

    finish(0, 0)
    wait(fin.at[1], fnr.at[0])
    finish(0, 1)
    arrivals = (1, 7, 2, 6, 3, 5, 4)
    for i, dy in enumerate(arrivals):
        wait(fin.at[2 * dy], fnr.at[2 * dy - 1])
        send(fin.at[2 * dy], fin.at[2 * dy + 1], fns.at[2 * dy], fnr.at[2 * dy], partner)
        finish(dy, 0)
        if i:
            before_dy = arrivals[i - 1]
            wait(fin.at[2 * before_dy + 1], fnr.at[2 * before_dy])
            finish(before_dy, 1)
    wait(fin.at[9], fnr.at[8])
    finish(4, 1)

    for step in range(4):
        for piece in (0, 1):
            for d in range(2):
                if step < 3 or piece == d:
                    wait(kv.at[0, (N, B)[piece]], kvs.at[d, step, piece])
                    wait(xg.at[0, pieces[piece]], xgs.at[d, step, piece])
                if step < length(d, piece):
                    wait(dsend.at[d, piece, step], dds.at[d, piece, step])
    for r in range(3):
        wait(qraw.at[0], qsd.at[r])
        wait(osend.at[r], osd.at[r])
        wait(ssend.at[r], ssd.at[r])
    wait(wp.at[0], wsd.at[0])
    for k, buf in enumerate((wg, wu, wd)):
        wait(buf.at[0], wsd.at[1 + k])
    wait(heads.at[0], hsd.at[0])
    for r in range(7):
        wait(rsend.at[r], rsd.at[r])
    for s in range(15):
        wait(stat1.at[0], s1s.at[s])
        wait(stat2.at[0], s2s.at[s])
        wait(fin.at[0], fns.at[s])
    wait_units(disp, dps.at[0])
    wait_units(ret, rts.at[0])
    for s in range(16):
        wait(outb.at[s], oud.at[s])


def on_device(
    tokens, query_narrow, key_narrow, value_narrow, query_broad, key_broad, value_broad, mix_lambda,
    head_gain, proj_narrow, proj_broad, gain_one, gain_two, expert_ids, expert_gates,
    gate_weight, up_weight, down_weight,
):
    vmem, anywhere = pl.BlockSpec(memory_space=pltpu.VMEM), pl.BlockSpec(memory_space=pltpu.HBM)
    dma = pltpu.SemaphoreType.DMA
    bf = lambda *s: pltpu.VMEM(s, BF16)
    fl = lambda *s: pltpu.VMEM(s, F32)
    scratch = [
        bf(8, 5, 128, 128), bf(4, 3, 128, 128), bf(4, 512, 128), fl(4, 128, 512), fl(8, 512),
        bf(3, 4, 128, 128), bf(3, 4, 128, 128), fl(3, 8, 128), fl(3, 8, 128),
        bf(2, 8, 256, 128), bf(8, 128, 512), bf(128, 128), fl(128, 128),
        fl(8, 128), fl(128, 128), bf(512, 128), bf(2, 128, 512),
        bf(2, 256, 128), bf(7, 128, 128), bf(7, 128, 128), fl(16, 8, 128),
        fl(128, 128), bf(512, 128), bf(8, 512, 128),
        bf(2, 2048, 256), bf(2, 2048, 256), bf(2, 256, 2048),
        fl(2, 256, 256), fl(2, 256, 256), bf(2, 256, 256), fl(8, 256, 256),
        bf(2, 2, 4, 256, 128), bf(2, 2, 4, 256, 128),
        bf(512, 128), bf(2, 256, 128), bf(16, 128, 128), fl(16, 8, 128), bf(16, 128, 128),
        dma((13,)), dma((2, 4, 2)), dma((8, 2)), dma((3,)), dma((3,)), dma((4,)), dma((4,)),
        dma((3,)), dma((3,)), dma((3,)), dma((3,)), dma((1,)), dma((1,)), dma((7,)), dma((7,)),
        dma((15,)), dma((15,)), dma((1,)), dma((1,)), dma((2, 4, 2)), dma((8, 2)),
        dma((2, 2, 4)), dma((2, 2, 4)), dma((1,)), dma((1,)), dma((15,)), dma((15,)), dma((15,)), dma((15,)),
        dma((16,)),
    ]
    return pl.pallas_call(
        kernel,
        out_shape=jax.ShapeDtypeStruct((128, 2048), BF16),
        in_specs=[pl.BlockSpec(memory_space=pltpu.SMEM)] + [vmem] * 5 + [anywhere] * 12,
        out_specs=anywhere,
        scratch_shapes=scratch,
        compiler_params=pltpu.CompilerParams(
            collective_id=0, has_side_effects=True, vmem_limit_bytes=60 * 1024 * 1024
        ),
        name="layer",
    )(
        mix_lambda, expert_ids, expert_gates, head_gain, gain_one.reshape(16, 128), gain_two.reshape(16, 128),
        tokens, query_narrow, key_narrow, value_narrow, query_broad, key_broad, value_broad,
        proj_narrow, proj_broad, gate_weight, up_weight, down_weight,
    )


def solution(mesh):
    finer = Mesh(mesh.devices.reshape(NZ, NX, NY, 2), ("z", "x", "y", "c"))
    sp, tp = ("z", "x"), ("y", "c")
    return jax.shard_map(
        on_device,
        mesh=finer,
        in_specs=(
            P(sp, None), P(sp, tp), P(sp, tp), P(sp, tp), P(sp, tp), P(sp, tp), P(sp, tp), P(None, tp),
            P(), P(tp, None), P(tp, None), P(), P(), P(sp, None), P(sp, None),
            P(sp, None, tp), P(sp, None, tp), P(sp, tp, None),
        ),
        out_specs=P(sp, None),
        check_vma=False,
    )
```

```python
import functools

import jax
import jax.numpy as jnp
from jax import lax
from jax.experimental import pallas as pl
from jax.experimental.pallas import tpu as pltpu
from jax.sharding import Mesh
from jax.sharding import PartitionSpec as P

MESH = pl.DeviceIdType.MESH
NZ, NX, NY = 8, 4, 8
NSP = NZ * NX
CAP = 16
F32, BF16 = jnp.float32, jnp.bfloat16
ALPHA = 8.0**0.25
EPS = 1e-05
LOG2E = 1.4426950408889634
SCALES = (64**-0.5 * LOG2E, 128**-0.5 * LOG2E)


def dot(a, b, ca, cb):
    return lax.dot_general(a, b, (((ca,), (cb,)), ((), ())), preferred_element_type=F32)


def wait(ref, sem):
    pltpu.make_async_copy(ref, ref, sem).wait()


def send(src, dst, send_sem, recv_sem, dev):
    pltpu.make_async_remote_copy(
        src_ref=src, dst_ref=dst, send_sem=send_sem, recv_sem=recv_sem, device_id=dev, device_id_type=MESH
    ).start()


def row_iota(shape):
    return lax.broadcasted_iota(jnp.int32, shape, 0)


def lane_iota(shape):
    return lax.broadcasted_iota(jnp.int32, shape, 1)


def kernel(
    lam_in, ids_in, gates_in, hgain_in, g1_in, g2_in, tok, qn, kn, vn, qb, kb, vb, pn, pb, gw, uw, dw,
    out,
    kv, qraw, qs, acc, ml, osend, orecv, ssend, srecv, wp, wpt, tokraw, tokt, cols, dmat, pmat, gat,
    heads, rsend, rrecv, stat1, mixed, disp, xg, wg, wu, wd, accg, accu, act, part, dsend, drecv,
    ret, eo, fin, stat2, lam, ids, gates, hgain, g1, g2, outb,
    loc, kvs, kvr, qsd, qrv, wsd, wrv, osd, orv, ssd, srv, hsd, hrv, rsd, rrv, s1s, s1r, dps, dpr,
    xgs, xgr, dds, ddr, rts, rtr, fns, fnr, s2s, s2r, smalls, ysem, oud,
):
    z, x, y, c = (lax.axis_index(n) for n in ("z", "x", "y", "c"))
    me = z * NX + x
    own = 2 * y + c
    other = 1 - c
    half = me // 16
    zp, zm = lax.rem(z + 1, NZ), lax.rem(z + NZ - 1, NZ)
    yp, ym = lax.rem(y + 1, NY), lax.rem(y + NY - 1, NY)
    partner = (z, x, y, other)

    def col(j):
        return pl.ds(pl.multiple_of(j * 128, 128), 128)

    def local(i, src, dst):
        cp = pltpu.make_async_copy(src, dst, loc.at[i])
        cp.start()
        return cp

    first = [
        local(0, kn, kv.at[0, 0]), local(1, vn, kv.at[0, 1]),
        local(2, kb.at[:, pl.ds(0, 128)], kv.at[0, 2]), local(3, kb.at[:, pl.ds(128, 128)], kv.at[0, 3]),
        local(4, vb, kv.at[0, 4]),
        local(5, qn, qraw.at[0, 0]), local(6, qb.at[:, pl.ds(0, 128)], qraw.at[0, 1]),
        local(7, qb.at[:, pl.ds(128, 128)], qraw.at[0, 2]),
    ]
    tokcp = local(8, tok.at[:, col(own)], tokraw)
    small = []
    for i, (src, dst) in enumerate(
        ((ids_in, ids), (gates_in, gates), (hgain_in, hgain), (g1_in, g1), (g2_in, g2), (lam_in, lam))
    ):
        small.append(pltpu.make_async_copy(src, dst, smalls.at[i]))
        small[-1].start()

    barrier = pltpu.get_barrier_semaphore()
    sides_y = ((z, x, yp, c), (z, x, ym, c))
    for dev in [(zp, x, y, c), (zm, x, y, c), partner, *sides_y] + [
        (z, lax.rem(x + r, NX), y, c) for r in range(1, NX)
    ]:
        pl.semaphore_signal(barrier, inc=1, device_id=dev, device_id_type=MESH)
    pl.semaphore_wait(barrier, 8)

    def relay(k):
        for dev in sides_y:
            pl.semaphore_signal(ysem.at[k], inc=1, device_id=dev, device_id_type=MESH)

    def relayed(k):
        pl.semaphore_wait(ysem.at[k], 2)

    for cp in first:
        cp.wait()
    def kv_send(d, step, piece, src_slot, dst_slot):
        send(
            kv.at[src_slot, piece], kv.at[dst_slot, piece], kvs.at[d, step, piece], kvr.at[dst_slot, piece],
            ((zp, zm)[d], x, y, c),
        )

    def kv_wait(slot, piece):
        wait(kv.at[slot, piece], kvr.at[slot, piece])

    for piece in range(5):
        kv_send(0, 0, piece, 0, 1)
        kv_send(1, 0, piece, 0, 5)
    q_parts = (pl.ds(0, 1), pl.ds(1, 2))
    for k in range(2):
        for r in (2, 1, 3):
            send(
                qraw.at[0, q_parts[k]], qraw.at[r, q_parts[k]], qsd.at[r - 1, k], qrv.at[r - 1, k],
                (z, lax.rem(x + NX - r, NX), y, c),
            )
    relay(0)

    def proj(j, carry):
        for k, w in enumerate((pn, pb)):
            dst = pl.ds(k * 128, 128)
            pltpu.make_async_copy(w.at[:, col(2 * j + c)], wp.at[0, j, dst], loc.at[9]).start()
            send(w.at[:, col(2 * j + other)], wp.at[1, j, dst], wsd.at[0], wrv.at[0], partner)
        return carry

    for k, (w, buf) in enumerate(((gw, wg), (uw, wu), (dw, wd))):
        local(10 + k, w.at[0], buf.at[0])

    def swap_expert():
        for k, (w, buf) in enumerate(((gw, wg), (uw, wu), (dw, wd))):
            send(w.at[0], buf.at[1], wsd.at[1 + k], wrv.at[1 + k], partner)

    lane = lane_iota((128, 128))
    sub = row_iota((128, 128))
    for cp in small:
        cp.wait()
    idr = ids[...].astype(F32)
    rows_e = row_iota((NSP, 128)).astype(F32)
    hot = [(idr[k : k + 1, :] == rows_e).astype(F32) for k in range(2)]
    upper = (sub < lane).astype(F32).astype(BF16)
    before = dot((hot[0] + hot[1]).astype(BF16), upper, 1, 0)
    pos = [
        idr[k : k + 1, :] * float(CAP) + jnp.sum(before * hot[k], axis=0, keepdims=True) for k in range(2)
    ]
    rows_s = row_iota((CAP * NSP, 128)).astype(F32)
    dmat[...] = ((pos[0] == rows_s).astype(F32) + (pos[1] == rows_s).astype(F32)).astype(BF16)
    posc = jnp.where(
        sub == 0, pos[0],
        jnp.where(sub == 1, pos[1], jnp.where(sub == 2, gates[0:1, :], jnp.where(sub == 3, gates[1:2, :], 0.0))),
    ).T
    gat[...] = posc
    lanes_s = lane_iota((128, CAP * NSP)).astype(F32)
    for k in range(2):
        pmat[k] = (posc[:, k : k + 1] == lanes_s).astype(F32).astype(BF16)
    gain_rows = jnp.where(
        sub == 0, hgain[0:1, :], jnp.where(sub == 1, hgain[1:2, :], jnp.where(sub == 2, g1[pl.ds(own, 1), :], 0.0))
    )
    cols[...] = gain_rows.T
    tokcp.wait()
    tokt[...] = tokraw[...].astype(F32).T

    low = lane < 64

    def queries(k):
        for r in (1, 3, 2):
            wait(qraw.at[r, q_parts[k]], qrv.at[r - 1, k])
        for r in range(NX):
            at = pl.ds(r * 128, 128)
            if k == 0:
                narrow = qraw[r, 0]
                qs[0, at, :] = jnp.where(low, narrow, jnp.zeros_like(narrow))
                qs[1, at, :] = jnp.where(low, jnp.zeros_like(narrow), narrow)
            else:
                qs[2, at, :] = qraw[r, 1]
                qs[3, at, :] = qraw[r, 2]

    def attend(group, slots, start=False):
        for m in (2 * group, 2 * group + 1):
            k_at = 0 if group == 0 else m
            v_at = 1 if group == 0 else 4
            query = qs[m]
            scores = [dot(kv[s, k_at], query, 1, 1) for s in slots]
            top = functools.reduce(jnp.maximum, [jnp.max(s, axis=0, keepdims=True) for s in scores])
            if not start:
                old = ml[m : m + 1, :]
                top = jnp.maximum(old, top)
            expo = [jnp.exp2((s - top) * SCALES[group]) for s in scores]
            total = functools.reduce(jnp.add, [jnp.sum(e, axis=0, keepdims=True) for e in expo])
            numer = functools.reduce(
                jnp.add, [dot(kv[s, v_at], e.astype(BF16), 0, 0) for s, e in zip(slots, expo)]
            )
            if start:
                acc[m] = numer
                ml[4 + m : 5 + m, :] = total
            else:
                shrink = jnp.exp2((old - top) * SCALES[group])
                acc[m] = acc[m] * shrink + numer
                ml[4 + m : 5 + m, :] = ml[4 + m : 5 + m, :] * shrink + total
            ml[m : m + 1, :] = top

    def arrive(d, group):
        for piece in ((0, 1), (2, 3, 4))[group]:
            kv_wait(d, piece)
            if d < 3 or group == 0:
                kv_send(0, d, piece, d, d + 1)
            kv_wait(4 + d, piece)
            if d < 3:
                kv_send(1, d, piece, 4 + d, 5 + d)
            elif group == 1:
                kv_send(1, d, piece, 7, 4)

    def far(group):
        for piece in ((0, 1), (2, 3, 4))[group]:
            kv_wait(4, piece)

    def share(group):
        for r in (2, 1, 3):
            at = pl.ds(r * 128, 128)
            for i in range(2):
                osend[r - 1, 2 * group + i] = acc[2 * group + i, :, at].astype(BF16)
            dev = (z, lax.rem(x + r, NX), y, c)
            pair = pl.ds(2 * group, 2)
            send(
                osend.at[r - 1, pair], orecv.at[r - 1, pair], osd.at[r - 1, group], orv.at[r - 1, group], dev
            )
            if group == 1:
                ssend[r - 1] = ml[:, at]
                send(ssend.at[r - 1], srecv.at[r - 1], ssd.at[r - 1], srv.at[r - 1], dev)

    arrive(1, 0)
    relayed(0)
    relay(1)
    queries(0)
    arrive(1, 1)
    attend(0, (0,), True)
    arrive(2, 0)
    attend(0, (1, 5))
    relayed(1)
    relay(2)
    queries(1)
    arrive(2, 1)
    lax.fori_loop(0, NY, proj, 0)
    attend(1, (0,), True)
    arrive(3, 0)
    attend(1, (1, 5))
    relayed(2)
    arrive(3, 1)
    swap_expert()
    attend(0, (2, 6))
    attend(1, (2, 6))
    attend(0, (3, 7))
    far(0)
    attend(0, (4,))
    share(0)
    attend(1, (3, 7))
    far(1)
    attend(1, (4,))
    share(1)

    wait(wp.at[0], loc.at[9])
    wait(wp.at[1], wrv.at[0])

    def turn(j, carry):
        for s in range(2):
            wpt[j, :, pl.ds(s * 256, 256)] = wp[s, j].T
        return carry

    lax.fori_loop(0, NY, turn, 0)

    for r in (1, 3, 2):
        for k in range(2):
            wait(orecv.at[r - 1, pl.ds(2 * k, 2)], orv.at[r - 1, k])
        wait(srecv.at[r - 1], srv.at[r - 1])
    for g in range(2):
        means = []
        for i in range(2):
            m = 2 * g + i
            tops = [ml[m : m + 1, 0:128]] + [srecv[r, m : m + 1, :] for r in range(3)]
            sums = [ml[4 + m : 5 + m, 0:128]] + [srecv[r, 4 + m : 5 + m, :] for r in range(3)]
            nums = [acc[m, :, 0:128]] + [orecv[r, m].astype(F32) for r in range(3)]
            top = functools.reduce(jnp.maximum, tops)
            w = [jnp.exp2((t - top) * SCALES[g]) for t in tops]
            total = functools.reduce(jnp.add, [a * b for a, b in zip(w, sums)])
            numer = functools.reduce(jnp.add, [a * b for a, b in zip(w, nums)])
            means.append(numer * ((1.0 if i == 0 else lam[0:1, g : g + 1]) / total))
        diff = means[0] - means[1]
        scale = lax.rsqrt(jnp.mean(diff * diff, axis=0, keepdims=True) + EPS)
        heads[0, pl.ds(g * 128, 128), :] = (diff * scale * cols[:, g : g + 1]).astype(BF16)
    send(heads.at[0], heads.at[1], hsd.at[0], hrv.at[0], partner)
    wait(heads.at[1], hrv.at[0])

    both = jnp.concatenate([heads[0], heads[1]], axis=0)
    for r in (4, 3, 5, 2, 6, 1, 7):
        t = lax.rem(y + r, NY)
        rsend[r - 1] = dot(wpt[t], both, 1, 0).astype(BF16)
        send(rsend.at[r - 1], rrecv.at[r - 1], rsd.at[r - 1], rrv.at[r - 1], (z, x, t, c))
    zt = ALPHA * tokt[...] + dot(wpt[y], both, 1, 0)
    for r in (1, 7, 2, 6, 3, 5, 4):
        wait(rrecv.at[r - 1], rrv.at[r - 1])
        zt = zt + rrecv[r - 1].astype(F32)

    sub8 = row_iota((8, 128))

    def local_stats(mean, dev2):
        return jnp.where(sub8 == 0, mean, jnp.where(sub8 == 1, dev2, 0.0))

    mean = jnp.mean(zt, axis=0, keepdims=True)
    dev2 = jnp.sum(jnp.square(zt - mean), axis=0, keepdims=True)
    stat1[0] = local_stats(mean, dev2)
    order = [(dy, dc) for dy in (4, 3, 5, 2, 6, 1, 7, 0) for dc in (1, 0) if dy or dc]
    for dy, dc in order:
        s = 2 * dy + dc
        send(
            stat1.at[0], stat1.at[s], s1s.at[s - 1], s1r.at[s - 1],
            (z, x, lax.rem(y + dy, NY), c if dc == 0 else other),
        )
    for s in range(1, 16):
        wait(stat1.at[s], s1r.at[s - 1])
    total = functools.reduce(jnp.add, [stat1[s] for s in range(16)])
    mean = total[0:1, :] * (1.0 / 16)
    spread = total[1:2, :] + 128.0 * functools.reduce(
        jnp.add, [jnp.square(stat1[s, 0:1, :] - mean) for s in range(16)]
    )
    scale = lax.rsqrt(spread * (1.0 / 2048) + EPS)
    normed = ((zt - mean) * scale * cols[:, 2:3]).astype(BF16)

    disp[...] = dot(dmat[...], normed, 1, 1).astype(BF16)

    def unit(j):
        return pl.ds(pl.multiple_of(j * CAP, CAP), CAP)

    arrive_at = unit(c * 16 + lax.rem(me, 16))

    def dispatch(j, carry):
        t = lax.rem(me + j, NSP)
        send(disp.at[unit(t)], xg.at[0, arrive_at], dps.at[0], dpr.at[0], (t // NX, lax.rem(t, NX), y, half))
        return carry

    lax.fori_loop(1, NSP, dispatch, 0)

    @pl.when(half == c)
    def _():
        xg[0, arrive_at, :] = disp[unit(me), :]

    @pl.when(half != c)
    def _():
        send(disp.at[unit(me)], xg.at[0, arrive_at], dps.at[0], dpr.at[0], partner)

    mixed[...] = normed.astype(F32).T * ALPHA
    for k, buf in enumerate((wg, wu, wd)):
        wait(buf.at[0], loc.at[10 + k])
        wait(buf.at[1], wrv.at[1 + k])

    def wait_units(ref, sem):
        @pl.when(half == c)
        def _():
            wait(ref.at[pl.ds(0, 496)], sem)

        @pl.when(half != c)
        def _():
            wait(ref, sem)

    wait_units(xg.at[0], dpr.at[0])

    def piece_of(h, k):
        return pl.ds(k * 256 + h * 128, 128)

    def xg_send(d, step, h, k, src_slot, dst_slot):
        send(
            xg.at[src_slot, piece_of(h, k)], xg.at[dst_slot, piece_of(h, k)], xgs.at[d, step, 2 * h + k],
            xgr.at[dst_slot, 2 * h + k], (z, x, (yp, ym)[d], c),
        )

    def xg_wait(slot, h, k):
        wait(xg.at[slot, piece_of(h, k)], xgr.at[slot, 2 * h + k])

    def xg_arrive(d, h, k):
        xg_wait(d, h, k)
        if d < 3 or k == 0:
            xg_send(0, d, h, k, d, d + 1)
        xg_wait(4 + d, h, k)
        if d < 3:
            xg_send(1, d, h, k, 4 + d, 5 + d)
        elif k == 1:
            xg_send(1, d, h, k, 7, 4)

    def slot_y(slot):
        away = NY - slot if slot <= 4 else slot - 4
        return lax.rem(y + away, NY)

    def absorb(slot, h, start=False):
        at = pl.ds(pl.multiple_of(slot_y(slot) * 256, 256), 256)
        rows_in = jnp.concatenate([xg[slot, piece_of(h, 0), :], xg[slot, piece_of(h, 1), :]], axis=1)
        for s in range(2):
            for w, a in ((wg, accg), (wu, accu)):
                value = dot(rows_in, w[s, at, :], 1, 0)
                a[h, s] = value if start else a[h, s] + value

    for h in (0, 1):
        for k in (0, 1):
            xg_send(0, 0, h, k, 0, 1)
            xg_send(1, 0, h, k, 0, 5)
    for h in (0, 1):
        absorb(0, h, True)
    for d in (1, 2, 3):
        for h in (0, 1):
            for k in (0, 1):
                xg_arrive(d, h, k)
            absorb(d, h)
            absorb(4 + d, h)

    def produce(h, r):
        at = pl.ds(pl.multiple_of(lax.rem(y + r, NY) * 256, 256), 256)
        part[h, r] = dot(act[h, 0], wd[0, :, at], 1, 0) + dot(act[h, 1], wd[1, :, at], 1, 0)

    def away(d, k, step):
        return (4 - k - step) if d == 0 else (NY - 3 - k + step) % NY

    def length(d, k):
        return 4 - k if d == 0 else 3 + k

    def pass_on(d, h, k, step):
        value = part[h, away(d, k, step), :, k * 128 : k * 128 + 128]
        p = 2 * h + k
        if step:
            wait(drecv.at[d, p, step - 1], ddr.at[d, p, step - 1])
            value = value + drecv[d, p, step - 1].astype(F32)
        dsend[d, p, step] = value.astype(BF16)
        send(
            dsend.at[d, p, step], drecv.at[d, p, step], dds.at[d, p, step], ddr.at[d, p, step],
            (z, x, (yp, ym)[d], c),
        )

    for h in (0, 1):
        for k in (0, 1):
            xg_wait(4, h, k)
        absorb(4, h)
        for s in range(2):
            g = accg[h, s]
            act[h, s] = (g / (1.0 + jnp.exp(-g)) * accu[h, s]).astype(BF16)
        produce(h, 4)
        pass_on(0, h, 0, 0)
        pass_on(1, h, 1, 0)
        produce(h, 3)
        pass_on(0, h, 1, 0)
        produce(h, 5)
        pass_on(1, h, 0, 0)
        for r in (2, 6, 1, 7, 0):
            produce(h, r)
    for step in (1, 2, 3):
        for h in (0, 1):
            for d, k in ((0, 0), (1, 1), (0, 1), (1, 0)):
                if step < length(d, k):
                    pass_on(d, h, k, step)

    ret_at = unit(me)

    def give_back(i, carry):
        t = c * 16 + i
        for k in range(2):
            @pl.when(jnp.logical_or(t != me, c != k))
            def _():
                send(eo.at[k, unit(i)], ret.at[ret_at], rts.at[0], rtr.at[0], (t // NX, lax.rem(t, NX), y, k))
        return carry

    for h in (0, 1):
        for k in (0, 1):
            value = part[h, 0, :, k * 128 : k * 128 + 128]
            for d in range(2):
                last, p = length(d, k) - 1, 2 * h + k
                wait(drecv.at[d, p, last], ddr.at[d, p, last])
                value = value + drecv[d, p, last].astype(F32)
            eo[k, pl.ds(h * 128, 128), :] = value.astype(BF16)
        lax.fori_loop(8 * h, 8 * h + 8, give_back, 0)

    @pl.when(half == c)
    def _():
        ret[ret_at, :] = eo[c, unit(lax.rem(me, 16)), :]

    wait_units(ret, rtr.at[0])

    zz = mixed[...]
    for k in range(2):
        zz = zz + gat[:, 2 + k : 3 + k] * dot(pmat[k], ret[...], 1, 0)

    mean = jnp.mean(zz, axis=1, keepdims=True)
    dev = zz - mean
    dev2 = jnp.sum(dev * dev, axis=1, keepdims=True)
    fin[0] = dev.astype(BF16)
    packed = jnp.where(lane == 0, mean, jnp.where(lane == 1, dev2, 0.0)).T
    stat2[0] = packed[0:8, :]
    send(fin.at[0], fin.at[1], fns.at[0], fnr.at[0], partner)
    for dy, dc in order:
        s = 2 * dy + dc
        dev_id = (z, x, lax.rem(y + dy, NY), c if dc == 0 else other)
        send(stat2.at[0], stat2.at[s], s2s.at[s - 1], s2r.at[s - 1], dev_id)
    for dy in (4, 3, 5, 2, 6, 1, 7):
        send(fin.at[0], fin.at[2 * dy], fns.at[2 * dy - 1], fnr.at[2 * dy - 1], (z, x, lax.rem(y + dy, NY), c))
    for s in range(1, 16):
        wait(stat2.at[s], s2r.at[s - 1])
    total = functools.reduce(jnp.add, [stat2[s] for s in range(16)])
    mean = total[0:1, :] * (1.0 / 16)
    spread = total[1:2, :] + 128.0 * functools.reduce(
        jnp.add, [jnp.square(stat2[s, 0:1, :] - mean) for s in range(16)]
    )
    scale = lax.rsqrt(spread * (1.0 / 2048) + EPS)
    table = jnp.where(sub == 16, scale, 0.0)
    for s in range(16):
        table = jnp.where(sub == s, stat2[s, 0:1, :] - mean, table)
    table = table.T

    def finish(dy, dc):
        s = 2 * dy + dc
        j = 2 * lax.rem(y + NY - dy, NY) + (c if dc == 0 else other)
        value = (fin[s].astype(F32) + table[:, s : s + 1]) * table[:, 16:17] * g2[pl.ds(j, 1), :]
        outb[s] = value.astype(BF16)
        pltpu.make_async_copy(outb.at[s], out.at[:, col(j)], oud.at[s]).start()

    finish(0, 0)
    wait(fin.at[1], fnr.at[0])
    finish(0, 1)
    arrivals = (1, 7, 2, 6, 3, 5, 4)
    for i, dy in enumerate(arrivals):
        wait(fin.at[2 * dy], fnr.at[2 * dy - 1])
        send(fin.at[2 * dy], fin.at[2 * dy + 1], fns.at[2 * dy], fnr.at[2 * dy], partner)
        finish(dy, 0)
        if i:
            before_dy = arrivals[i - 1]
            wait(fin.at[2 * before_dy + 1], fnr.at[2 * before_dy])
            finish(before_dy, 1)
    wait(fin.at[9], fnr.at[8])
    finish(4, 1)

    for step in range(4):
        for d in range(2):
            for piece in range(5):
                if step < 3 or (piece >= 2) == d:
                    wait(kv.at[0, piece], kvs.at[d, step, piece])
            for p in range(4):
                if step < 3 or p % 2 == d:
                    wait(xg.at[0, pl.ds(0, 128)], xgs.at[d, step, p])
                if step < length(d, p % 2):
                    wait(dsend.at[d, p, step], dds.at[d, p, step])
    for r in range(3):
        for k in range(2):
            wait(qraw.at[0, q_parts[k]], qsd.at[r, k])
            wait(osend.at[r, pl.ds(2 * k, 2)], osd.at[r, k])
        wait(ssend.at[r], ssd.at[r])
    wait(wp.at[0], wsd.at[0])
    for k, buf in enumerate((wg, wu, wd)):
        wait(buf.at[0], wsd.at[1 + k])
    wait(heads.at[0], hsd.at[0])
    for r in range(7):
        wait(rsend.at[r], rsd.at[r])
    for s in range(15):
        wait(stat1.at[0], s1s.at[s])
        wait(stat2.at[0], s2s.at[s])
        wait(fin.at[0], fns.at[s])
    wait_units(disp, dps.at[0])
    wait_units(ret, rts.at[0])
    for s in range(16):
        wait(outb.at[s], oud.at[s])


def on_device(
    tokens, query_narrow, key_narrow, value_narrow, query_broad, key_broad, value_broad, mix_lambda,
    head_gain, proj_narrow, proj_broad, gain_one, gain_two, expert_ids, expert_gates,
    gate_weight, up_weight, down_weight,
):
    memory = pl.BlockSpec(memory_space=pltpu.HBM)
    dma = pltpu.SemaphoreType.DMA
    bf = lambda *s: pltpu.VMEM(s, BF16)
    fl = lambda *s: pltpu.VMEM(s, F32)
    scratch = [
        bf(8, 5, 128, 128), bf(4, 3, 128, 128), bf(4, 512, 128), fl(4, 128, 512), fl(8, 512),
        bf(3, 4, 128, 128), bf(3, 4, 128, 128), fl(3, 8, 128), fl(3, 8, 128),
        bf(2, 8, 256, 128), bf(8, 128, 512), bf(128, 128), fl(128, 128),
        fl(128, 128), bf(512, 128), bf(2, 128, 512), fl(128, 128),
        bf(2, 256, 128), bf(7, 128, 128), bf(7, 128, 128), fl(16, 8, 128),
        fl(128, 128), bf(512, 128), bf(8, 512, 128),
        bf(2, 2048, 256), bf(2, 2048, 256), bf(2, 256, 2048),
        fl(2, 2, 128, 256), fl(2, 2, 128, 256), bf(2, 2, 128, 256), fl(2, 8, 128, 256),
        bf(2, 4, 4, 128, 128), bf(2, 4, 4, 128, 128),
        bf(512, 128), bf(2, 256, 128), bf(16, 128, 128), fl(16, 8, 128),
        fl(1, 2), pltpu.VMEM((2, 128), jnp.int32), fl(2, 128), fl(2, 128), fl(16, 128), fl(16, 128),
        bf(16, 128, 128),
        dma((13,)), dma((2, 4, 5)), dma((8, 5)), dma((3, 2)), dma((3, 2)), dma((4,)), dma((4,)),
        dma((3, 2)), dma((3, 2)), dma((3,)), dma((3,)), dma((1,)), dma((1,)), dma((7,)), dma((7,)),
        dma((15,)), dma((15,)), dma((1,)), dma((1,)), dma((2, 4, 4)), dma((8, 4)),
        dma((2, 4, 4)), dma((2, 4, 4)), dma((1,)), dma((1,)), dma((15,)), dma((15,)), dma((15,)), dma((15,)),
        dma((6,)), pltpu.SemaphoreType.REGULAR((3,)), dma((16,)),
    ]
    return pl.pallas_call(
        kernel,
        out_shape=jax.ShapeDtypeStruct((128, 2048), BF16),
        in_specs=[memory] * 18,
        out_specs=memory,
        scratch_shapes=scratch,
        compiler_params=pltpu.CompilerParams(
            collective_id=0, has_side_effects=True, vmem_limit_bytes=60 * 1024 * 1024
        ),
        name="layer",
    )(
        mix_lambda.T, expert_ids.T, expert_gates.T, head_gain, gain_one.reshape(16, 128), gain_two.reshape(16, 128),
        tokens, query_narrow, key_narrow, value_narrow, query_broad, key_broad, value_broad,
        proj_narrow, proj_broad, gate_weight, up_weight, down_weight,
    )


def solution(mesh):
    finer = Mesh(mesh.devices.reshape(NZ, NX, NY, 2), ("z", "x", "y", "c"))
    sp, tp = ("z", "x"), ("y", "c")
    return jax.shard_map(
        on_device,
        mesh=finer,
        in_specs=(
            P(sp, None), P(sp, tp), P(sp, tp), P(sp, tp), P(sp, tp), P(sp, tp), P(sp, tp), P(None, tp),
            P(), P(tp, None), P(tp, None), P(), P(), P(sp, None), P(sp, None),
            P(sp, None, tp), P(sp, None, tp), P(sp, tp, None),
        ),
        out_specs=P(sp, None),
        check_vma=False,
    )
```

```python
import functools

import jax
import jax.numpy as jnp
from jax import lax
from jax.experimental import pallas as pl
from jax.experimental.pallas import tpu as pltpu
from jax.sharding import Mesh
from jax.sharding import PartitionSpec as P

MESH = pl.DeviceIdType.MESH
NZ, NX, NY = 8, 4, 8
NSP = NZ * NX
CAP = 16
F32, BF16 = jnp.float32, jnp.bfloat16
ALPHA = 8.0**0.25
EPS = 1e-05
LOG2E = 1.4426950408889634
SCALES = (64**-0.5 * LOG2E, 128**-0.5 * LOG2E)


def dot(a, b, ca, cb):
    return lax.dot_general(a, b, (((ca,), (cb,)), ((), ())), preferred_element_type=F32)


def wait(ref, sem):
    pltpu.make_async_copy(ref, ref, sem).wait()


def send(src, dst, send_sem, recv_sem, dev):
    pltpu.make_async_remote_copy(
        src_ref=src, dst_ref=dst, send_sem=send_sem, recv_sem=recv_sem, device_id=dev, device_id_type=MESH
    ).start()


def row_iota(shape):
    return lax.broadcasted_iota(jnp.int32, shape, 0)


def lane_iota(shape):
    return lax.broadcasted_iota(jnp.int32, shape, 1)


def kernel(
    lam_in, ids_in, gates_in, hgain_in, g1_in, g2_in, tok, qn, kn, vn, qb, kb, vb, pn, pb, gw, uw, dw,
    out,
    kv, qraw, qs, acc, ml, osend, orecv, ssend, srecv, wp, wpt, tokraw, tokt, cols, dmat, pmat, gat,
    heads, rsend, rrecv, stat1, mixed, disp, xg, wg, wu, wd, accg, accu, act, part, dsend, drecv,
    ret, eo, fin, stat2, lam, ids, gates, hgain, g1, g2, outb, blocks, gsum, tdisp, sx,
    loc, kvs, kvr, qsd, qrv, wsd, wrv, osd, orv, ssd, srv, hsd, hrv, rsd, rrv, s1s, s1r, dps, dpr,
    xgs, xgr, dds, ddr, rts, rtr, fns, fnr, s2s, s2r, smalls, ysem, oud, tds, tdr,
):
    z, x, y, c = (lax.axis_index(n) for n in ("z", "x", "y", "c"))
    me = z * NX + x
    own = 2 * y + c
    other = 1 - c
    half = me // 16
    zp, zm = lax.rem(z + 1, NZ), lax.rem(z + NZ - 1, NZ)
    yp, ym = lax.rem(y + 1, NY), lax.rem(y + NY - 1, NY)
    partner = (z, x, y, other)

    def col(j):
        return pl.ds(pl.multiple_of(j * 128, 128), 128)

    def local(i, src, dst):
        cp = pltpu.make_async_copy(src, dst, loc.at[i])
        cp.start()
        return cp

    first = [
        local(0, kn, kv.at[0, 0]), local(1, vn, kv.at[0, 1]),
        local(2, kb.at[:, pl.ds(0, 128)], kv.at[0, 2]), local(3, kb.at[:, pl.ds(128, 128)], kv.at[0, 3]),
        local(4, vb, kv.at[0, 4]),
        local(5, qn, qraw.at[0, 0]), local(6, qb.at[:, pl.ds(0, 128)], qraw.at[0, 1]),
        local(7, qb.at[:, pl.ds(128, 128)], qraw.at[0, 2]),
    ]
    tokcp = local(8, tok.at[:, col(own)], tokraw)
    small = []
    for i, (src, dst) in enumerate(
        ((ids_in, ids), (gates_in, gates), (hgain_in, hgain), (g1_in, g1), (g2_in, g2), (lam_in, lam))
    ):
        small.append(pltpu.make_async_copy(src, dst, smalls.at[i]))
        small[-1].start()

    barrier = pltpu.get_barrier_semaphore()
    sides_y = ((z, x, yp, c), (z, x, ym, c))
    for dev in [(zp, x, y, c), (zm, x, y, c), partner, *sides_y] + [
        (z, lax.rem(x + r, NX), y, c) for r in range(1, NX)
    ]:
        pl.semaphore_signal(barrier, inc=1, device_id=dev, device_id_type=MESH)
    pl.semaphore_wait(barrier, 8)

    def relay(k):
        for dev in sides_y:
            pl.semaphore_signal(ysem.at[k], inc=1, device_id=dev, device_id_type=MESH)

    def relayed(k):
        pl.semaphore_wait(ysem.at[k], 2)

    for cp in first:
        cp.wait()
    def kv_send(d, step, piece, src_slot, dst_slot):
        send(
            kv.at[src_slot, piece], kv.at[dst_slot, piece], kvs.at[d, step, piece], kvr.at[dst_slot, piece],
            ((zp, zm)[d], x, y, c),
        )

    def kv_wait(slot, piece):
        wait(kv.at[slot, piece], kvr.at[slot, piece])

    for piece in range(5):
        kv_send(0, 0, piece, 0, 1)
        kv_send(1, 0, piece, 0, 5)
    q_parts = (pl.ds(0, 1), pl.ds(1, 2))
    for k in range(2):
        for r in (2, 1, 3):
            send(
                qraw.at[0, q_parts[k]], qraw.at[r, q_parts[k]], qsd.at[r - 1, k], qrv.at[r - 1, k],
                (z, lax.rem(x + NX - r, NX), y, c),
            )
    relay(0)

    def proj(j, carry):
        for k, w in enumerate((pn, pb)):
            dst = pl.ds(k * 128, 128)
            pltpu.make_async_copy(w.at[:, col(2 * j + c)], wp.at[0, j, dst], loc.at[9]).start()
            send(w.at[:, col(2 * j + other)], wp.at[1, j, dst], wsd.at[0], wrv.at[0], partner)
        return carry

    for k, (w, buf) in enumerate(((gw, wg), (uw, wu), (dw, wd))):
        local(10 + k, w.at[0], buf.at[0])

    def swap_expert():
        for k, (w, buf) in enumerate(((gw, wg), (uw, wu), (dw, wd))):
            send(w.at[0], buf.at[1], wsd.at[1 + k], wrv.at[1 + k], partner)

    lane = lane_iota((128, 128))
    sub = row_iota((128, 128))
    for cp in small:
        cp.wait()
    idr = ids[...].astype(F32)
    rows_e = row_iota((NSP, 128)).astype(F32)
    hot = [(idr[k : k + 1, :] == rows_e).astype(F32) for k in range(2)]
    upper = (sub < lane).astype(F32).astype(BF16)
    before = dot((hot[0] + hot[1]).astype(BF16), upper, 1, 0)
    pos = [
        idr[k : k + 1, :] * float(CAP) + jnp.sum(before * hot[k], axis=0, keepdims=True) for k in range(2)
    ]
    rows_s = row_iota((CAP * NSP, 128)).astype(F32)
    dmat[...] = ((pos[0] == rows_s).astype(F32) + (pos[1] == rows_s).astype(F32)).astype(BF16)
    posc = jnp.where(
        sub == 0, pos[0],
        jnp.where(sub == 1, pos[1], jnp.where(sub == 2, gates[0:1, :], jnp.where(sub == 3, gates[1:2, :], 0.0))),
    ).T
    gat[...] = posc
    lanes_s = lane_iota((128, CAP * NSP)).astype(F32)
    for k in range(2):
        pmat[k] = (posc[:, k : k + 1] == lanes_s).astype(F32).astype(BF16)
    gain_rows = jnp.where(
        sub == 0, hgain[0:1, :], jnp.where(sub == 1, hgain[1:2, :], jnp.where(sub == 2, g1[pl.ds(own, 1), :], 0.0))
    )
    cols[...] = gain_rows.T
    tokcp.wait()
    tokt[...] = tokraw[...].astype(F32).T

    low = lane < 64

    def queries(k):
        for r in (1, 3, 2):
            wait(qraw.at[r, q_parts[k]], qrv.at[r - 1, k])
        for r in range(NX):
            at = pl.ds(r * 128, 128)
            if k == 0:
                narrow = qraw[r, 0]
                qs[0, at, :] = jnp.where(low, narrow, jnp.zeros_like(narrow))
                qs[1, at, :] = jnp.where(low, jnp.zeros_like(narrow), narrow)
            else:
                qs[2, at, :] = qraw[r, 1]
                qs[3, at, :] = qraw[r, 2]

    def attend(group, slots, start=False):
        v_at = 1 if group == 0 else 4
        turned = [kv[s, v_at].T for s in slots]
        for m in (2 * group, 2 * group + 1):
            k_at = 0 if group == 0 else m
            for at in [pl.ds(0, 512)] if len(slots) == 2 else [pl.ds(0, 256), pl.ds(256, 256)]:
                query = qs[m, at, :]
                scores = [dot(kv[s, k_at], query, 1, 1) for s in slots]
                top = functools.reduce(jnp.maximum, [jnp.max(s, axis=0, keepdims=True) for s in scores])
                if not start:
                    old = ml[m : m + 1, at]
                    top = jnp.maximum(old, top)
                expo = [jnp.exp2((s - top) * SCALES[group]) for s in scores]
                total = functools.reduce(jnp.add, [jnp.sum(e, axis=0, keepdims=True) for e in expo])
                numer = functools.reduce(jnp.add, [dot(v, e.astype(BF16), 1, 0) for v, e in zip(turned, expo)])
                if start:
                    acc[m, :, at] = numer
                    ml[4 + m : 5 + m, at] = total
                else:
                    shrink = jnp.exp2((old - top) * SCALES[group])
                    acc[m, :, at] = acc[m, :, at] * shrink + numer
                    ml[4 + m : 5 + m, at] = ml[4 + m : 5 + m, at] * shrink + total
                ml[m : m + 1, at] = top

    def arrive(d, group):
        for piece in ((0, 1), (2, 3, 4))[group]:
            kv_wait(d, piece)
            if d < 3 or group == 0:
                kv_send(0, d, piece, d, d + 1)
            kv_wait(4 + d, piece)
            if d < 3:
                kv_send(1, d, piece, 4 + d, 5 + d)
            elif group == 1:
                kv_send(1, d, piece, 7, 4)

    def far(group):
        for piece in ((0, 1), (2, 3, 4))[group]:
            kv_wait(4, piece)

    def share(group):
        for r in (2, 1, 3):
            at = pl.ds(r * 128, 128)
            for i in range(2):
                osend[r - 1, 2 * group + i] = acc[2 * group + i, :, at].astype(BF16)
            dev = (z, lax.rem(x + r, NX), y, c)
            pair = pl.ds(2 * group, 2)
            send(
                osend.at[r - 1, pair], orecv.at[r - 1, pair], osd.at[r - 1, group], orv.at[r - 1, group], dev
            )
            if group == 1:
                ssend[r - 1] = ml[:, at]
                send(ssend.at[r - 1], srecv.at[r - 1], ssd.at[r - 1], srv.at[r - 1], dev)

    arrive(1, 0)
    relayed(0)
    relay(1)
    queries(0)
    arrive(1, 1)
    attend(0, (0,), True)
    arrive(2, 0)
    attend(0, (1, 5))
    relayed(1)
    relay(2)
    queries(1)
    arrive(2, 1)
    lax.fori_loop(0, NY, proj, 0)
    attend(1, (0,), True)
    arrive(3, 0)
    attend(1, (1, 5))
    relayed(2)
    arrive(3, 1)
    swap_expert()
    attend(0, (2, 6))
    attend(1, (2, 6))
    attend(0, (3, 7))
    far(0)
    attend(0, (4,))
    share(0)
    attend(1, (3, 7))
    far(1)
    attend(1, (4,))
    share(1)

    wait(wp.at[0], loc.at[9])
    wait(wp.at[1], wrv.at[0])

    def turn(j, carry):
        for s in range(2):
            wpt[j, :, pl.ds(s * 256, 256)] = wp[s, j].T
        return carry

    lax.fori_loop(0, NY, turn, 0)

    for r in (1, 3, 2):
        for k in range(2):
            wait(orecv.at[r - 1, pl.ds(2 * k, 2)], orv.at[r - 1, k])
        wait(srecv.at[r - 1], srv.at[r - 1])
    for g in range(2):
        means = []
        for i in range(2):
            m = 2 * g + i
            tops = [ml[m : m + 1, 0:128]] + [srecv[r, m : m + 1, :] for r in range(3)]
            sums = [ml[4 + m : 5 + m, 0:128]] + [srecv[r, 4 + m : 5 + m, :] for r in range(3)]
            nums = [acc[m, :, 0:128]] + [orecv[r, m].astype(F32) for r in range(3)]
            top = functools.reduce(jnp.maximum, tops)
            w = [jnp.exp2((t - top) * SCALES[g]) for t in tops]
            total = functools.reduce(jnp.add, [a * b for a, b in zip(w, sums)])
            numer = functools.reduce(jnp.add, [a * b for a, b in zip(w, nums)])
            means.append(numer * ((1.0 if i == 0 else lam[0:1, g : g + 1]) / total))
        diff = means[0] - means[1]
        scale = lax.rsqrt(jnp.mean(diff * diff, axis=0, keepdims=True) + EPS)
        heads[0, pl.ds(g * 128, 128), :] = (diff * scale * cols[:, g : g + 1]).astype(BF16)
    send(heads.at[0], heads.at[1], hsd.at[0], hrv.at[0], partner)
    wait(heads.at[1], hrv.at[0])

    both = jnp.concatenate([heads[0], heads[1]], axis=0)
    for r in (4, 3, 5, 2, 6, 1, 7):
        t = lax.rem(y + r, NY)
        rsend[r - 1] = dot(wpt[t], both, 1, 0).astype(BF16)
        send(rsend.at[r - 1], rrecv.at[r - 1], rsd.at[r - 1], rrv.at[r - 1], (z, x, t, c))
    zt = ALPHA * tokt[...] + dot(wpt[y], both, 1, 0)

    for k, buf in enumerate((wg, wu, wd)):
        wait(buf.at[0], loc.at[10 + k])
        wait(buf.at[1], wrv.at[1 + k])
    sub32 = row_iota((32, 128))
    for s in range(16):
        dy, dc = s // 2, s % 2
        j = 2 * lax.rem(y + NY - dy, NY) + (c if dc == 0 else other)
        gain = g1[pl.ds(j, 1), :]
        top = gain.astype(BF16).astype(F32)
        blocks[:, col(j)] = jnp.where(sub32 == s, top, jnp.where(sub32 == 16 + s, gain - top, 0.0)).astype(BF16)
    for k, w in enumerate((wg, wu)):
        for s in range(2):
            value = dot(blocks[...], w[s], 1, 0)
            value = value[0:16] + value[16:32]
            top = value.astype(BF16).astype(F32)
            gsum[k, s] = jnp.concatenate([top, top, value - top, jnp.zeros((80, 256), F32)], axis=0).astype(BF16)
    for r in (1, 7, 2, 6, 3, 5, 4):
        wait(rrecv.at[r - 1], rrv.at[r - 1])
        zt = zt + rrecv[r - 1].astype(F32)

    sub8 = row_iota((8, 128))

    def local_stats(mean, dev2):
        return jnp.where(sub8 == 0, mean, jnp.where(sub8 == 1, dev2, 0.0))

    mean = jnp.mean(zt, axis=0, keepdims=True)
    dev2 = jnp.sum(jnp.square(zt - mean), axis=0, keepdims=True)
    stat1[0] = local_stats(mean, dev2)
    order = [(dy, dc) for dy in (4, 3, 5, 2, 6, 1, 7, 0) for dc in (1, 0) if dy or dc]
    for dy, dc in order:
        s = 2 * dy + dc
        send(
            stat1.at[0], stat1.at[s], s1s.at[s - 1], s1r.at[s - 1],
            (z, x, lax.rem(y + dy, NY), c if dc == 0 else other),
        )
    raised = ((zt - mean) * cols[:, 2:3]).astype(BF16)
    disp[...] = dot(dmat[...], raised, 1, 1).astype(BF16)

    def unit(j):
        return pl.ds(pl.multiple_of(j * CAP, CAP), CAP)

    arrive_at = unit(c * 16 + lax.rem(me, 16))

    def dispatch(j, carry):
        t = lax.rem(me + j, NSP)
        send(disp.at[unit(t)], xg.at[0, arrive_at], dps.at[0], dpr.at[0], (t // NX, lax.rem(t, NX), y, half))
        return carry

    lax.fori_loop(1, NSP, dispatch, 0)

    @pl.when(half == c)
    def _():
        xg[0, arrive_at, :] = disp[unit(me), :]

    @pl.when(half != c)
    def _():
        send(disp.at[unit(me)], xg.at[0, arrive_at], dps.at[0], dpr.at[0], partner)

    for s in range(1, 16):
        wait(stat1.at[s], s1r.at[s - 1])
    total = functools.reduce(jnp.add, [stat1[s] for s in range(16)])
    mean = total[0:1, :] * (1.0 / 16)
    spread = total[1:2, :] + 128.0 * functools.reduce(
        jnp.add, [jnp.square(stat1[s, 0:1, :] - mean) for s in range(16)]
    )
    scale = lax.rsqrt(spread * (1.0 / 2048) + EPS)
    sub16 = row_iota((16, 128))
    shift = jnp.zeros((16, 128), F32)
    for s in range(16):
        shift = jnp.where(sub16 == s, stat1[s, 0:1, :] - mean, shift)
    top = shift.astype(BF16).astype(F32)
    one = scale.astype(BF16).astype(F32)
    two = (scale - one).astype(BF16).astype(F32)
    parts = jnp.where(
        sub16 == 0, one, jnp.where(sub16 == 1, two, jnp.where(sub16 == 2, scale - one - two, 0.0))
    )
    table = jnp.concatenate([top, shift - top, top, parts, jnp.zeros((64, 128), F32)], axis=0).astype(BF16)
    tdisp[...] = dot(dmat[...], table, 1, 1).astype(BF16)

    def follow(j, carry):
        t = lax.rem(me + j, NSP)
        send(
            tdisp.at[unit(t)], sx.at[unit(lax.rem(me, 16))], tds.at[0], tdr.at[0], (t // NX, lax.rem(t, NX), y, c)
        )
        return carry

    @pl.when(half == c)
    def _():
        lax.fori_loop(1, NSP, follow, 0)
        sx[unit(lax.rem(me, 16)), :] = tdisp[unit(me), :]

    mixed[...] = ((zt - mean) * scale * cols[:, 2:3]).astype(BF16).astype(F32).T * ALPHA

    def wait_units(ref, sem):
        @pl.when(half == c)
        def _():
            wait(ref.at[pl.ds(0, 496)], sem)

        @pl.when(half != c)
        def _():
            wait(ref, sem)

    wait_units(xg.at[0], dpr.at[0])

    def piece_of(h, k):
        return pl.ds(k * 256 + h * 128, 128)

    def xg_send(d, step, h, k, src_slot, dst_slot):
        send(
            xg.at[src_slot, piece_of(h, k)], xg.at[dst_slot, piece_of(h, k)], xgs.at[d, step, 2 * h + k],
            xgr.at[dst_slot, 2 * h + k], (z, x, (yp, ym)[d], c),
        )

    def xg_wait(slot, h, k):
        wait(xg.at[slot, piece_of(h, k)], xgr.at[slot, 2 * h + k])

    def xg_arrive(d, h, k):
        xg_wait(d, h, k)
        if d < 3 or k == 0:
            xg_send(0, d, h, k, d, d + 1)
        xg_wait(4 + d, h, k)
        if d < 3:
            xg_send(1, d, h, k, 4 + d, 5 + d)
        elif k == 1:
            xg_send(1, d, h, k, 7, 4)

    def slot_y(slot):
        away = NY - slot if slot <= 4 else slot - 4
        return lax.rem(y + away, NY)

    def absorb(slot, h, start=False):
        at = pl.ds(pl.multiple_of(slot_y(slot) * 256, 256), 256)
        rows_in = jnp.concatenate([xg[slot, piece_of(h, 0), :], xg[slot, piece_of(h, 1), :]], axis=1)
        for s in range(2):
            for w, a in ((wg, accg), (wu, accu)):
                value = dot(rows_in, w[s, at, :], 1, 0)
                a[h, s] = value if start else a[h, s] + value

    for h in (0, 1):
        for k in (0, 1):
            xg_send(0, 0, h, k, 0, 1)
            xg_send(1, 0, h, k, 0, 5)
    for h in (0, 1):
        absorb(0, h, True)
    for d in (1, 2, 3):
        for h in (0, 1):
            for k in (0, 1):
                xg_arrive(d, h, k)
            absorb(d, h)
            absorb(4 + d, h)

    def produce(h, r):
        at = pl.ds(pl.multiple_of(lax.rem(y + r, NY) * 256, 256), 256)
        part[h, r] = dot(act[h, 0], wd[0, :, at], 1, 0) + dot(act[h, 1], wd[1, :, at], 1, 0)

    def away(d, k, step):
        return (4 - k - step) if d == 0 else (NY - 3 - k + step) % NY

    def length(d, k):
        return 4 - k if d == 0 else 3 + k

    def pass_on(d, h, k, step):
        value = part[h, away(d, k, step), :, k * 128 : k * 128 + 128]
        p = 2 * h + k
        if step:
            wait(drecv.at[d, p, step - 1], ddr.at[d, p, step - 1])
            value = value + drecv[d, p, step - 1].astype(F32)
        dsend[d, p, step] = value.astype(BF16)
        send(
            dsend.at[d, p, step], drecv.at[d, p, step], dds.at[d, p, step], ddr.at[d, p, step],
            (z, x, (yp, ym)[d], c),
        )

    @pl.when(half == c)
    def _():
        wait(sx.at[pl.ds(0, 240)], tdr.at[0])

    @pl.when(half != c)
    def _():
        wait(sx, tdr.at[0])

    for h in (0, 1):
        stat = sx[h * 128 : h * 128 + 128, :]
        scales = stat[:, 48:64].astype(F32)
        scales = scales[:, 0:1] + scales[:, 1:2] + scales[:, 2:3]
        shifts = [[dot(stat, gsum[k, s], 1, 0) for s in range(2)] for k in range(2)]
        for k in (0, 1):
            xg_wait(4, h, k)
        absorb(4, h)
        for s in range(2):
            g = (accg[h, s] + shifts[0][s]) * scales
            act[h, s] = (g / (1.0 + jnp.exp(-g)) * ((accu[h, s] + shifts[1][s]) * scales)).astype(BF16)
        produce(h, 4)
        pass_on(0, h, 0, 0)
        pass_on(1, h, 1, 0)
        produce(h, 3)
        pass_on(0, h, 1, 0)
        produce(h, 5)
        pass_on(1, h, 0, 0)
        for r in (2, 6, 1, 7, 0):
            produce(h, r)
    for step in (1, 2, 3):
        for h in (0, 1):
            for d, k in ((0, 0), (1, 1), (0, 1), (1, 0)):
                if step < length(d, k):
                    pass_on(d, h, k, step)

    ret_at = unit(me)

    def give_back(i, carry):
        t = c * 16 + i
        for k in range(2):
            @pl.when(jnp.logical_or(t != me, c != k))
            def _():
                send(eo.at[k, unit(i)], ret.at[ret_at], rts.at[0], rtr.at[0], (t // NX, lax.rem(t, NX), y, k))
        return carry

    for h in (0, 1):
        for k in (0, 1):
            value = part[h, 0, :, k * 128 : k * 128 + 128]
            for d in range(2):
                last, p = length(d, k) - 1, 2 * h + k
                wait(drecv.at[d, p, last], ddr.at[d, p, last])
                value = value + drecv[d, p, last].astype(F32)
            eo[k, pl.ds(h * 128, 128), :] = value.astype(BF16)
        lax.fori_loop(8 * h, 8 * h + 8, give_back, 0)

    @pl.when(half == c)
    def _():
        ret[ret_at, :] = eo[c, unit(lax.rem(me, 16)), :]

    wait_units(ret, rtr.at[0])

    zz = mixed[...]
    for k in range(2):
        zz = zz + gat[:, 2 + k : 3 + k] * dot(pmat[k], ret[...], 1, 0)

    mean = jnp.mean(zz, axis=1, keepdims=True)
    dev = zz - mean
    dev2 = jnp.sum(dev * dev, axis=1, keepdims=True)
    fin[0] = dev.astype(BF16)
    packed = jnp.where(lane == 0, mean, jnp.where(lane == 1, dev2, 0.0)).T
    stat2[0] = packed[0:8, :]
    send(fin.at[0], fin.at[1], fns.at[0], fnr.at[0], partner)
    for dy, dc in order:
        s = 2 * dy + dc
        dev_id = (z, x, lax.rem(y + dy, NY), c if dc == 0 else other)
        send(stat2.at[0], stat2.at[s], s2s.at[s - 1], s2r.at[s - 1], dev_id)
    for dy in (4, 3, 5, 2, 6, 1, 7):
        send(fin.at[0], fin.at[2 * dy], fns.at[2 * dy - 1], fnr.at[2 * dy - 1], (z, x, lax.rem(y + dy, NY), c))
    for s in range(1, 16):
        wait(stat2.at[s], s2r.at[s - 1])
    total = functools.reduce(jnp.add, [stat2[s] for s in range(16)])
    mean = total[0:1, :] * (1.0 / 16)
    spread = total[1:2, :] + 128.0 * functools.reduce(
        jnp.add, [jnp.square(stat2[s, 0:1, :] - mean) for s in range(16)]
    )
    scale = lax.rsqrt(spread * (1.0 / 2048) + EPS)
    table = jnp.where(sub == 16, scale, 0.0)
    for s in range(16):
        table = jnp.where(sub == s, stat2[s, 0:1, :] - mean, table)
    table = table.T

    def finish(dy, dc):
        s = 2 * dy + dc
        j = 2 * lax.rem(y + NY - dy, NY) + (c if dc == 0 else other)
        value = (fin[s].astype(F32) + table[:, s : s + 1]) * table[:, 16:17] * g2[pl.ds(j, 1), :]
        outb[s] = value.astype(BF16)
        pltpu.make_async_copy(outb.at[s], out.at[:, col(j)], oud.at[s]).start()

    finish(0, 0)
    wait(fin.at[1], fnr.at[0])
    finish(0, 1)
    arrivals = (1, 7, 2, 6, 3, 5, 4)
    for i, dy in enumerate(arrivals):
        wait(fin.at[2 * dy], fnr.at[2 * dy - 1])
        send(fin.at[2 * dy], fin.at[2 * dy + 1], fns.at[2 * dy], fnr.at[2 * dy], partner)
        finish(dy, 0)
        if i:
            before_dy = arrivals[i - 1]
            wait(fin.at[2 * before_dy + 1], fnr.at[2 * before_dy])
            finish(before_dy, 1)
    wait(fin.at[9], fnr.at[8])
    finish(4, 1)

    for step in range(4):
        for d in range(2):
            for piece in range(5):
                if step < 3 or (piece >= 2) == d:
                    wait(kv.at[0, piece], kvs.at[d, step, piece])
            for p in range(4):
                if step < 3 or p % 2 == d:
                    wait(xg.at[0, pl.ds(0, 128)], xgs.at[d, step, p])
                if step < length(d, p % 2):
                    wait(dsend.at[d, p, step], dds.at[d, p, step])
    for r in range(3):
        for k in range(2):
            wait(qraw.at[0, q_parts[k]], qsd.at[r, k])
            wait(osend.at[r, pl.ds(2 * k, 2)], osd.at[r, k])
        wait(ssend.at[r], ssd.at[r])
    wait(wp.at[0], wsd.at[0])
    for k, buf in enumerate((wg, wu, wd)):
        wait(buf.at[0], wsd.at[1 + k])
    wait(heads.at[0], hsd.at[0])
    for r in range(7):
        wait(rsend.at[r], rsd.at[r])
    for s in range(15):
        wait(stat1.at[0], s1s.at[s])
        wait(stat2.at[0], s2s.at[s])
        wait(fin.at[0], fns.at[s])
    wait_units(disp, dps.at[0])

    @pl.when(half == c)
    def _():
        wait(tdisp.at[pl.ds(0, 496)], tds.at[0])

    wait_units(ret, rts.at[0])
    for s in range(16):
        wait(outb.at[s], oud.at[s])


def on_device(
    tokens, query_narrow, key_narrow, value_narrow, query_broad, key_broad, value_broad, mix_lambda,
    head_gain, proj_narrow, proj_broad, gain_one, gain_two, expert_ids, expert_gates,
    gate_weight, up_weight, down_weight,
):
    memory = pl.BlockSpec(memory_space=pltpu.HBM)
    dma = pltpu.SemaphoreType.DMA
    bf = lambda *s: pltpu.VMEM(s, BF16)
    fl = lambda *s: pltpu.VMEM(s, F32)
    scratch = [
        bf(8, 5, 128, 128), bf(4, 3, 128, 128), bf(4, 512, 128), fl(4, 128, 512), fl(8, 512),
        bf(3, 4, 128, 128), bf(3, 4, 128, 128), fl(3, 8, 128), fl(3, 8, 128),
        bf(2, 8, 256, 128), bf(8, 128, 512), bf(128, 128), fl(128, 128),
        fl(128, 128), bf(512, 128), bf(2, 128, 512), fl(128, 128),
        bf(2, 256, 128), bf(7, 128, 128), bf(7, 128, 128), fl(16, 8, 128),
        fl(128, 128), bf(512, 128), bf(8, 512, 128),
        bf(2, 2048, 256), bf(2, 2048, 256), bf(2, 256, 2048),
        fl(2, 2, 128, 256), fl(2, 2, 128, 256), bf(2, 2, 128, 256), fl(2, 8, 128, 256),
        bf(2, 4, 4, 128, 128), bf(2, 4, 4, 128, 128),
        bf(512, 128), bf(2, 256, 128), bf(16, 128, 128), fl(16, 8, 128),
        fl(1, 2), pltpu.VMEM((2, 128), jnp.int32), fl(2, 128), fl(2, 128), fl(16, 128), fl(16, 128),
        bf(16, 128, 128), bf(32, 2048), bf(2, 2, 128, 256), bf(512, 128), bf(256, 128),
        dma((13,)), dma((2, 4, 5)), dma((8, 5)), dma((3, 2)), dma((3, 2)), dma((4,)), dma((4,)),
        dma((3, 2)), dma((3, 2)), dma((3,)), dma((3,)), dma((1,)), dma((1,)), dma((7,)), dma((7,)),
        dma((15,)), dma((15,)), dma((1,)), dma((1,)), dma((2, 4, 4)), dma((8, 4)),
        dma((2, 4, 4)), dma((2, 4, 4)), dma((1,)), dma((1,)), dma((15,)), dma((15,)), dma((15,)), dma((15,)),
        dma((6,)), pltpu.SemaphoreType.REGULAR((3,)), dma((16,)), dma((1,)), dma((1,)),
    ]
    return pl.pallas_call(
        kernel,
        out_shape=jax.ShapeDtypeStruct((128, 2048), BF16),
        in_specs=[memory] * 18,
        out_specs=memory,
        scratch_shapes=scratch,
        compiler_params=pltpu.CompilerParams(
            collective_id=0, has_side_effects=True, vmem_limit_bytes=60 * 1024 * 1024
        ),
        name="layer",
    )(
        mix_lambda.T, expert_ids.T, expert_gates.T, head_gain, gain_one.reshape(16, 128), gain_two.reshape(16, 128),
        tokens, query_narrow, key_narrow, value_narrow, query_broad, key_broad, value_broad,
        proj_narrow, proj_broad, gate_weight, up_weight, down_weight,
    )


def solution(mesh):
    finer = Mesh(mesh.devices.reshape(NZ, NX, NY, 2), ("z", "x", "y", "c"))
    sp, tp = ("z", "x"), ("y", "c")
    return jax.shard_map(
        on_device,
        mesh=finer,
        in_specs=(
            P(sp, None), P(sp, tp), P(sp, tp), P(sp, tp), P(sp, tp), P(sp, tp), P(sp, tp), P(None, tp),
            P(), P(tp, None), P(tp, None), P(), P(), P(sp, None), P(sp, None),
            P(sp, None, tp), P(sp, None, tp), P(sp, tp, None),
        ),
        out_specs=P(sp, None),
        check_vma=False,
    )
```

```python
import functools

import jax
import jax.numpy as jnp
from jax import lax
from jax.experimental import pallas as pl
from jax.experimental.pallas import tpu as pltpu
from jax.sharding import Mesh
from jax.sharding import PartitionSpec as P

MESH = pl.DeviceIdType.MESH
NZ, NX, NY = 8, 4, 8
NSP = NZ * NX
CAP = 16
F32, BF16 = jnp.float32, jnp.bfloat16
ALPHA = 8.0**0.25
EPS = 1e-05
LOG2E = 1.4426950408889634
SCALES = (64**-0.5 * LOG2E, 128**-0.5 * LOG2E)


def dot(a, b, ca, cb):
    return lax.dot_general(a, b, (((ca,), (cb,)), ((), ())), preferred_element_type=F32)


def wait(ref, sem):
    pltpu.make_async_copy(ref, ref, sem).wait()


def send(src, dst, send_sem, recv_sem, dev):
    pltpu.make_async_remote_copy(
        src_ref=src, dst_ref=dst, send_sem=send_sem, recv_sem=recv_sem, device_id=dev, device_id_type=MESH
    ).start()


def row_iota(shape):
    return lax.broadcasted_iota(jnp.int32, shape, 0)


def lane_iota(shape):
    return lax.broadcasted_iota(jnp.int32, shape, 1)


def kernel(
    lam_in, ids_in, gates_in, hgain_in, g1_in, g2_in, tok, qn, kn, vn, qb, kb, vb, pn, pb, gw, uw, dw,
    out,
    kv, qraw, qs, acc, ml, osend, orecv, ssend, srecv, wp, wpt, tokraw, tokt, cols, dmat, pmat, gat,
    heads, rsend, rrecv, stat1, mixed, disp, xg, wg, wu, wd, accg, accu, act, part, dsend, drecv,
    ret, eo, fin, stat2, lam, ids, gates, hgain, g1, g2, outb, blocks, gsum, tdisp, sx,
    loc, kvs, kvr, qsd, qrv, wsd, wrv, osd, orv, ssd, srv, hsd, hrv, rsd, rrv, s1s, s1r, dps, dpr,
    xgs, xgr, dds, ddr, rts, rtr, fns, fnr, s2s, s2r, smalls, ysem, oud, tds, tdr,
):
    z, x, y, c = (lax.axis_index(n) for n in ("z", "x", "y", "c"))
    me = z * NX + x
    own = 2 * y + c
    other = 1 - c
    half = me // 16
    zp, zm = lax.rem(z + 1, NZ), lax.rem(z + NZ - 1, NZ)
    yp, ym = lax.rem(y + 1, NY), lax.rem(y + NY - 1, NY)
    partner = (z, x, y, other)

    def col(j):
        return pl.ds(pl.multiple_of(j * 128, 128), 128)

    def local(i, src, dst):
        cp = pltpu.make_async_copy(src, dst, loc.at[i])
        cp.start()
        return cp

    first = [
        local(0, kn, kv.at[0, 0]), local(1, vn, kv.at[0, 1]),
        local(2, kb.at[:, pl.ds(0, 128)], kv.at[0, 2]), local(3, kb.at[:, pl.ds(128, 128)], kv.at[0, 3]),
        local(4, vb, kv.at[0, 4]),
        local(5, qn, qraw.at[0, 0]), local(6, qb.at[:, pl.ds(0, 128)], qraw.at[0, 1]),
        local(7, qb.at[:, pl.ds(128, 128)], qraw.at[0, 2]),
    ]
    tokcp = local(8, tok.at[:, col(own)], tokraw)
    small = []
    for i, (src, dst) in enumerate(
        ((ids_in, ids), (gates_in, gates), (hgain_in, hgain), (g1_in, g1), (g2_in, g2), (lam_in, lam))
    ):
        small.append(pltpu.make_async_copy(src, dst, smalls.at[i]))
        small[-1].start()

    barrier = pltpu.get_barrier_semaphore()
    sides_y = ((z, x, yp, c), (z, x, ym, c))
    for dev in [(zp, x, y, c), (zm, x, y, c), partner, *sides_y] + [
        (z, lax.rem(x + r, NX), y, c) for r in range(1, NX)
    ]:
        pl.semaphore_signal(barrier, inc=1, device_id=dev, device_id_type=MESH)
    pl.semaphore_wait(barrier, 8)

    def relay(k):
        for dev in sides_y:
            pl.semaphore_signal(ysem.at[k], inc=1, device_id=dev, device_id_type=MESH)

    def relayed(k):
        pl.semaphore_wait(ysem.at[k], 2)

    for cp in first:
        cp.wait()
    def kv_send(d, step, piece, src_slot, dst_slot):
        send(
            kv.at[src_slot, piece], kv.at[dst_slot, piece], kvs.at[d, step, piece], kvr.at[dst_slot, piece],
            ((zp, zm)[d], x, y, c),
        )

    def kv_wait(slot, piece):
        wait(kv.at[slot, piece], kvr.at[slot, piece])

    for piece in range(5):
        kv_send(0, 0, piece, 0, 1)
        kv_send(1, 0, piece, 0, 5)
    q_parts = (pl.ds(0, 1), pl.ds(1, 2))
    for k in range(2):
        for r in (2, 1, 3):
            send(
                qraw.at[0, q_parts[k]], qraw.at[r, q_parts[k]], qsd.at[r - 1, k], qrv.at[r - 1, k],
                (z, lax.rem(x + NX - r, NX), y, c),
            )
    relay(0)

    def proj(j, carry):
        for k, w in enumerate((pn, pb)):
            dst = pl.ds(k * 128, 128)
            pltpu.make_async_copy(w.at[:, col(2 * j + c)], wp.at[0, j, dst], loc.at[9]).start()
            send(w.at[:, col(2 * j + other)], wp.at[1, j, dst], wsd.at[0], wrv.at[0], partner)
        return carry

    for k, (w, buf) in enumerate(((gw, wg), (uw, wu), (dw, wd))):
        local(10 + k, w.at[0], buf.at[0])

    def swap_expert():
        for k, (w, buf) in enumerate(((gw, wg), (uw, wu), (dw, wd))):
            send(w.at[0], buf.at[1], wsd.at[1 + k], wrv.at[1 + k], partner)

    lane = lane_iota((128, 128))
    sub = row_iota((128, 128))
    for cp in small:
        cp.wait()
    idr = ids[...].astype(F32)
    rows_e = row_iota((NSP, 128)).astype(F32)
    hot = [(idr[k : k + 1, :] == rows_e).astype(F32) for k in range(2)]
    upper = (sub < lane).astype(F32).astype(BF16)
    before = dot((hot[0] + hot[1]).astype(BF16), upper, 1, 0)
    pos = [
        idr[k : k + 1, :] * float(CAP) + jnp.sum(before * hot[k], axis=0, keepdims=True) for k in range(2)
    ]
    rows_s = row_iota((CAP * NSP, 128)).astype(F32)
    dmat[...] = ((pos[0] == rows_s).astype(F32) + (pos[1] == rows_s).astype(F32)).astype(BF16)
    posc = jnp.where(
        sub == 0, pos[0],
        jnp.where(sub == 1, pos[1], jnp.where(sub == 2, gates[0:1, :], jnp.where(sub == 3, gates[1:2, :], 0.0))),
    ).T
    gat[...] = posc
    lanes_s = lane_iota((128, CAP * NSP)).astype(F32)
    for k in range(2):
        pmat[k] = (posc[:, k : k + 1] == lanes_s).astype(F32).astype(BF16)
    gain_rows = jnp.where(
        sub == 0, hgain[0:1, :], jnp.where(sub == 1, hgain[1:2, :], jnp.where(sub == 2, g1[pl.ds(own, 1), :], 0.0))
    )
    cols[...] = gain_rows.T
    tokcp.wait()
    tokt[...] = tokraw[...].astype(F32).T

    low = lane < 64

    def queries(k):
        for r in (1, 3, 2):
            wait(qraw.at[r, q_parts[k]], qrv.at[r - 1, k])
        for r in range(NX):
            at = pl.ds(r * 128, 128)
            if k == 0:
                narrow = qraw[r, 0]
                qs[0, at, :] = jnp.where(low, narrow, jnp.zeros_like(narrow))
                qs[1, at, :] = jnp.where(low, jnp.zeros_like(narrow), narrow)
            else:
                qs[2, at, :] = qraw[r, 1]
                qs[3, at, :] = qraw[r, 2]

    def attend(group, slots, start=False):
        turned = [kv[s, 1 if group == 0 else 4].T for s in slots]
        tiles = [(m, pl.ds(q * 256, 256)) for m in (2 * group, 2 * group + 1) for q in range(2)]
        scores = [[dot(kv[s, 0 if group == 0 else m], qs[m, at, :], 1, 1) for s in slots] for m, at in tiles]
        state = []
        for (m, at), score in zip(tiles, scores):
            top = functools.reduce(jnp.maximum, [jnp.max(s, axis=0, keepdims=True) for s in score])
            old = None
            if not start:
                old = ml[m : m + 1, at]
                top = jnp.maximum(old, top)
            expo = [jnp.exp2((s - top) * SCALES[group]) for s in score]
            total = functools.reduce(jnp.add, [jnp.sum(e, axis=0, keepdims=True) for e in expo])
            state.append((old, top, total, [e.astype(BF16) for e in expo]))
        for (m, at), (old, top, total, expo) in zip(tiles, state):
            numer = functools.reduce(jnp.add, [dot(v, e, 1, 0) for v, e in zip(turned, expo)])
            if start:
                acc[m, :, at] = numer
                ml[4 + m : 5 + m, at] = total
            else:
                shrink = jnp.exp2((old - top) * SCALES[group])
                acc[m, :, at] = acc[m, :, at] * shrink + numer
                ml[4 + m : 5 + m, at] = ml[4 + m : 5 + m, at] * shrink + total
            ml[m : m + 1, at] = top

    def arrive(d, group):
        for piece in ((0, 1), (2, 3, 4))[group]:
            kv_wait(d, piece)
            if d < 3 or group == 0:
                kv_send(0, d, piece, d, d + 1)
            kv_wait(4 + d, piece)
            if d < 3:
                kv_send(1, d, piece, 4 + d, 5 + d)
            elif group == 1:
                kv_send(1, d, piece, 7, 4)

    def far(group):
        for piece in ((0, 1), (2, 3, 4))[group]:
            kv_wait(4, piece)

    def share(group):
        for r in (2, 1, 3):
            at = pl.ds(r * 128, 128)
            for i in range(2):
                osend[r - 1, 2 * group + i] = acc[2 * group + i, :, at].astype(BF16)
            dev = (z, lax.rem(x + r, NX), y, c)
            pair = pl.ds(2 * group, 2)
            send(
                osend.at[r - 1, pair], orecv.at[r - 1, pair], osd.at[r - 1, group], orv.at[r - 1, group], dev
            )
            if group == 1:
                ssend[r - 1] = ml[:, at]
                send(ssend.at[r - 1], srecv.at[r - 1], ssd.at[r - 1], srv.at[r - 1], dev)

    arrive(1, 0)
    relayed(0)
    relay(1)
    queries(0)
    arrive(1, 1)
    attend(0, (0,), True)
    arrive(2, 0)
    attend(0, (1, 5))
    relayed(1)
    relay(2)
    queries(1)
    arrive(2, 1)
    lax.fori_loop(0, NY, proj, 0)
    attend(1, (0,), True)
    arrive(3, 0)
    attend(1, (1, 5))
    relayed(2)
    arrive(3, 1)
    swap_expert()
    attend(0, (2, 6))
    attend(1, (2, 6))
    attend(0, (3, 7))
    far(0)
    attend(0, (4,))
    share(0)
    attend(1, (3, 7))
    far(1)
    attend(1, (4,))
    share(1)

    wait(wp.at[0], loc.at[9])
    wait(wp.at[1], wrv.at[0])

    def turn(j, carry):
        for s in range(2):
            wpt[j, :, pl.ds(s * 256, 256)] = wp[s, j].T
        return carry

    lax.fori_loop(0, NY, turn, 0)

    for r in (1, 3, 2):
        for k in range(2):
            wait(orecv.at[r - 1, pl.ds(2 * k, 2)], orv.at[r - 1, k])
        wait(srecv.at[r - 1], srv.at[r - 1])
    for g in range(2):
        means = []
        for i in range(2):
            m = 2 * g + i
            tops = [ml[m : m + 1, 0:128]] + [srecv[r, m : m + 1, :] for r in range(3)]
            sums = [ml[4 + m : 5 + m, 0:128]] + [srecv[r, 4 + m : 5 + m, :] for r in range(3)]
            nums = [acc[m, :, 0:128]] + [orecv[r, m].astype(F32) for r in range(3)]
            top = functools.reduce(jnp.maximum, tops)
            w = [jnp.exp2((t - top) * SCALES[g]) for t in tops]
            total = functools.reduce(jnp.add, [a * b for a, b in zip(w, sums)])
            numer = functools.reduce(jnp.add, [a * b for a, b in zip(w, nums)])
            means.append(numer * ((1.0 if i == 0 else lam[0:1, g : g + 1]) / total))
        diff = means[0] - means[1]
        scale = lax.rsqrt(jnp.mean(diff * diff, axis=0, keepdims=True) + EPS)
        heads[0, pl.ds(g * 128, 128), :] = (diff * scale * cols[:, g : g + 1]).astype(BF16)
    send(heads.at[0], heads.at[1], hsd.at[0], hrv.at[0], partner)
    for r in (4, 3, 5, 2, 6, 1, 7, 0):
        part[0, r, :, 0:128] = dot(wpt[lax.rem(y + r, NY), :, 0:256], heads[0], 1, 0)
    wait(heads.at[1], hrv.at[0])

    far_first = (4, 3, 5, 2, 6, 1, 7)
    for r in far_first:
        t = lax.rem(y + r, NY)
        rsend[r - 1] = (part[0, r, :, 0:128] + dot(wpt[t, :, 256:512], heads[1], 1, 0)).astype(BF16)
        send(rsend.at[r - 1], rrecv.at[r - 1], rsd.at[r - 1], rrv.at[r - 1], (z, x, t, c))
    zt = ALPHA * tokt[...] + part[0, 0, :, 0:128] + dot(wpt[y, :, 256:512], heads[1], 1, 0)

    for k, buf in enumerate((wg, wu, wd)):
        wait(buf.at[0], loc.at[10 + k])
        wait(buf.at[1], wrv.at[1 + k])
    sub32 = row_iota((32, 128))
    for s in range(16):
        dy, dc = s // 2, s % 2
        j = 2 * lax.rem(y + NY - dy, NY) + (c if dc == 0 else other)
        gain = g1[pl.ds(j, 1), :]
        top = gain.astype(BF16).astype(F32)
        blocks[:, col(j)] = jnp.where(sub32 == s, top, jnp.where(sub32 == 16 + s, gain - top, 0.0)).astype(BF16)
    for k, w in enumerate((wg, wu)):
        for s in range(2):
            value = dot(blocks[...], w[s], 1, 0)
            value = value[0:16] + value[16:32]
            top = value.astype(BF16).astype(F32)
            gsum[k, s] = jnp.concatenate([top, top, value - top, jnp.zeros((80, 256), F32)], axis=0).astype(BF16)
    for r in far_first:
        wait(rrecv.at[r - 1], rrv.at[r - 1])
        zt = zt + rrecv[r - 1].astype(F32)

    sub2 = row_iota((2, 128))

    def local_stats(mean, dev2):
        return jnp.where(sub2 == 0, mean, dev2)

    mean = jnp.mean(zt, axis=0, keepdims=True)
    dev2 = jnp.sum(jnp.square(zt - mean), axis=0, keepdims=True)
    stat1[0] = local_stats(mean, dev2)
    order = [(dy, dc) for dy in (4, 3, 5, 2, 6, 1, 7, 0) for dc in (1, 0) if dy or dc]
    for dy, dc in order:
        s = 2 * dy + dc
        send(
            stat1.at[0], stat1.at[s], s1s.at[s - 1], s1r.at[s - 1],
            (z, x, lax.rem(y + dy, NY), c if dc == 0 else other),
        )
    raised = ((zt - mean) * cols[:, 2:3]).astype(BF16)
    disp[...] = dot(dmat[...], raised, 1, 1).astype(BF16)

    def unit(j):
        return pl.ds(pl.multiple_of(j * CAP, CAP), CAP)

    arrive_at = unit(c * 16 + lax.rem(me, 16))

    def dispatch(j, carry):
        t = lax.rem(me + j, NSP)
        send(disp.at[unit(t)], xg.at[0, arrive_at], dps.at[0], dpr.at[0], (t // NX, lax.rem(t, NX), y, half))
        return carry

    lax.fori_loop(1, NSP, dispatch, 0)

    @pl.when(half == c)
    def _():
        xg[0, arrive_at, :] = disp[unit(me), :]

    @pl.when(half != c)
    def _():
        send(disp.at[unit(me)], xg.at[0, arrive_at], dps.at[0], dpr.at[0], partner)

    for s in range(1, 16):
        wait(stat1.at[s], s1r.at[s - 1])
    total = functools.reduce(jnp.add, [stat1[s] for s in range(16)])
    mean = total[0:1, :] * (1.0 / 16)
    spread = total[1:2, :] + 128.0 * functools.reduce(
        jnp.add, [jnp.square(stat1[s, 0:1, :] - mean) for s in range(16)]
    )
    scale = lax.rsqrt(spread * (1.0 / 2048) + EPS)
    sub16 = row_iota((16, 128))
    shift = jnp.zeros((16, 128), F32)
    for s in range(16):
        shift = jnp.where(sub16 == s, stat1[s, 0:1, :] - mean, shift)
    top = shift.astype(BF16).astype(F32)
    one = scale.astype(BF16).astype(F32)
    two = (scale - one).astype(BF16).astype(F32)
    parts = jnp.where(
        sub16 == 0, one, jnp.where(sub16 == 1, two, jnp.where(sub16 == 2, scale - one - two, 0.0))
    )
    table = jnp.concatenate([top, shift - top, top, parts, jnp.zeros((64, 128), F32)], axis=0).astype(BF16)
    tdisp[...] = dot(dmat[...], table, 1, 1).astype(BF16)

    def follow(j, carry):
        t = lax.rem(me + j, NSP)
        send(
            tdisp.at[unit(t)], sx.at[unit(lax.rem(me, 16))], tds.at[0], tdr.at[0], (t // NX, lax.rem(t, NX), y, c)
        )
        return carry

    @pl.when(half == c)
    def _():
        lax.fori_loop(1, NSP, follow, 0)
        sx[unit(lax.rem(me, 16)), :] = tdisp[unit(me), :]

    mixed[...] = ((zt - mean) * scale * cols[:, 2:3]).astype(BF16).astype(F32).T * ALPHA

    def wait_units(ref, sem):
        @pl.when(half == c)
        def _():
            wait(ref.at[pl.ds(0, 496)], sem)

        @pl.when(half != c)
        def _():
            wait(ref, sem)

    wait_units(xg.at[0], dpr.at[0])

    def piece_of(h, k):
        return pl.ds(k * 256 + h * 128, 128)

    def xg_send(d, step, h, k, src_slot, dst_slot):
        send(
            xg.at[src_slot, piece_of(h, k)], xg.at[dst_slot, piece_of(h, k)], xgs.at[d, step, 2 * h + k],
            xgr.at[dst_slot, 2 * h + k], (z, x, (yp, ym)[d], c),
        )

    def xg_wait(slot, h, k):
        wait(xg.at[slot, piece_of(h, k)], xgr.at[slot, 2 * h + k])

    def xg_arrive(d, h, k):
        xg_wait(d, h, k)
        if d < 3 or k == 0:
            xg_send(0, d, h, k, d, d + 1)
        xg_wait(4 + d, h, k)
        if d < 3:
            xg_send(1, d, h, k, 4 + d, 5 + d)
        elif k == 1:
            xg_send(1, d, h, k, 7, 4)

    def slot_y(slot):
        away = NY - slot if slot <= 4 else slot - 4
        return lax.rem(y + away, NY)

    def absorb(slot, h, start=False):
        at = pl.ds(pl.multiple_of(slot_y(slot) * 256, 256), 256)
        rows_in = jnp.concatenate([xg[slot, piece_of(h, 0), :], xg[slot, piece_of(h, 1), :]], axis=1)
        for s in range(2):
            for w, a in ((wg, accg), (wu, accu)):
                value = dot(rows_in, w[s, at, :], 1, 0)
                a[h, s] = value if start else a[h, s] + value

    for h in (0, 1):
        for k in (0, 1):
            xg_send(0, 0, h, k, 0, 1)
            xg_send(1, 0, h, k, 0, 5)
    for h in (0, 1):
        absorb(0, h, True)
    for d in (1, 2, 3):
        for h in (0, 1):
            for k in (0, 1):
                xg_arrive(d, h, k)
            absorb(d, h)
            absorb(4 + d, h)

    def produce(h, r):
        at = pl.ds(pl.multiple_of(lax.rem(y + r, NY) * 256, 256), 256)
        part[h, r] = dot(act[h, 0], wd[0, :, at], 1, 0) + dot(act[h, 1], wd[1, :, at], 1, 0)

    def away(d, k, step):
        return (4 - k - step) if d == 0 else (NY - 3 - k + step) % NY

    def length(d, k):
        return 4 - k if d == 0 else 3 + k

    def pass_on(d, h, k, step):
        value = part[h, away(d, k, step), :, k * 128 : k * 128 + 128]
        p = 2 * h + k
        if step:
            wait(drecv.at[d, p, step - 1], ddr.at[d, p, step - 1])
            value = value + drecv[d, p, step - 1].astype(F32)
        dsend[d, p, step] = value.astype(BF16)
        send(
            dsend.at[d, p, step], drecv.at[d, p, step], dds.at[d, p, step], ddr.at[d, p, step],
            (z, x, (yp, ym)[d], c),
        )

    @pl.when(half == c)
    def _():
        wait(sx.at[pl.ds(0, 240)], tdr.at[0])

    @pl.when(half != c)
    def _():
        wait(sx, tdr.at[0])

    for h in (0, 1):
        stat = sx[h * 128 : h * 128 + 128, :]
        scales = stat[:, 48:64].astype(F32)
        scales = scales[:, 0:1] + scales[:, 1:2] + scales[:, 2:3]
        shifts = [[dot(stat, gsum[k, s], 1, 0) for s in range(2)] for k in range(2)]
        for k in (0, 1):
            xg_wait(4, h, k)
        absorb(4, h)
        for s in range(2):
            g = (accg[h, s] + shifts[0][s]) * scales
            act[h, s] = (g / (1.0 + jnp.exp(-g)) * ((accu[h, s] + shifts[1][s]) * scales)).astype(BF16)
        produce(h, 4)
        pass_on(0, h, 0, 0)
        pass_on(1, h, 1, 0)
        produce(h, 3)
        pass_on(0, h, 1, 0)
        produce(h, 5)
        pass_on(1, h, 0, 0)
        for r in (2, 6, 1, 7, 0):
            produce(h, r)
    for step in (1, 2, 3):
        for h in (0, 1):
            for d, k in ((0, 0), (1, 1), (0, 1), (1, 0)):
                if step < length(d, k):
                    pass_on(d, h, k, step)

    ret_at = unit(me)

    def give_back(i, carry):
        t = c * 16 + i
        for k in range(2):
            @pl.when(jnp.logical_or(t != me, c != k))
            def _():
                send(eo.at[k, unit(i)], ret.at[ret_at], rts.at[0], rtr.at[0], (t // NX, lax.rem(t, NX), y, k))
        return carry

    for h in (0, 1):
        for k in (0, 1):
            value = part[h, 0, :, k * 128 : k * 128 + 128]
            for d in range(2):
                last, p = length(d, k) - 1, 2 * h + k
                wait(drecv.at[d, p, last], ddr.at[d, p, last])
                value = value + drecv[d, p, last].astype(F32)
            eo[k, pl.ds(h * 128, 128), :] = value.astype(BF16)
        lax.fori_loop(8 * h, 8 * h + 8, give_back, 0)

    @pl.when(half == c)
    def _():
        ret[ret_at, :] = eo[c, unit(lax.rem(me, 16)), :]

    wait_units(ret, rtr.at[0])

    zz = mixed[...]
    for k in range(2):
        zz = zz + gat[:, 2 + k : 3 + k] * dot(pmat[k], ret[...], 1, 0)

    mean = jnp.mean(zz, axis=1, keepdims=True)
    dev = zz - mean
    dev2 = jnp.sum(dev * dev, axis=1, keepdims=True)
    fin[0] = dev.astype(BF16)
    packed = jnp.where(lane == 0, mean, jnp.where(lane == 1, dev2, 0.0)).T
    stat2[0] = packed[0:2, :]
    send(fin.at[0], fin.at[1], fns.at[0], fnr.at[0], partner)
    for dy, dc in order:
        s = 2 * dy + dc
        dev_id = (z, x, lax.rem(y + dy, NY), c if dc == 0 else other)
        send(stat2.at[0], stat2.at[s], s2s.at[s - 1], s2r.at[s - 1], dev_id)
    for dy in far_first:
        send(fin.at[0], fin.at[2 * dy], fns.at[2 * dy - 1], fnr.at[2 * dy - 1], (z, x, lax.rem(y + dy, NY), c))
    for step in range(4):
        for d in range(2):
            for piece in range(5):
                if step < 3 or (piece >= 2) == d:
                    wait(kv.at[0, piece], kvs.at[d, step, piece])
            for p in range(4):
                if step < 3 or p % 2 == d:
                    wait(xg.at[0, pl.ds(0, 128)], xgs.at[d, step, p])
                if step < length(d, p % 2):
                    wait(dsend.at[d, p, step], dds.at[d, p, step])
    for r in range(3):
        for k in range(2):
            wait(qraw.at[0, q_parts[k]], qsd.at[r, k])
            wait(osend.at[r, pl.ds(2 * k, 2)], osd.at[r, k])
        wait(ssend.at[r], ssd.at[r])
    wait(wp.at[0], wsd.at[0])
    for k, buf in enumerate((wg, wu, wd)):
        wait(buf.at[0], wsd.at[1 + k])
    wait(heads.at[0], hsd.at[0])
    for r in range(7):
        wait(rsend.at[r], rsd.at[r])
    for s in range(15):
        wait(stat1.at[0], s1s.at[s])
    wait_units(disp, dps.at[0])

    @pl.when(half == c)
    def _():
        wait(tdisp.at[pl.ds(0, 496)], tds.at[0])

    wait_units(ret, rts.at[0])
    for s in range(1, 16):
        wait(stat2.at[s], s2r.at[s - 1])
    total = functools.reduce(jnp.add, [stat2[s] for s in range(16)])
    mean = total[0:1, :] * (1.0 / 16)
    spread = total[1:2, :] + 128.0 * functools.reduce(
        jnp.add, [jnp.square(stat2[s, 0:1, :] - mean) for s in range(16)]
    )
    scale = lax.rsqrt(spread * (1.0 / 2048) + EPS)
    table = jnp.where(sub == 16, scale, 0.0)
    for s in range(16):
        table = jnp.where(sub == s, stat2[s, 0:1, :] - mean, table)
    table = table.T

    def finish(dy, dc):
        s = 2 * dy + dc
        j = 2 * lax.rem(y + NY - dy, NY) + (c if dc == 0 else other)
        value = (fin[s].astype(F32) + table[:, s : s + 1]) * table[:, 16:17] * g2[pl.ds(j, 1), :]
        outb[s] = value.astype(BF16)
        pltpu.make_async_copy(outb.at[s], out.at[:, col(j)], oud.at[s]).start()

    finish(0, 0)
    wait(fin.at[1], fnr.at[0])
    finish(0, 1)
    arrivals = far_first
    for i, dy in enumerate(arrivals):
        wait(fin.at[2 * dy], fnr.at[2 * dy - 1])
        send(fin.at[2 * dy], fin.at[2 * dy + 1], fns.at[2 * dy], fnr.at[2 * dy], partner)
        finish(dy, 0)
        if i:
            before_dy = arrivals[i - 1]
            wait(fin.at[2 * before_dy + 1], fnr.at[2 * before_dy])
            finish(before_dy, 1)
    wait(fin.at[15], fnr.at[14])
    finish(7, 1)

    for s in range(15):
        wait(stat2.at[0], s2s.at[s])
        wait(fin.at[0], fns.at[s])
    for s in range(16):
        wait(outb.at[s], oud.at[s])


def on_device(
    tokens, query_narrow, key_narrow, value_narrow, query_broad, key_broad, value_broad, mix_lambda,
    head_gain, proj_narrow, proj_broad, gain_one, gain_two, expert_ids, expert_gates,
    gate_weight, up_weight, down_weight,
):
    memory = pl.BlockSpec(memory_space=pltpu.HBM)
    dma = pltpu.SemaphoreType.DMA
    bf = lambda *s: pltpu.VMEM(s, BF16)
    fl = lambda *s: pltpu.VMEM(s, F32)
    scratch = [
        bf(8, 5, 128, 128), bf(4, 3, 128, 128), bf(4, 512, 128), fl(4, 128, 512), fl(8, 512),
        bf(3, 4, 128, 128), bf(3, 4, 128, 128), fl(3, 8, 128), fl(3, 8, 128),
        bf(2, 8, 256, 128), bf(8, 128, 512), bf(128, 128), fl(128, 128),
        fl(128, 128), bf(512, 128), bf(2, 128, 512), fl(128, 128),
        bf(2, 256, 128), bf(7, 128, 128), bf(7, 128, 128), fl(16, 2, 128),
        fl(128, 128), bf(512, 128), bf(8, 512, 128),
        bf(2, 2048, 256), bf(2, 2048, 256), bf(2, 256, 2048),
        fl(2, 2, 128, 256), fl(2, 2, 128, 256), bf(2, 2, 128, 256), fl(2, 8, 128, 256),
        bf(2, 4, 4, 128, 128), bf(2, 4, 4, 128, 128),
        bf(512, 128), bf(2, 256, 128), bf(16, 128, 128), fl(16, 2, 128),
        fl(1, 2), pltpu.VMEM((2, 128), jnp.int32), fl(2, 128), fl(2, 128), fl(16, 128), fl(16, 128),
        bf(16, 128, 128), bf(32, 2048), bf(2, 2, 128, 256), bf(512, 128), bf(256, 128),
        dma((13,)), dma((2, 4, 5)), dma((8, 5)), dma((3, 2)), dma((3, 2)), dma((4,)), dma((4,)),
        dma((3, 2)), dma((3, 2)), dma((3,)), dma((3,)), dma((1,)), dma((1,)), dma((7,)), dma((7,)),
        dma((15,)), dma((15,)), dma((1,)), dma((1,)), dma((2, 4, 4)), dma((8, 4)),
        dma((2, 4, 4)), dma((2, 4, 4)), dma((1,)), dma((1,)), dma((15,)), dma((15,)), dma((15,)), dma((15,)),
        dma((6,)), pltpu.SemaphoreType.REGULAR((3,)), dma((16,)), dma((1,)), dma((1,)),
    ]
    return pl.pallas_call(
        kernel,
        out_shape=jax.ShapeDtypeStruct((128, 2048), BF16),
        in_specs=[memory] * 18,
        out_specs=memory,
        scratch_shapes=scratch,
        compiler_params=pltpu.CompilerParams(
            collective_id=0, has_side_effects=True, vmem_limit_bytes=60 * 1024 * 1024
        ),
        name="layer",
    )(
        mix_lambda.T, expert_ids.T, expert_gates.T, head_gain, gain_one.reshape(16, 128), gain_two.reshape(16, 128),
        tokens, query_narrow, key_narrow, value_narrow, query_broad, key_broad, value_broad,
        proj_narrow, proj_broad, gate_weight, up_weight, down_weight,
    )


def solution(mesh):
    finer = Mesh(mesh.devices.reshape(NZ, NX, NY, 2), ("z", "x", "y", "c"))
    sp, tp = ("z", "x"), ("y", "c")
    return jax.shard_map(
        on_device,
        mesh=finer,
        in_specs=(
            P(sp, None), P(sp, tp), P(sp, tp), P(sp, tp), P(sp, tp), P(sp, tp), P(sp, tp), P(None, tp),
            P(), P(tp, None), P(tp, None), P(), P(), P(sp, None), P(sp, None),
            P(sp, None, tp), P(sp, None, tp), P(sp, tp, None),
        ),
        out_specs=P(sp, None),
        check_vma=False,
    )
```

```python
import functools

import jax
import jax.numpy as jnp
from jax import lax
from jax.experimental import pallas as pl
from jax.experimental.pallas import tpu as pltpu
from jax.sharding import Mesh
from jax.sharding import PartitionSpec as P

MESH = pl.DeviceIdType.MESH
NZ, NX, NY = 8, 4, 8
NSP = NZ * NX
CAP = 16
F32, BF16 = jnp.float32, jnp.bfloat16
ALPHA = 8.0**0.25
EPS = 1e-05
LOG2E = 1.4426950408889634
SCALES = (64**-0.5 * LOG2E, 128**-0.5 * LOG2E)


def dot(a, b, ca, cb):
    return lax.dot_general(a, b, (((ca,), (cb,)), ((), ())), preferred_element_type=F32)


def wait(ref, sem):
    pltpu.make_async_copy(ref, ref, sem).wait()


def send(src, dst, send_sem, recv_sem, dev):
    pltpu.make_async_remote_copy(
        src_ref=src, dst_ref=dst, send_sem=send_sem, recv_sem=recv_sem, device_id=dev, device_id_type=MESH
    ).start()


def row_iota(shape):
    return lax.broadcasted_iota(jnp.int32, shape, 0)


def lane_iota(shape):
    return lax.broadcasted_iota(jnp.int32, shape, 1)


def kernel(
    lam_in, ids_in, gates_in, hgain_in, g1_in, g2_in, tok, qn, kn, vn, qb, kb, vb, pn, pb, gw, uw, dw,
    out,
    kv, qraw, qs, acc, ml, osend, orecv, ssend, srecv, wp, wpt, tokraw, tokt, cols, dmat, pmat, gat,
    heads, rsend, rrecv, stat1, mixed, disp, xg, wg, wu, wd, accg, accu, act, part, dsend, drecv,
    ret, eo, fin, stat2, lam, ids, gates, hgain, g1, g2, outb, blocks, gsum, tdisp, sx,
    loc, kvs, kvr, qsd, qrv, wsd, wrv, osd, orv, ssd, srv, hsd, hrv, rsd, rrv, s1s, s1r, dps, dpr,
    xgs, xgr, dds, ddr, rts, rtr, fns, fnr, s2s, s2r, smalls, ysem, oud, tds, tdr,
):
    z, x, y, c = (lax.axis_index(n) for n in ("z", "x", "y", "c"))
    me = z * NX + x
    own = 2 * y + c
    other = 1 - c
    half = lax.rem(x, 2)
    place = (x // 2) * NZ + z
    far_z, far_x = (4, 3, 5, 2, 6, 1, 7, 0), (2, 1, 3, 0)
    zp, zm = lax.rem(z + 1, NZ), lax.rem(z + NZ - 1, NZ)
    yp, ym = lax.rem(y + 1, NY), lax.rem(y + NY - 1, NY)
    partner = (z, x, y, other)

    def col(j):
        return pl.ds(pl.multiple_of(j * 128, 128), 128)

    def local(i, src, dst):
        cp = pltpu.make_async_copy(src, dst, loc.at[i])
        cp.start()
        return cp

    first = [
        local(0, kn, kv.at[0, 0]), local(1, vn, kv.at[0, 1]),
        local(2, kb.at[:, pl.ds(0, 128)], kv.at[0, 2]), local(3, kb.at[:, pl.ds(128, 128)], kv.at[0, 3]),
        local(4, vb, kv.at[0, 4]),
        local(5, qn, qraw.at[0, 0]), local(6, qb.at[:, pl.ds(0, 128)], qraw.at[0, 1]),
        local(7, qb.at[:, pl.ds(128, 128)], qraw.at[0, 2]),
    ]
    tokcp = local(8, tok.at[:, col(own)], tokraw)
    small = []
    for i, (src, dst) in enumerate(
        ((ids_in, ids), (gates_in, gates), (hgain_in, hgain), (g1_in, g1), (g2_in, g2), (lam_in, lam))
    ):
        small.append(pltpu.make_async_copy(src, dst, smalls.at[i]))
        small[-1].start()

    barrier = pltpu.get_barrier_semaphore()
    sides_y = ((z, x, yp, c), (z, x, ym, c))
    for dev in [(zp, x, y, c), (zm, x, y, c), partner, *sides_y] + [
        (z, lax.rem(x + r, NX), y, c) for r in range(1, NX)
    ]:
        pl.semaphore_signal(barrier, inc=1, device_id=dev, device_id_type=MESH)
    pl.semaphore_wait(barrier, 8)

    def relay(k):
        for dev in sides_y:
            pl.semaphore_signal(ysem.at[k], inc=1, device_id=dev, device_id_type=MESH)

    def relayed(k):
        pl.semaphore_wait(ysem.at[k], 2)

    for cp in first:
        cp.wait()
    def kv_send(d, step, piece, src_slot, dst_slot):
        send(
            kv.at[src_slot, piece], kv.at[dst_slot, piece], kvs.at[d, step, piece], kvr.at[dst_slot, piece],
            ((zp, zm)[d], x, y, c),
        )

    def kv_wait(slot, piece):
        wait(kv.at[slot, piece], kvr.at[slot, piece])

    for piece in range(5):
        kv_send(0, 0, piece, 0, 1)
        kv_send(1, 0, piece, 0, 5)
    q_parts = (pl.ds(0, 1), pl.ds(1, 2))
    for k in range(2):
        for r in (2, 1, 3):
            send(
                qraw.at[0, q_parts[k]], qraw.at[r, q_parts[k]], qsd.at[r - 1, k], qrv.at[r - 1, k],
                (z, lax.rem(x + NX - r, NX), y, c),
            )
    relay(0)

    def proj(j, carry):
        for k, w in enumerate((pn, pb)):
            dst = pl.ds(k * 128, 128)
            pltpu.make_async_copy(w.at[:, col(2 * j + c)], wp.at[0, j, dst], loc.at[9]).start()
            send(w.at[:, col(2 * j + other)], wp.at[1, j, dst], wsd.at[0], wrv.at[0], partner)
        return carry

    for k, (w, buf) in enumerate(((gw, wg), (uw, wu), (dw, wd))):
        local(10 + k, w.at[0], buf.at[0])

    def swap_expert():
        for k, (w, buf) in enumerate(((gw, wg), (uw, wu), (dw, wd))):
            send(w.at[0], buf.at[1], wsd.at[1 + k], wrv.at[1 + k], partner)

    lane = lane_iota((128, 128))
    sub = row_iota((128, 128))
    for cp in small:
        cp.wait()
    idr = ids[...].astype(F32)
    rows_e = row_iota((NSP, 128)).astype(F32)
    hot = [(idr[k : k + 1, :] == rows_e).astype(F32) for k in range(2)]
    upper = (sub < lane).astype(F32).astype(BF16)
    before = dot((hot[0] + hot[1]).astype(BF16), upper, 1, 0)
    pos = [
        idr[k : k + 1, :] * float(CAP) + jnp.sum(before * hot[k], axis=0, keepdims=True) for k in range(2)
    ]
    rows_s = row_iota((CAP * NSP, 128)).astype(F32)
    dmat[...] = ((pos[0] == rows_s).astype(F32) + (pos[1] == rows_s).astype(F32)).astype(BF16)
    posc = jnp.where(
        sub == 0, pos[0],
        jnp.where(sub == 1, pos[1], jnp.where(sub == 2, gates[0:1, :], jnp.where(sub == 3, gates[1:2, :], 0.0))),
    ).T
    gat[...] = posc
    lanes_s = lane_iota((128, CAP * NSP)).astype(F32)
    for k in range(2):
        pmat[k] = (posc[:, k : k + 1] == lanes_s).astype(F32).astype(BF16)
    gain_rows = jnp.where(
        sub == 0, hgain[0:1, :], jnp.where(sub == 1, hgain[1:2, :], jnp.where(sub == 2, g1[pl.ds(own, 1), :], 0.0))
    )
    cols[...] = gain_rows.T
    tokcp.wait()
    tokt[...] = tokraw[...].astype(F32).T

    low = lane < 64

    def queries(k):
        for r in (1, 3, 2):
            wait(qraw.at[r, q_parts[k]], qrv.at[r - 1, k])
        for r in range(NX):
            at = pl.ds(r * 128, 128)
            if k == 0:
                narrow = qraw[r, 0]
                qs[0, at, :] = jnp.where(low, narrow, jnp.zeros_like(narrow))
                qs[1, at, :] = jnp.where(low, jnp.zeros_like(narrow), narrow)
            else:
                qs[2, at, :] = qraw[r, 1]
                qs[3, at, :] = qraw[r, 2]

    def attend(group, slots, start=False):
        turned = [kv[s, 1 if group == 0 else 4].T for s in slots]
        tiles = [(m, pl.ds(q * 256, 256)) for m in (2 * group, 2 * group + 1) for q in range(2)]
        scores = [[dot(kv[s, 0 if group == 0 else m], qs[m, at, :], 1, 1) for s in slots] for m, at in tiles]
        state = []
        for (m, at), score in zip(tiles, scores):
            top = functools.reduce(jnp.maximum, [jnp.max(s, axis=0, keepdims=True) for s in score])
            old = None
            if not start:
                old = ml[m : m + 1, at]
                top = jnp.maximum(old, top)
            expo = [jnp.exp2((s - top) * SCALES[group]) for s in score]
            total = functools.reduce(jnp.add, [jnp.sum(e, axis=0, keepdims=True) for e in expo])
            state.append((old, top, total, [e.astype(BF16) for e in expo]))
        for (m, at), (old, top, total, expo) in zip(tiles, state):
            numer = functools.reduce(jnp.add, [dot(v, e, 1, 0) for v, e in zip(turned, expo)])
            if start:
                acc[m, :, at] = numer
                ml[4 + m : 5 + m, at] = total
            else:
                shrink = jnp.exp2((old - top) * SCALES[group])
                acc[m, :, at] = acc[m, :, at] * shrink + numer
                ml[4 + m : 5 + m, at] = ml[4 + m : 5 + m, at] * shrink + total
            ml[m : m + 1, at] = top

    def arrive(d, group):
        for piece in ((0, 1), (2, 3, 4))[group]:
            kv_wait(d, piece)
            if d < 3 or group == 0:
                kv_send(0, d, piece, d, d + 1)
            kv_wait(4 + d, piece)
            if d < 3:
                kv_send(1, d, piece, 4 + d, 5 + d)
            elif group == 1:
                kv_send(1, d, piece, 7, 4)

    def far(group):
        for piece in ((0, 1), (2, 3, 4))[group]:
            kv_wait(4, piece)

    def share(group):
        for r in (2, 1, 3):
            at = pl.ds(r * 128, 128)
            for i in range(2):
                osend[r - 1, 2 * group + i] = acc[2 * group + i, :, at].astype(BF16)
            dev = (z, lax.rem(x + r, NX), y, c)
            pair = pl.ds(2 * group, 2)
            send(
                osend.at[r - 1, pair], orecv.at[r - 1, pair], osd.at[r - 1, group], orv.at[r - 1, group], dev
            )
            if group == 1:
                ssend[r - 1] = ml[:, at]
                send(ssend.at[r - 1], srecv.at[r - 1], ssd.at[r - 1], srv.at[r - 1], dev)

    arrive(1, 0)
    relayed(0)
    relay(1)
    queries(0)
    arrive(1, 1)
    attend(0, (0,), True)
    arrive(2, 0)
    attend(0, (1, 5))
    relayed(1)
    relay(2)
    queries(1)
    arrive(2, 1)
    lax.fori_loop(0, NY, proj, 0)
    attend(1, (0,), True)
    arrive(3, 0)
    attend(1, (1, 5))
    relayed(2)
    arrive(3, 1)
    swap_expert()
    attend(0, (2, 6))
    attend(1, (2, 6))
    attend(0, (3, 7))
    far(0)
    attend(0, (4,))
    share(0)
    attend(1, (3, 7))
    far(1)
    attend(1, (4,))
    share(1)

    wait(wp.at[0], loc.at[9])
    wait(wp.at[1], wrv.at[0])

    def turn(j, carry):
        for s in range(2):
            wpt[j, :, pl.ds(s * 256, 256)] = wp[s, j].T
        return carry

    lax.fori_loop(0, NY, turn, 0)

    for r in (1, 3, 2):
        for k in range(2):
            wait(orecv.at[r - 1, pl.ds(2 * k, 2)], orv.at[r - 1, k])
        wait(srecv.at[r - 1], srv.at[r - 1])
    for g in range(2):
        means = []
        for i in range(2):
            m = 2 * g + i
            tops = [ml[m : m + 1, 0:128]] + [srecv[r, m : m + 1, :] for r in range(3)]
            sums = [ml[4 + m : 5 + m, 0:128]] + [srecv[r, 4 + m : 5 + m, :] for r in range(3)]
            nums = [acc[m, :, 0:128]] + [orecv[r, m].astype(F32) for r in range(3)]
            top = functools.reduce(jnp.maximum, tops)
            w = [jnp.exp2((t - top) * SCALES[g]) for t in tops]
            total = functools.reduce(jnp.add, [a * b for a, b in zip(w, sums)])
            numer = functools.reduce(jnp.add, [a * b for a, b in zip(w, nums)])
            means.append(numer * ((1.0 if i == 0 else lam[0:1, g : g + 1]) / total))
        diff = means[0] - means[1]
        scale = lax.rsqrt(jnp.mean(diff * diff, axis=0, keepdims=True) + EPS)
        heads[0, pl.ds(g * 128, 128), :] = (diff * scale * cols[:, g : g + 1]).astype(BF16)
    send(heads.at[0], heads.at[1], hsd.at[0], hrv.at[0], partner)
    for r in (4, 3, 5, 2, 6, 1, 7, 0):
        part[0, r, :, 0:128] = dot(wpt[lax.rem(y + r, NY), :, 0:256], heads[0], 1, 0)
    wait(heads.at[1], hrv.at[0])

    def product(r):
        return part[0, r, :, 0:128] + dot(wpt[lax.rem(y + r, NY), :, 256:512], heads[1], 1, 0)

    def give(r):
        send(rsend.at[r - 1], rrecv.at[r - 1], rsd.at[r - 1], rrv.at[r - 1], (z, x, lax.rem(y + r, NY), c))

    ends = (pl.ds(0, 64), pl.ds(64, 64))
    rsend[3] = product(4).astype(BF16)
    for k, r in enumerate((3, 5)):
        send(
            rsend.at[3, ends[k]], rrecv.at[3, ends[k]], rsd.at[(3, 7)[k]], rrv.at[(3, 7)[k]],
            (z, x, lax.rem(y + r, NY), c),
        )
    for r in (3, 5, 2, 6):
        rsend[r - 1] = product(r).astype(BF16)
        give(r)
    near = [product(1), product(7)]
    zt = ALPHA * tokt[...] + product(0)

    for k, buf in enumerate((wg, wu, wd)):
        wait(buf.at[0], loc.at[10 + k])
        wait(buf.at[1], wrv.at[1 + k])
    sub32 = row_iota((32, 128))
    for s in range(16):
        dy, dc = s // 2, s % 2
        j = 2 * lax.rem(y + NY - dy, NY) + (c if dc == 0 else other)
        gain = g1[pl.ds(j, 1), :]
        top = gain.astype(BF16).astype(F32)
        blocks[:, col(j)] = jnp.where(sub32 == s, top, jnp.where(sub32 == 16 + s, gain - top, 0.0)).astype(BF16)
    for k, w in enumerate((wg, wu)):
        for s in range(2):
            value = dot(blocks[...], w[s], 1, 0)
            value = value[0:16] + value[16:32]
            top = value.astype(BF16).astype(F32)
            gsum[k, s] = jnp.concatenate([top, top, value - top, jnp.zeros((80, 256), F32)], axis=0).astype(BF16)
    for k, r in enumerate((1, 7)):
        wait(rrecv.at[3, ends[k]], rrv.at[(3, 7)[k]])
        passed = rrecv[3, ends[k], :].astype(F32)
        rest = near[k][64:128] if k == 0 else near[k][0:64]
        mine = near[k][0:64] if k == 0 else near[k][64:128]
        rsend[r - 1, ends[k], :] = (mine + passed).astype(BF16)
        rsend[r - 1, ends[1 - k], :] = rest.astype(BF16)
        give(r)
    for r in (3, 5, 2, 6, 1, 7):
        wait(rrecv.at[r - 1], rrv.at[r - 1])
        zt = zt + rrecv[r - 1].astype(F32)

    sub2 = row_iota((2, 128))

    def local_stats(mean, dev2):
        return jnp.where(sub2 == 0, mean, dev2)

    mean = jnp.mean(zt, axis=0, keepdims=True)
    dev2 = jnp.sum(jnp.square(zt - mean), axis=0, keepdims=True)
    stat1[0] = local_stats(mean, dev2)
    order = [(dy, dc) for dy in (4, 3, 5, 2, 6, 1, 7, 0) for dc in (1, 0) if dy or dc]
    for dy, dc in order:
        s = 2 * dy + dc
        send(
            stat1.at[0], stat1.at[s], s1s.at[s - 1], s1r.at[s - 1],
            (z, x, lax.rem(y + dy, NY), c if dc == 0 else other),
        )
    raised = ((zt - mean) * cols[:, 2:3]).astype(BF16)
    disp[...] = dot(dmat[...], raised, 1, 1).astype(BF16)

    def unit(j):
        return pl.ds(pl.multiple_of(j * CAP, CAP), CAP)

    arrive_at = unit(c * 16 + place)

    for dz in far_z:
        for dx in far_x:
            if dz or dx:
                tz, tx = lax.rem(z + dz, NZ), lax.rem(x + dx, NX)
                send(disp.at[unit(tz * NX + tx)], xg.at[0, arrive_at], dps.at[0], dpr.at[0], (tz, tx, y, half))

    @pl.when(half == c)
    def _():
        xg[0, arrive_at, :] = disp[unit(me), :]

    @pl.when(half != c)
    def _():
        send(disp.at[unit(me)], xg.at[0, arrive_at], dps.at[0], dpr.at[0], partner)

    for s in range(1, 16):
        wait(stat1.at[s], s1r.at[s - 1])
    total = functools.reduce(jnp.add, [stat1[s] for s in range(16)])
    mean = total[0:1, :] * (1.0 / 16)
    spread = total[1:2, :] + 128.0 * functools.reduce(
        jnp.add, [jnp.square(stat1[s, 0:1, :] - mean) for s in range(16)]
    )
    scale = lax.rsqrt(spread * (1.0 / 2048) + EPS)
    sub16 = row_iota((16, 128))
    shift = jnp.zeros((16, 128), F32)
    for s in range(16):
        shift = jnp.where(sub16 == s, stat1[s, 0:1, :] - mean, shift)
    top = shift.astype(BF16).astype(F32)
    one = scale.astype(BF16).astype(F32)
    two = (scale - one).astype(BF16).astype(F32)
    parts = jnp.where(
        sub16 == 0, one, jnp.where(sub16 == 1, two, jnp.where(sub16 == 2, scale - one - two, 0.0))
    )
    table = jnp.concatenate([top, shift - top, top, parts, jnp.zeros((64, 128), F32)], axis=0).astype(BF16)
    tdisp[...] = dot(dmat[...], table, 1, 1).astype(BF16)

    @pl.when(half == c)
    def _():
        for dz in far_z:
            for dx in far_x:
                if dz or dx:
                    tz, tx = lax.rem(z + dz, NZ), lax.rem(x + dx, NX)
                    send(tdisp.at[unit(tz * NX + tx)], sx.at[unit(place)], tds.at[0], tdr.at[0], (tz, tx, y, c))
        sx[unit(place), :] = tdisp[unit(me), :]

    mixed[...] = ((zt - mean) * scale * cols[:, 2:3]).astype(BF16).astype(F32).T * ALPHA

    def wait_units(ref, sem):
        @pl.when(half == c)
        def _():
            wait(ref.at[pl.ds(0, 496)], sem)

        @pl.when(half != c)
        def _():
            wait(ref, sem)

    wait_units(xg.at[0], dpr.at[0])

    def piece_of(h, k):
        return pl.ds(k * 256 + h * 128, 128)

    def xg_send(d, step, h, k, src_slot, dst_slot):
        send(
            xg.at[src_slot, piece_of(h, k)], xg.at[dst_slot, piece_of(h, k)], xgs.at[d, step, 2 * h + k],
            xgr.at[dst_slot, 2 * h + k], (z, x, (yp, ym)[d], c),
        )

    def xg_wait(slot, h, k):
        wait(xg.at[slot, piece_of(h, k)], xgr.at[slot, 2 * h + k])

    def xg_arrive(d, h, k):
        xg_wait(d, h, k)
        if d < 3 or k == 0:
            xg_send(0, d, h, k, d, d + 1)
        xg_wait(4 + d, h, k)
        if d < 3:
            xg_send(1, d, h, k, 4 + d, 5 + d)
        elif k == 1:
            xg_send(1, d, h, k, 7, 4)

    def slot_y(slot):
        away = NY - slot if slot <= 4 else slot - 4
        return lax.rem(y + away, NY)

    def absorb(slot, h, start=False):
        at = pl.ds(pl.multiple_of(slot_y(slot) * 256, 256), 256)
        rows_in = jnp.concatenate([xg[slot, piece_of(h, 0), :], xg[slot, piece_of(h, 1), :]], axis=1)
        for s in range(2):
            for w, a in ((wg, accg), (wu, accu)):
                value = dot(rows_in, w[s, at, :], 1, 0)
                a[h, s] = value if start else a[h, s] + value

    for h in (0, 1):
        for k in (0, 1):
            xg_send(0, 0, h, k, 0, 1)
            xg_send(1, 0, h, k, 0, 5)
    for h in (0, 1):
        absorb(0, h, True)
    for d in (1, 2, 3):
        for h in (0, 1):
            for k in (0, 1):
                xg_arrive(d, h, k)
            absorb(d, h)
            absorb(4 + d, h)

    def produce(h, r):
        at = pl.ds(pl.multiple_of(lax.rem(y + r, NY) * 256, 256), 256)
        part[h, r] = dot(act[h, 0], wd[0, :, at], 1, 0) + dot(act[h, 1], wd[1, :, at], 1, 0)

    def away(d, k, step):
        return (4 - k - step) if d == 0 else (NY - 3 - k + step) % NY

    def length(d, k):
        return 4 - k if d == 0 else 3 + k

    def pass_on(d, h, k, step):
        value = part[h, away(d, k, step), :, k * 128 : k * 128 + 128]
        p = 2 * h + k
        if step:
            wait(drecv.at[d, p, step - 1], ddr.at[d, p, step - 1])
            value = value + drecv[d, p, step - 1].astype(F32)
        dsend[d, p, step] = value.astype(BF16)
        send(
            dsend.at[d, p, step], drecv.at[d, p, step], dds.at[d, p, step], ddr.at[d, p, step],
            (z, x, (yp, ym)[d], c),
        )

    @pl.when(half == c)
    def _():
        wait(sx.at[pl.ds(0, 240)], tdr.at[0])

    @pl.when(half != c)
    def _():
        wait(sx, tdr.at[0])

    for h in (0, 1):
        stat = sx[h * 128 : h * 128 + 128, :]
        scales = stat[:, 48:64].astype(F32)
        scales = scales[:, 0:1] + scales[:, 1:2] + scales[:, 2:3]
        shifts = [[dot(stat, gsum[k, s], 1, 0) for s in range(2)] for k in range(2)]
        for k in (0, 1):
            xg_wait(4, h, k)
        absorb(4, h)
        for s in range(2):
            g = (accg[h, s] + shifts[0][s]) * scales
            act[h, s] = (g / (1.0 + jnp.exp(-g)) * ((accu[h, s] + shifts[1][s]) * scales)).astype(BF16)
        produce(h, 4)
        pass_on(0, h, 0, 0)
        pass_on(1, h, 1, 0)
        produce(h, 3)
        pass_on(0, h, 1, 0)
        produce(h, 5)
        pass_on(1, h, 0, 0)
        for r in (2, 6, 1, 7, 0):
            produce(h, r)
    for step in (1, 2, 3):
        for h in (0, 1):
            for d, k in ((0, 0), (1, 1), (0, 1), (1, 0)):
                if step < length(d, k):
                    pass_on(d, h, k, step)

    ret_at = unit(me)

    def give_back(h):
        tx = c + 2 * h
        for dz in far_z:
            tz = lax.rem(z + dz, NZ)
            for k in range(2):
                def go():
                    send(eo.at[k, unit(h * NZ + tz)], ret.at[ret_at], rts.at[0], rtr.at[0], (tz, tx, y, k))

                if dz:
                    go()
                else:
                    pl.when(jnp.logical_or(tx != x, c != k))(go)

    for h in (0, 1):
        for k in (0, 1):
            value = part[h, 0, :, k * 128 : k * 128 + 128]
            for d in range(2):
                last, p = length(d, k) - 1, 2 * h + k
                wait(drecv.at[d, p, last], ddr.at[d, p, last])
                value = value + drecv[d, p, last].astype(F32)
            eo[k, pl.ds(h * 128, 128), :] = value.astype(BF16)
        give_back(h)

    @pl.when(half == c)
    def _():
        ret[ret_at, :] = eo[c, unit(place), :]

    wait_units(ret, rtr.at[0])

    zz = mixed[...]
    for k in range(2):
        zz = zz + gat[:, 2 + k : 3 + k] * dot(pmat[k], ret[...], 1, 0)

    mean = jnp.mean(zz, axis=1, keepdims=True)
    dev = zz - mean
    dev2 = jnp.sum(dev * dev, axis=1, keepdims=True)
    fin[0] = dev.astype(BF16)
    packed = jnp.where(lane == 0, mean, jnp.where(lane == 1, dev2, 0.0)).T
    stat2[0] = packed[0:2, :]
    send(fin.at[0], fin.at[1], fns.at[0], fnr.at[0], partner)
    for dy, dc in order:
        s = 2 * dy + dc
        dev_id = (z, x, lax.rem(y + dy, NY), c if dc == 0 else other)
        send(stat2.at[0], stat2.at[s], s2s.at[s - 1], s2r.at[s - 1], dev_id)
    direct = (5, 3, 2, 6, 1, 7)
    for dy in direct:
        send(fin.at[0], fin.at[2 * dy], fns.at[2 * dy - 1], fnr.at[2 * dy - 1], (z, x, lax.rem(y + dy, NY), c))
    for step in range(4):
        for d in range(2):
            for piece in range(5):
                if step < 3 or (piece >= 2) == d:
                    wait(kv.at[0, piece], kvs.at[d, step, piece])
            for p in range(4):
                if step < 3 or p % 2 == d:
                    wait(xg.at[0, pl.ds(0, 128)], xgs.at[d, step, p])
                if step < length(d, p % 2):
                    wait(dsend.at[d, p, step], dds.at[d, p, step])
    for r in range(3):
        for k in range(2):
            wait(qraw.at[0, q_parts[k]], qsd.at[r, k])
            wait(osend.at[r, pl.ds(2 * k, 2)], osd.at[r, k])
        wait(ssend.at[r], ssd.at[r])
    wait(wp.at[0], wsd.at[0])
    for k, buf in enumerate((wg, wu, wd)):
        wait(buf.at[0], wsd.at[1 + k])
    wait(heads.at[0], hsd.at[0])
    for r in (0, 1, 2, 4, 5, 6):
        wait(rsend.at[r], rsd.at[r])
    for k in range(2):
        wait(rsend.at[3, ends[k]], rsd.at[(3, 7)[k]])
    for s in range(15):
        wait(stat1.at[0], s1s.at[s])
    wait_units(disp, dps.at[0])

    @pl.when(half == c)
    def _():
        wait(tdisp.at[pl.ds(0, 496)], tds.at[0])

    wait_units(ret, rts.at[0])
    for s in range(1, 16):
        wait(stat2.at[s], s2r.at[s - 1])
    total = functools.reduce(jnp.add, [stat2[s] for s in range(16)])
    mean = total[0:1, :] * (1.0 / 16)
    spread = total[1:2, :] + 128.0 * functools.reduce(
        jnp.add, [jnp.square(stat2[s, 0:1, :] - mean) for s in range(16)]
    )
    scale = lax.rsqrt(spread * (1.0 / 2048) + EPS)
    table = jnp.where(sub == 16, scale, 0.0)
    for s in range(16):
        table = jnp.where(sub == s, stat2[s, 0:1, :] - mean, table)
    table = table.T

    def finish(dy, dc):
        s = 2 * dy + dc
        j = 2 * lax.rem(y + NY - dy, NY) + (c if dc == 0 else other)
        value = (fin[s].astype(F32) + table[:, s : s + 1]) * table[:, 16:17] * g2[pl.ds(j, 1), :]
        outb[s] = value.astype(BF16)
        pltpu.make_async_copy(outb.at[s], out.at[:, col(j)], oud.at[s]).start()

    finish(0, 0)
    wait(fin.at[1], fnr.at[0])
    finish(0, 1)
    arrivals = (*direct, 4)
    for i, dy in enumerate(arrivals):
        wait(fin.at[2 * dy], fnr.at[2 * dy - 1])
        if dy == 5:
            send(fin.at[10], fin.at[8], fns.at[7], fnr.at[7], (z, x, ym, c))
        send(fin.at[2 * dy], fin.at[2 * dy + 1], fns.at[2 * dy], fnr.at[2 * dy], partner)
        finish(dy, 0)
        if i:
            before_dy = arrivals[i - 1]
            wait(fin.at[2 * before_dy + 1], fnr.at[2 * before_dy])
            finish(before_dy, 1)
    wait(fin.at[9], fnr.at[8])
    finish(4, 1)

    for s in range(15):
        wait(stat2.at[0], s2s.at[s])
        wait(fin.at[0], fns.at[s])
    for s in range(16):
        wait(outb.at[s], oud.at[s])


def on_device(
    tokens, query_narrow, key_narrow, value_narrow, query_broad, key_broad, value_broad, mix_lambda,
    head_gain, proj_narrow, proj_broad, gain_one, gain_two, expert_ids, expert_gates,
    gate_weight, up_weight, down_weight,
):
    memory = pl.BlockSpec(memory_space=pltpu.HBM)
    dma = pltpu.SemaphoreType.DMA
    bf = lambda *s: pltpu.VMEM(s, BF16)
    fl = lambda *s: pltpu.VMEM(s, F32)
    scratch = [
        bf(8, 5, 128, 128), bf(4, 3, 128, 128), bf(4, 512, 128), fl(4, 128, 512), fl(8, 512),
        bf(3, 4, 128, 128), bf(3, 4, 128, 128), fl(3, 8, 128), fl(3, 8, 128),
        bf(2, 8, 256, 128), bf(8, 128, 512), bf(128, 128), fl(128, 128),
        fl(128, 128), bf(512, 128), bf(2, 128, 512), fl(128, 128),
        bf(2, 256, 128), bf(7, 128, 128), bf(7, 128, 128), fl(16, 2, 128),
        fl(128, 128), bf(512, 128), bf(8, 512, 128),
        bf(2, 2048, 256), bf(2, 2048, 256), bf(2, 256, 2048),
        fl(2, 2, 128, 256), fl(2, 2, 128, 256), bf(2, 2, 128, 256), fl(2, 8, 128, 256),
        bf(2, 4, 4, 128, 128), bf(2, 4, 4, 128, 128),
        bf(512, 128), bf(2, 256, 128), bf(16, 128, 128), fl(16, 2, 128),
        fl(1, 2), pltpu.VMEM((2, 128), jnp.int32), fl(2, 128), fl(2, 128), fl(16, 128), fl(16, 128),
        bf(16, 128, 128), bf(32, 2048), bf(2, 2, 128, 256), bf(512, 128), bf(256, 128),
        dma((13,)), dma((2, 4, 5)), dma((8, 5)), dma((3, 2)), dma((3, 2)), dma((4,)), dma((4,)),
        dma((3, 2)), dma((3, 2)), dma((3,)), dma((3,)), dma((1,)), dma((1,)), dma((8,)), dma((8,)),
        dma((15,)), dma((15,)), dma((1,)), dma((1,)), dma((2, 4, 4)), dma((8, 4)),
        dma((2, 4, 4)), dma((2, 4, 4)), dma((1,)), dma((1,)), dma((15,)), dma((15,)), dma((15,)), dma((15,)),
        dma((6,)), pltpu.SemaphoreType.REGULAR((3,)), dma((16,)), dma((1,)), dma((1,)),
    ]
    return pl.pallas_call(
        kernel,
        out_shape=jax.ShapeDtypeStruct((128, 2048), BF16),
        in_specs=[memory] * 18,
        out_specs=memory,
        scratch_shapes=scratch,
        compiler_params=pltpu.CompilerParams(
            collective_id=0, has_side_effects=True, vmem_limit_bytes=60 * 1024 * 1024
        ),
        name="layer",
    )(
        mix_lambda.T, expert_ids.T, expert_gates.T, head_gain, gain_one.reshape(16, 128), gain_two.reshape(16, 128),
        tokens, query_narrow, key_narrow, value_narrow, query_broad, key_broad, value_broad,
        proj_narrow, proj_broad, gate_weight, up_weight, down_weight,
    )


def solution(mesh):
    finer = Mesh(mesh.devices.reshape(NZ, NX, NY, 2), ("z", "x", "y", "c"))
    sp, tp = ("z", "x"), ("y", "c")
    return jax.shard_map(
        on_device,
        mesh=finer,
        in_specs=(
            P(sp, None), P(sp, tp), P(sp, tp), P(sp, tp), P(sp, tp), P(sp, tp), P(sp, tp), P(None, tp),
            P(), P(tp, None), P(tp, None), P(), P(), P(sp, None), P(sp, None),
            P(sp, None, tp), P(sp, None, tp), P(sp, tp, None),
        ),
        out_specs=P(sp, None),
        check_vma=False,
    )
```

```python
import functools

import jax
import jax.numpy as jnp
from jax import lax
from jax.experimental import pallas as pl
from jax.experimental.pallas import tpu as pltpu
from jax.sharding import Mesh
from jax.sharding import PartitionSpec as P

MESH = pl.DeviceIdType.MESH
NZ, NX, NY = 8, 4, 8
NSP = NZ * NX
CAP = 16
F32, BF16 = jnp.float32, jnp.bfloat16
ALPHA = 8.0**0.25
EPS = 1e-05
LOG2E = 1.4426950408889634
SCALES = (64**-0.5 * LOG2E, 128**-0.5 * LOG2E)


def dot(a, b, ca, cb):
    return lax.dot_general(a, b, (((ca,), (cb,)), ((), ())), preferred_element_type=F32)


def wait(ref, sem):
    pltpu.make_async_copy(ref, ref, sem).wait()


def send(src, dst, send_sem, recv_sem, dev):
    pltpu.make_async_remote_copy(
        src_ref=src, dst_ref=dst, send_sem=send_sem, recv_sem=recv_sem, device_id=dev, device_id_type=MESH
    ).start()


def row_iota(shape):
    return lax.broadcasted_iota(jnp.int32, shape, 0)


def lane_iota(shape):
    return lax.broadcasted_iota(jnp.int32, shape, 1)


def kernel(
    lam_in, ids_in, gates_in, hgain_in, g1_in, g2_in, tok, qn, kn, vn, qb, kb, vb, pn, pb, gw, uw, dw,
    out,
    kv, qraw, qs, acc, ml, osend, orecv, ssend, srecv, wp, wpt, tokraw, tokt, cols, dmat, pmat, gat,
    heads, rsend, rrecv, stat1, mixed, disp, xg, wg, wu, wd, accg, accu, act, part, dsend, drecv,
    ret, eo, fin, stat2, lam, ids, gates, hgain, g1, g2, outb, blocks, gsum, tdisp, sx,
    loc, kvs, kvr, qsd, qrv, wsd, wrv, osd, orv, ssd, srv, hsd, hrv, rsd, rrv, s1s, s1r, dps, dpr,
    xgs, xgr, dds, ddr, rts, rtr, fns, fnr, s2s, s2r, smalls, ysem, oud, tds, tdr,
):
    z, x, y, c = (lax.axis_index(n) for n in ("z", "x", "y", "c"))
    me = z * NX + x
    own = 2 * y + c
    other = 1 - c
    half = lax.rem(x, 2)
    place = (x // 2) * NZ + z
    far_z, far_x = (4, 3, 5, 2, 6, 1, 7, 0), (2, 1, 3, 0)
    zp, zm = lax.rem(z + 1, NZ), lax.rem(z + NZ - 1, NZ)
    yp, ym = lax.rem(y + 1, NY), lax.rem(y + NY - 1, NY)
    partner = (z, x, y, other)

    def col(j):
        return pl.ds(pl.multiple_of(j * 128, 128), 128)

    def local(i, src, dst):
        cp = pltpu.make_async_copy(src, dst, loc.at[i])
        cp.start()
        return cp

    first = [
        local(0, kn, kv.at[0, 0]), local(1, vn, kv.at[0, 1]),
        local(2, kb.at[:, pl.ds(0, 128)], kv.at[0, 2]), local(3, kb.at[:, pl.ds(128, 128)], kv.at[0, 3]),
        local(4, vb, kv.at[0, 4]),
        local(5, qn, qraw.at[0, 0]), local(6, qb.at[:, pl.ds(0, 128)], qraw.at[0, 1]),
        local(7, qb.at[:, pl.ds(128, 128)], qraw.at[0, 2]),
    ]
    tokcp = local(8, tok.at[:, col(own)], tokraw)
    small = []
    for i, (src, dst) in enumerate(
        ((ids_in, ids), (gates_in, gates), (hgain_in, hgain), (g1_in, g1), (g2_in, g2), (lam_in, lam))
    ):
        small.append(pltpu.make_async_copy(src, dst, smalls.at[i]))
        small[-1].start()

    barrier = pltpu.get_barrier_semaphore()
    sides_y = ((z, x, yp, c), (z, x, ym, c))
    for dev in [(zp, x, y, c), (zm, x, y, c), partner, *sides_y] + [
        (z, lax.rem(x + r, NX), y, c) for r in range(1, NX)
    ]:
        pl.semaphore_signal(barrier, inc=1, device_id=dev, device_id_type=MESH)
    pl.semaphore_wait(barrier, 8)

    def relay(k):
        for dev in sides_y:
            pl.semaphore_signal(ysem.at[k], inc=1, device_id=dev, device_id_type=MESH)

    def relayed(k):
        pl.semaphore_wait(ysem.at[k], 2)

    for cp in first:
        cp.wait()
    def kv_send(d, step, piece, src_slot, dst_slot):
        send(
            kv.at[src_slot, piece], kv.at[dst_slot, piece], kvs.at[d, step, piece], kvr.at[dst_slot, piece],
            ((zp, zm)[d], x, y, c),
        )

    def kv_wait(slot, piece):
        wait(kv.at[slot, piece], kvr.at[slot, piece])

    for piece in range(5):
        kv_send(0, 0, piece, 0, 1)
        kv_send(1, 0, piece, 0, 5)
    q_parts = (pl.ds(0, 1), pl.ds(1, 2))
    for k in range(2):
        for r in (2, 1, 3):
            send(
                qraw.at[0, q_parts[k]], qraw.at[r, q_parts[k]], qsd.at[r - 1, k], qrv.at[r - 1, k],
                (z, lax.rem(x + NX - r, NX), y, c),
            )
    relay(0)

    def proj(j, carry):
        for k, w in enumerate((pn, pb)):
            dst = pl.ds(k * 128, 128)
            pltpu.make_async_copy(w.at[:, col(2 * j + c)], wp.at[0, j, dst], loc.at[9]).start()
            send(w.at[:, col(2 * j + other)], wp.at[1, j, dst], wsd.at[0], wrv.at[0], partner)
        return carry

    for k, (w, buf) in enumerate(((gw, wg), (uw, wu), (dw, wd))):
        local(10 + k, w.at[0], buf.at[0])

    def swap_expert():
        for k, (w, buf) in enumerate(((gw, wg), (uw, wu), (dw, wd))):
            send(w.at[0], buf.at[1], wsd.at[1 + k], wrv.at[1 + k], partner)

    lane = lane_iota((128, 128))
    sub = row_iota((128, 128))
    for cp in small:
        cp.wait()
    idr = ids[...].astype(F32)
    rows_e = row_iota((NSP, 128)).astype(F32)
    hot = [(idr[k : k + 1, :] == rows_e).astype(F32) for k in range(2)]
    upper = (sub < lane).astype(F32).astype(BF16)
    before = dot((hot[0] + hot[1]).astype(BF16), upper, 1, 0)
    pos = [
        idr[k : k + 1, :] * float(CAP) + jnp.sum(before * hot[k], axis=0, keepdims=True) for k in range(2)
    ]
    rows_s = row_iota((CAP * NSP, 128)).astype(F32)
    dmat[...] = ((pos[0] == rows_s).astype(F32) + (pos[1] == rows_s).astype(F32)).astype(BF16)
    posc = jnp.where(
        sub == 0, pos[0],
        jnp.where(sub == 1, pos[1], jnp.where(sub == 2, gates[0:1, :], jnp.where(sub == 3, gates[1:2, :], 0.0))),
    ).T
    gat[...] = posc
    lanes_s = lane_iota((128, CAP * NSP)).astype(F32)
    for k in range(2):
        pmat[k] = (posc[:, k : k + 1] == lanes_s).astype(F32).astype(BF16)
    gain_rows = jnp.where(
        sub == 0, hgain[0:1, :], jnp.where(sub == 1, hgain[1:2, :], jnp.where(sub == 2, g1[pl.ds(own, 1), :], 0.0))
    )
    cols[...] = gain_rows.T
    tokcp.wait()
    tokt[...] = tokraw[...].astype(F32).T

    low = lane < 64

    def queries(k):
        for r in (1, 3, 2):
            wait(qraw.at[r, q_parts[k]], qrv.at[r - 1, k])
        for r in range(NX):
            at = pl.ds(r * 128, 128)
            if k == 0:
                narrow = qraw[r, 0]
                qs[0, at, :] = jnp.where(low, narrow, jnp.zeros_like(narrow))
                qs[1, at, :] = jnp.where(low, jnp.zeros_like(narrow), narrow)
            else:
                qs[2, at, :] = qraw[r, 1]
                qs[3, at, :] = qraw[r, 2]

    def attend(group, slots, start=False):
        turned = [kv[s, 1 if group == 0 else 4].T for s in slots]
        tiles = [(m, pl.ds(q * 256, 256)) for m in (2 * group, 2 * group + 1) for q in range(2)]
        scores = [[dot(kv[s, 0 if group == 0 else m], qs[m, at, :], 1, 1) for s in slots] for m, at in tiles]
        state = []
        for (m, at), score in zip(tiles, scores):
            top = functools.reduce(jnp.maximum, [jnp.max(s, axis=0, keepdims=True) for s in score])
            old = None
            if not start:
                old = ml[m : m + 1, at]
                top = jnp.maximum(old, top)
            expo = [jnp.exp2((s - top) * SCALES[group]) for s in score]
            total = functools.reduce(jnp.add, [jnp.sum(e, axis=0, keepdims=True) for e in expo])
            state.append((old, top, total, [e.astype(BF16) for e in expo]))
        for (m, at), (old, top, total, expo) in zip(tiles, state):
            numer = functools.reduce(jnp.add, [dot(v, e, 1, 0) for v, e in zip(turned, expo)])
            if start:
                acc[m, :, at] = numer
                ml[4 + m : 5 + m, at] = total
            else:
                shrink = jnp.exp2((old - top) * SCALES[group])
                acc[m, :, at] = acc[m, :, at] * shrink + numer
                ml[4 + m : 5 + m, at] = ml[4 + m : 5 + m, at] * shrink + total
            ml[m : m + 1, at] = top

    def arrive(d, group):
        for piece in ((0, 1), (2, 3, 4))[group]:
            kv_wait(d, piece)
            if d < 3 or group == 0:
                kv_send(0, d, piece, d, d + 1)
            kv_wait(4 + d, piece)
            if d < 3:
                kv_send(1, d, piece, 4 + d, 5 + d)
            elif group == 1:
                kv_send(1, d, piece, 7, 4)

    def far(group):
        for piece in ((0, 1), (2, 3, 4))[group]:
            kv_wait(4, piece)

    def share(group):
        for r in (2, 1, 3):
            at = pl.ds(r * 128, 128)
            for i in range(2):
                osend[r - 1, 2 * group + i] = acc[2 * group + i, :, at].astype(BF16)
            dev = (z, lax.rem(x + r, NX), y, c)
            pair = pl.ds(2 * group, 2)
            send(
                osend.at[r - 1, pair], orecv.at[r - 1, pair], osd.at[r - 1, group], orv.at[r - 1, group], dev
            )
            if group == 1:
                ssend[r - 1] = ml[:, at]
                send(ssend.at[r - 1], srecv.at[r - 1], ssd.at[r - 1], srv.at[r - 1], dev)

    arrive(1, 0)
    relayed(0)
    relay(1)
    queries(0)
    arrive(1, 1)
    attend(0, (0,), True)
    arrive(2, 0)
    attend(0, (1, 5))
    relayed(1)
    relay(2)
    queries(1)
    arrive(2, 1)
    lax.fori_loop(0, NY, proj, 0)
    attend(1, (0,), True)
    arrive(3, 0)
    attend(1, (1, 5))
    relayed(2)
    arrive(3, 1)
    swap_expert()
    attend(0, (2, 6))
    attend(1, (2, 6))
    attend(0, (3, 7))
    far(0)
    attend(0, (4,))
    share(0)
    attend(1, (3, 7))
    far(1)
    attend(1, (4,))
    share(1)

    wait(wp.at[0], loc.at[9])
    wait(wp.at[1], wrv.at[0])

    def turn(j, carry):
        for s in range(2):
            wpt[j, :, pl.ds(s * 256, 256)] = wp[s, j].T
        return carry

    lax.fori_loop(0, NY, turn, 0)

    for r in (1, 3, 2):
        for k in range(2):
            wait(orecv.at[r - 1, pl.ds(2 * k, 2)], orv.at[r - 1, k])
        wait(srecv.at[r - 1], srv.at[r - 1])
    for g in range(2):
        means = []
        for i in range(2):
            m = 2 * g + i
            tops = [ml[m : m + 1, 0:128]] + [srecv[r, m : m + 1, :] for r in range(3)]
            sums = [ml[4 + m : 5 + m, 0:128]] + [srecv[r, 4 + m : 5 + m, :] for r in range(3)]
            nums = [acc[m, :, 0:128]] + [orecv[r, m].astype(F32) for r in range(3)]
            top = functools.reduce(jnp.maximum, tops)
            w = [jnp.exp2((t - top) * SCALES[g]) for t in tops]
            total = functools.reduce(jnp.add, [a * b for a, b in zip(w, sums)])
            numer = functools.reduce(jnp.add, [a * b for a, b in zip(w, nums)])
            means.append(numer * ((1.0 if i == 0 else lam[0:1, g : g + 1]) / total))
        diff = means[0] - means[1]
        scale = lax.rsqrt(jnp.mean(diff * diff, axis=0, keepdims=True) + EPS)
        heads[0, pl.ds(g * 128, 128), :] = (diff * scale * cols[:, g : g + 1]).astype(BF16)
    send(heads.at[0], heads.at[1], hsd.at[0], hrv.at[0], partner)
    for r in (4, 3, 5, 2, 6, 1, 7, 0):
        part[0, r, :, 0:128] = dot(wpt[lax.rem(y + r, NY), :, 0:256], heads[0], 1, 0)
    wait(heads.at[1], hrv.at[0])

    def product(r):
        return part[0, r, :, 0:128] + dot(wpt[lax.rem(y + r, NY), :, 256:512], heads[1], 1, 0)

    def give(r):
        send(rsend.at[r - 1], rrecv.at[r - 1], rsd.at[r - 1], rrv.at[r - 1], (z, x, lax.rem(y + r, NY), c))

    ends = (pl.ds(0, 64), pl.ds(64, 64))
    rsend[3] = product(4).astype(BF16)
    for k, r in enumerate((3, 5)):
        send(
            rsend.at[3, ends[k]], rrecv.at[3, ends[k]], rsd.at[(3, 7)[k]], rrv.at[(3, 7)[k]],
            (z, x, lax.rem(y + r, NY), c),
        )
    for r in (3, 5, 2, 6):
        rsend[r - 1] = product(r).astype(BF16)
        give(r)
    near = [product(1), product(7)]
    zt = ALPHA * tokt[...] + product(0)

    for k, buf in enumerate((wg, wu, wd)):
        wait(buf.at[0], loc.at[10 + k])
        wait(buf.at[1], wrv.at[1 + k])
    sub32 = row_iota((32, 128))
    for s in range(16):
        dy, dc = s // 2, s % 2
        j = 2 * lax.rem(y + NY - dy, NY) + (c if dc == 0 else other)
        gain = g1[pl.ds(j, 1), :]
        top = gain.astype(BF16).astype(F32)
        blocks[:, col(j)] = jnp.where(sub32 == s, top, jnp.where(sub32 == 16 + s, gain - top, 0.0)).astype(BF16)
    for k, w in enumerate((wg, wu)):
        for s in range(2):
            value = dot(blocks[...], w[s], 1, 0)
            value = value[0:16] + value[16:32]
            top = value.astype(BF16).astype(F32)
            gsum[k, s] = jnp.concatenate([top, top, value - top, jnp.zeros((80, 256), F32)], axis=0).astype(BF16)
    for k, r in enumerate((1, 7)):
        wait(rrecv.at[3, ends[k]], rrv.at[(3, 7)[k]])
        passed = rrecv[3, ends[k], :].astype(F32)
        rest = near[k][64:128] if k == 0 else near[k][0:64]
        mine = near[k][0:64] if k == 0 else near[k][64:128]
        rsend[r - 1, ends[k], :] = (mine + passed).astype(BF16)
        rsend[r - 1, ends[1 - k], :] = rest.astype(BF16)
        give(r)
    for r in (3, 5, 2, 6, 1, 7):
        wait(rrecv.at[r - 1], rrv.at[r - 1])
        zt = zt + rrecv[r - 1].astype(F32)

    sub2 = row_iota((2, 128))

    def local_stats(mean, dev2):
        return jnp.where(sub2 == 0, mean, dev2)

    mean = jnp.mean(zt, axis=0, keepdims=True)
    dev2 = jnp.sum(jnp.square(zt - mean), axis=0, keepdims=True)
    stat1[0] = local_stats(mean, dev2)
    order = [(dy, dc) for dy in (4, 3, 5, 2, 6, 1, 7, 0) for dc in (1, 0) if dy or dc]
    for dy, dc in order:
        s = 2 * dy + dc
        send(
            stat1.at[0], stat1.at[s], s1s.at[s - 1], s1r.at[s - 1],
            (z, x, lax.rem(y + dy, NY), c if dc == 0 else other),
        )
    raised = ((zt - mean) * cols[:, 2:3]).astype(BF16)
    disp[...] = dot(dmat[...], raised, 1, 1).astype(BF16)

    def unit(j):
        return pl.ds(pl.multiple_of(j * CAP, CAP), CAP)

    arrive_at = unit(c * 16 + place)

    for dz in far_z:
        for dx in far_x:
            if dz or dx:
                tz, tx = lax.rem(z + dz, NZ), lax.rem(x + dx, NX)
                send(disp.at[unit(tz * NX + tx)], xg.at[0, arrive_at], dps.at[0], dpr.at[0], (tz, tx, y, half))

    @pl.when(half == c)
    def _():
        xg[0, arrive_at, :] = disp[unit(me), :]

    @pl.when(half != c)
    def _():
        send(disp.at[unit(me)], xg.at[0, arrive_at], dps.at[0], dpr.at[0], partner)

    def wait_units(ref, sem):
        @pl.when(half == c)
        def _():
            wait(ref.at[pl.ds(0, 496)], sem)

        @pl.when(half != c)
        def _():
            wait(ref, sem)

    wait_units(xg.at[0], dpr.at[0])

    def piece_of(h, k):
        return pl.ds(k * 256 + h * 128, 128)

    def xg_send(d, step, h, k, src_slot, dst_slot):
        send(
            xg.at[src_slot, piece_of(h, k)], xg.at[dst_slot, piece_of(h, k)], xgs.at[d, step, 2 * h + k],
            xgr.at[dst_slot, 2 * h + k], (z, x, (yp, ym)[d], c),
        )

    def xg_wait(slot, h, k):
        wait(xg.at[slot, piece_of(h, k)], xgr.at[slot, 2 * h + k])

    def xg_arrive(d, h, k):
        xg_wait(d, h, k)
        if d < 3 or k == 0:
            xg_send(0, d, h, k, d, d + 1)
        xg_wait(4 + d, h, k)
        if d < 3:
            xg_send(1, d, h, k, 4 + d, 5 + d)
        elif k == 1:
            xg_send(1, d, h, k, 7, 4)

    def slot_y(slot):
        away = NY - slot if slot <= 4 else slot - 4
        return lax.rem(y + away, NY)

    def absorb(slot, h, start=False):
        at = pl.ds(pl.multiple_of(slot_y(slot) * 256, 256), 256)
        rows_in = jnp.concatenate([xg[slot, piece_of(h, 0), :], xg[slot, piece_of(h, 1), :]], axis=1)
        for s in range(2):
            for w, a in ((wg, accg), (wu, accu)):
                value = dot(rows_in, w[s, at, :], 1, 0)
                a[h, s] = value if start else a[h, s] + value

    for h in (0, 1):
        for k in (0, 1):
            xg_send(0, 0, h, k, 0, 1)
            xg_send(1, 0, h, k, 0, 5)
    for s in range(1, 16):
        wait(stat1.at[s], s1r.at[s - 1])
    total = functools.reduce(jnp.add, [stat1[s] for s in range(16)])
    mean = total[0:1, :] * (1.0 / 16)
    spread = total[1:2, :] + 128.0 * functools.reduce(
        jnp.add, [jnp.square(stat1[s, 0:1, :] - mean) for s in range(16)]
    )
    scale = lax.rsqrt(spread * (1.0 / 2048) + EPS)
    sub16 = row_iota((16, 128))
    shift = jnp.zeros((16, 128), F32)
    for s in range(16):
        shift = jnp.where(sub16 == s, stat1[s, 0:1, :] - mean, shift)
    top = shift.astype(BF16).astype(F32)
    one = scale.astype(BF16).astype(F32)
    two = (scale - one).astype(BF16).astype(F32)
    parts = jnp.where(
        sub16 == 0, one, jnp.where(sub16 == 1, two, jnp.where(sub16 == 2, scale - one - two, 0.0))
    )
    table = jnp.concatenate([top, shift - top, top, parts, jnp.zeros((64, 128), F32)], axis=0).astype(BF16)
    tdisp[...] = dot(dmat[...], table, 1, 1).astype(BF16)

    @pl.when(half == c)
    def _():
        for dz in far_z:
            for dx in far_x:
                if dz or dx:
                    tz, tx = lax.rem(z + dz, NZ), lax.rem(x + dx, NX)
                    send(tdisp.at[unit(tz * NX + tx)], sx.at[unit(place)], tds.at[0], tdr.at[0], (tz, tx, y, c))
        sx[unit(place), :] = tdisp[unit(me), :]

    mixed[...] = ((zt - mean) * scale * cols[:, 2:3]).astype(BF16).astype(F32).T * ALPHA

    for h in (0, 1):
        absorb(0, h, True)
    for d in (1, 2, 3):
        for h in (0, 1):
            for k in (0, 1):
                xg_arrive(d, h, k)
            absorb(d, h)
            absorb(4 + d, h)

    def produce(h, r):
        at = pl.ds(pl.multiple_of(lax.rem(y + r, NY) * 256, 256), 256)
        part[h, r] = dot(act[h, 0], wd[0, :, at], 1, 0) + dot(act[h, 1], wd[1, :, at], 1, 0)

    def away(d, k, step):
        return (4 - k - step) if d == 0 else (NY - 3 - k + step) % NY

    def length(d, k):
        return 4 - k if d == 0 else 3 + k

    def pass_on(d, h, k, step):
        value = part[h, away(d, k, step), :, k * 128 : k * 128 + 128]
        p = 2 * h + k
        if step:
            wait(drecv.at[d, p, step - 1], ddr.at[d, p, step - 1])
            value = value + drecv[d, p, step - 1].astype(F32)
        dsend[d, p, step] = value.astype(BF16)
        send(
            dsend.at[d, p, step], drecv.at[d, p, step], dds.at[d, p, step], ddr.at[d, p, step],
            (z, x, (yp, ym)[d], c),
        )

    @pl.when(half == c)
    def _():
        wait(sx.at[pl.ds(0, 240)], tdr.at[0])

    @pl.when(half != c)
    def _():
        wait(sx, tdr.at[0])

    for h in (0, 1):
        stat = sx[h * 128 : h * 128 + 128, :]
        scales = stat[:, 48:64].astype(F32)
        scales = scales[:, 0:1] + scales[:, 1:2] + scales[:, 2:3]
        shifts = [[dot(stat, gsum[k, s], 1, 0) for s in range(2)] for k in range(2)]
        for k in (0, 1):
            xg_wait(4, h, k)
        absorb(4, h)
        for s in range(2):
            g = (accg[h, s] + shifts[0][s]) * scales
            act[h, s] = (g / (1.0 + jnp.exp(-g)) * ((accu[h, s] + shifts[1][s]) * scales)).astype(BF16)
        produce(h, 4)
        pass_on(0, h, 0, 0)
        pass_on(1, h, 1, 0)
        produce(h, 3)
        pass_on(0, h, 1, 0)
        produce(h, 5)
        pass_on(1, h, 0, 0)
    for r in (2, 6, 1, 7, 0):
        for h in (0, 1):
            produce(h, r)
    for step in (1, 2, 3):
        for h in (0, 1):
            for d, k in ((0, 0), (1, 1), (0, 1), (1, 0)):
                if step < length(d, k):
                    pass_on(d, h, k, step)

    ret_at = unit(me)

    def give_back(h):
        tx = c + 2 * h
        for dz in far_z:
            tz = lax.rem(z + dz, NZ)
            for k in range(2):
                def go():
                    send(eo.at[k, unit(h * NZ + tz)], ret.at[ret_at], rts.at[0], rtr.at[0], (tz, tx, y, k))

                if dz:
                    go()
                else:
                    pl.when(jnp.logical_or(tx != x, c != k))(go)

    for h in (0, 1):
        for k in (0, 1):
            value = part[h, 0, :, k * 128 : k * 128 + 128]
            for d in range(2):
                last, p = length(d, k) - 1, 2 * h + k
                wait(drecv.at[d, p, last], ddr.at[d, p, last])
                value = value + drecv[d, p, last].astype(F32)
            eo[k, pl.ds(h * 128, 128), :] = value.astype(BF16)
        give_back(h)

    @pl.when(half == c)
    def _():
        ret[ret_at, :] = eo[c, unit(place), :]

    wait_units(ret, rtr.at[0])

    zz = mixed[...]
    for k in range(2):
        zz = zz + gat[:, 2 + k : 3 + k] * dot(pmat[k], ret[...], 1, 0)

    mean = jnp.mean(zz, axis=1, keepdims=True)
    dev = zz - mean
    dev2 = jnp.sum(dev * dev, axis=1, keepdims=True)
    fin[0] = dev.astype(BF16)
    packed = jnp.where(lane == 0, mean, jnp.where(lane == 1, dev2, 0.0)).T
    stat2[0] = packed[0:2, :]
    send(fin.at[0], fin.at[1], fns.at[0], fnr.at[0], partner)
    for dy, dc in order:
        s = 2 * dy + dc
        dev_id = (z, x, lax.rem(y + dy, NY), c if dc == 0 else other)
        send(stat2.at[0], stat2.at[s], s2s.at[s - 1], s2r.at[s - 1], dev_id)
    direct = (5, 3, 2, 6, 1, 7)
    for dy in direct:
        send(fin.at[0], fin.at[2 * dy], fns.at[2 * dy - 1], fnr.at[2 * dy - 1], (z, x, lax.rem(y + dy, NY), c))
    for step in range(4):
        for d in range(2):
            for piece in range(5):
                if step < 3 or (piece >= 2) == d:
                    wait(kv.at[0, piece], kvs.at[d, step, piece])
            for p in range(4):
                if step < 3 or p % 2 == d:
                    wait(xg.at[0, pl.ds(0, 128)], xgs.at[d, step, p])
                if step < length(d, p % 2):
                    wait(dsend.at[d, p, step], dds.at[d, p, step])
    for r in range(3):
        for k in range(2):
            wait(qraw.at[0, q_parts[k]], qsd.at[r, k])
            wait(osend.at[r, pl.ds(2 * k, 2)], osd.at[r, k])
        wait(ssend.at[r], ssd.at[r])
    wait(wp.at[0], wsd.at[0])
    for k, buf in enumerate((wg, wu, wd)):
        wait(buf.at[0], wsd.at[1 + k])
    wait(heads.at[0], hsd.at[0])
    for r in (0, 1, 2, 4, 5, 6):
        wait(rsend.at[r], rsd.at[r])
    for k in range(2):
        wait(rsend.at[3, ends[k]], rsd.at[(3, 7)[k]])
    for s in range(15):
        wait(stat1.at[0], s1s.at[s])
    wait_units(disp, dps.at[0])

    @pl.when(half == c)
    def _():
        wait(tdisp.at[pl.ds(0, 496)], tds.at[0])

    wait_units(ret, rts.at[0])
    for s in range(1, 16):
        wait(stat2.at[s], s2r.at[s - 1])
    total = functools.reduce(jnp.add, [stat2[s] for s in range(16)])
    mean = total[0:1, :] * (1.0 / 16)
    spread = total[1:2, :] + 128.0 * functools.reduce(
        jnp.add, [jnp.square(stat2[s, 0:1, :] - mean) for s in range(16)]
    )
    scale = lax.rsqrt(spread * (1.0 / 2048) + EPS)
    table = jnp.where(sub == 16, scale, 0.0)
    for s in range(16):
        table = jnp.where(sub == s, stat2[s, 0:1, :] - mean, table)
    table = table.T

    def finish(dy, dc):
        s = 2 * dy + dc
        j = 2 * lax.rem(y + NY - dy, NY) + (c if dc == 0 else other)
        value = (fin[s].astype(F32) + table[:, s : s + 1]) * table[:, 16:17] * g2[pl.ds(j, 1), :]
        outb[s] = value.astype(BF16)
        pltpu.make_async_copy(outb.at[s], out.at[:, col(j)], oud.at[s]).start()

    finish(0, 0)
    wait(fin.at[1], fnr.at[0])
    finish(0, 1)
    arrivals = (*direct, 4)
    for i, dy in enumerate(arrivals):
        wait(fin.at[2 * dy], fnr.at[2 * dy - 1])
        if dy == 5:
            send(fin.at[10], fin.at[8], fns.at[7], fnr.at[7], (z, x, ym, c))
        send(fin.at[2 * dy], fin.at[2 * dy + 1], fns.at[2 * dy], fnr.at[2 * dy], partner)
        finish(dy, 0)
        if i:
            before_dy = arrivals[i - 1]
            wait(fin.at[2 * before_dy + 1], fnr.at[2 * before_dy])
            finish(before_dy, 1)
    wait(fin.at[9], fnr.at[8])
    finish(4, 1)

    for s in range(15):
        wait(stat2.at[0], s2s.at[s])
        wait(fin.at[0], fns.at[s])
    for s in range(16):
        wait(outb.at[s], oud.at[s])


def on_device(
    tokens, query_narrow, key_narrow, value_narrow, query_broad, key_broad, value_broad, mix_lambda,
    head_gain, proj_narrow, proj_broad, gain_one, gain_two, expert_ids, expert_gates,
    gate_weight, up_weight, down_weight,
):
    memory = pl.BlockSpec(memory_space=pltpu.HBM)
    dma = pltpu.SemaphoreType.DMA
    bf = lambda *s: pltpu.VMEM(s, BF16)
    fl = lambda *s: pltpu.VMEM(s, F32)
    scratch = [
        bf(8, 5, 128, 128), bf(4, 3, 128, 128), bf(4, 512, 128), fl(4, 128, 512), fl(8, 512),
        bf(3, 4, 128, 128), bf(3, 4, 128, 128), fl(3, 8, 128), fl(3, 8, 128),
        bf(2, 8, 256, 128), bf(8, 128, 512), bf(128, 128), fl(128, 128),
        fl(128, 128), bf(512, 128), bf(2, 128, 512), fl(128, 128),
        bf(2, 256, 128), bf(7, 128, 128), bf(7, 128, 128), fl(16, 2, 128),
        fl(128, 128), bf(512, 128), bf(8, 512, 128),
        bf(2, 2048, 256), bf(2, 2048, 256), bf(2, 256, 2048),
        fl(2, 2, 128, 256), fl(2, 2, 128, 256), bf(2, 2, 128, 256), fl(2, 8, 128, 256),
        bf(2, 4, 4, 128, 128), bf(2, 4, 4, 128, 128),
        bf(512, 128), bf(2, 256, 128), bf(16, 128, 128), fl(16, 2, 128),
        fl(1, 2), pltpu.VMEM((2, 128), jnp.int32), fl(2, 128), fl(2, 128), fl(16, 128), fl(16, 128),
        bf(16, 128, 128), bf(32, 2048), bf(2, 2, 128, 256), bf(512, 128), bf(256, 128),
        dma((13,)), dma((2, 4, 5)), dma((8, 5)), dma((3, 2)), dma((3, 2)), dma((4,)), dma((4,)),
        dma((3, 2)), dma((3, 2)), dma((3,)), dma((3,)), dma((1,)), dma((1,)), dma((8,)), dma((8,)),
        dma((15,)), dma((15,)), dma((1,)), dma((1,)), dma((2, 4, 4)), dma((8, 4)),
        dma((2, 4, 4)), dma((2, 4, 4)), dma((1,)), dma((1,)), dma((15,)), dma((15,)), dma((15,)), dma((15,)),
        dma((6,)), pltpu.SemaphoreType.REGULAR((3,)), dma((16,)), dma((1,)), dma((1,)),
    ]
    return pl.pallas_call(
        kernel,
        out_shape=jax.ShapeDtypeStruct((128, 2048), BF16),
        in_specs=[memory] * 18,
        out_specs=memory,
        scratch_shapes=scratch,
        compiler_params=pltpu.CompilerParams(
            collective_id=0, has_side_effects=True, vmem_limit_bytes=60 * 1024 * 1024
        ),
        name="layer",
    )(
        mix_lambda.T, expert_ids.T, expert_gates.T, head_gain, gain_one.reshape(16, 128), gain_two.reshape(16, 128),
        tokens, query_narrow, key_narrow, value_narrow, query_broad, key_broad, value_broad,
        proj_narrow, proj_broad, gate_weight, up_weight, down_weight,
    )


def solution(mesh):
    finer = Mesh(mesh.devices.reshape(NZ, NX, NY, 2), ("z", "x", "y", "c"))
    sp, tp = ("z", "x"), ("y", "c")
    return jax.shard_map(
        on_device,
        mesh=finer,
        in_specs=(
            P(sp, None), P(sp, tp), P(sp, tp), P(sp, tp), P(sp, tp), P(sp, tp), P(sp, tp), P(None, tp),
            P(), P(tp, None), P(tp, None), P(), P(), P(sp, None), P(sp, None),
            P(sp, None, tp), P(sp, None, tp), P(sp, tp, None),
        ),
        out_specs=P(sp, None),
        check_vma=False,
    )
```
